128 devices in a mesh: tp: 16 (over z, y), dp: 8 (over x, core).
Axes of the slice: x: 4, y: 4, z: 4, core: 2. Of those that a mesh axis runs over, the one named last changes fastest.
Arguments:
- tokens: bfloat16 [256, 4096], P('dp', 'tp'), may hold values from -6 to 6
- lengths: int32 [256], P('dp'), may hold values from 1 to 96, 6144 in all
- norm_gain: float32 [2, 4096], replicated, may hold values from 0.1 to 1.9
- w_recept: bfloat16 [2, 4096, 4096], P(None, None, ('tp', 'dp')), may hold values from -0.09375 to 0.09375
- w_key: bfloat16 [2, 4096, 4096], P(None, None, ('tp', 'dp')), may hold values from -0.09375 to 0.09375
- w_value: bfloat16 [2, 4096, 4096], P(None, None, ('tp', 'dp')), may hold values from -0.09375 to 0.09375
- w_decay: bfloat16 [2, 4096, 4096], P(None, None, ('tp', 'dp')), may hold values from -0.09375 to 0.09375
- w_rate: bfloat16 [2, 4096, 4096], P(None, None, ('tp', 'dp')), may hold values from -0.09375 to 0.09375
- w_gate: bfloat16 [2, 4096, 4096], P(None, None, ('tp', 'dp')), may hold values from -0.09375 to 0.09375
- w_out: bfloat16 [2, 4096, 4096], P(None, None, ('tp', 'dp')), may hold values from -0.09375 to 0.09375
- decay_base: float32 [2, 4096], P(None, 'tp'), may hold values from -3 to 1
- rate_base: float32 [2, 4096], P(None, 'tp'), may hold values from -3 to 3
- group_gain: float32 [2, 4096], P(None, 'tp'), may hold values from 0.1 to 1.9
- state: float32 [2, 256, 64, 64, 64], P(None, 'dp', 'tp'), may hold values from -6 to 6
Outputs:
- mixed: bfloat16 [256, 4096], P('dp', 'tp')
- new_state: float32 [2, 256, 64, 64, 64], P(None, 'dp', 'tp')
The draws below stay inside these ranges and needn't reach their ends.
Inputs may be any that keep to these rules, and one draw needn't show every extreme that they name: Each sequence's live length lies between 1 and 96, some sequences reach 96, and the lengths sum to 6144.
All inputs are finite; a program needn't handle non-finite values.
Results may differ from the reference program's by a relative error of at most 0.025.
Values may be sent and summed in bfloat16 or wider, within the bound.
No kernel may reach another device: no remote copies, remote signals or barrier semaphores. Data moves between devices by JAX's collectives and lax.ppermute only.
A program may use at most 128 MiB of HBM per device.

```python
import math
import jax
import jax.numpy as jnp
import numpy as np
from jax import lax

D = 4096
HEAD = 64
STEP = 16
BATCH = 256


def steps_of(key, extent, cuts, least, high):
    gain, own = 1.0, jax.random.fold_in(key, 6)
    for dim, blocks in cuts:
        heights = jnp.exp(jax.random.uniform(jax.random.fold_in(own, dim), (blocks,), jnp.float32, least / len(cuts), high / len(cuts)))
        gain = gain * jnp.repeat(heights, extent[dim] // blocks).reshape([-1 if axis == dim else 1 for axis in range(len(extent))])
    return gain


def profile(amount, total, reach, slope):
    loads = [(1 << 20) // math.isqrt(grade ** slope) + 1 for grade in range(2, amount + 1)]
    surplus, given = total - reach - (amount - 1), [1] * (amount - 1)
    while surplus > 0:
        candidates = [i for i in range(amount - 1) if given[i] < reach]
        pool, left = sum([loads[i] for i in candidates]), surplus
        for i in candidates:
            addition = min(reach - given[i], max(1, left * loads[i] // pool), surplus)
            given[i] = given[i] + addition
            surplus = surplus - addition
    return np.array([reach] + given)


def uneven_parts(key, amount, total, limit, slope):
    if amount == 2:
        one = jax.random.randint(key, (), max(1, total - limit), min(limit, total - 1) + 1)
        return jnp.stack([one, total - one])
    sizes = jnp.asarray(profile(amount, total, limit, slope), jnp.int32)
    couples = (amount - 1) // 2
    donor, receiver = sizes[1:1 + 2 * couples:2], sizes[2:2 + 2 * couples:2]
    room = jnp.minimum(donor - 1, limit - receiver)
    moved = jax.random.randint(jax.random.fold_in(key, 1), (couples,), 0, 1 << 20) % (room + 1)
    sizes = sizes.at[1:1 + 2 * couples:2].set(donor - moved).at[2:2 + 2 * couples:2].set(receiver + moved)
    return sizes[jax.random.permutation(jax.random.fold_in(key, 2), amount)]


def scatter_about(rng, dims, width, reach, pieces=(), dtype=jnp.bfloat16):
    level = steps_of(rng, dims, pieces, -0.22, 0.18) if pieces else 1.0
    values = jax.random.normal(rng, dims, jnp.float32) * width * level
    return jnp.minimum(jnp.maximum(values, -reach), reach).astype(dtype)


def setup_inputs(seed: int = 0) -> dict:
    splits = jax.random.split(jax.random.key(seed), 15)
    tokens = scatter_about(splits[0], (BATCH, D), 1.0, 6.0, ((0, 8), (1, 16)))
    lengths = uneven_parts(splits[1], BATCH, 24 * BATCH, 96, 2).astype(jnp.int32)
    norm_gain = jnp.clip(1.0 + 0.18 * jax.random.normal(splits[2], (2, D), jnp.float32), 0.1, 1.9)
    w_recept = scatter_about(splits[3], (2, D, D), D ** -0.5, 0.09375, ((2, 128),))
    w_key = scatter_about(splits[4], (2, D, D), D ** -0.5, 0.09375, ((2, 128),))
    w_value = scatter_about(splits[5], (2, D, D), D ** -0.5, 0.09375, ((2, 128),))
    w_decay = scatter_about(splits[6], (2, D, D), D ** -0.5, 0.09375, ((2, 128),))
    w_rate = scatter_about(splits[7], (2, D, D), D ** -0.5, 0.09375, ((2, 128),))
    w_gate = scatter_about(splits[8], (2, D, D), D ** -0.5, 0.09375, ((2, 128),))
    w_out = scatter_about(splits[9], (2, D, D), D ** -0.5, 0.09375, ((2, 128),))
    decay_base = jnp.clip(-3.0 + 4.0 * jax.random.uniform(splits[10], (2, D), jnp.float32) ** steps_of(splits[10], (2, D), ((1, 16),), -0.2, 0.2), -3.0, 1.0)
    rate_base = scatter_about(splits[11], (2, D), 0.5, 3.0, ((1, 16),), jnp.float32)
    group_gain = jnp.clip(1.0 + 0.18 * jax.random.normal(splits[12], (2, D), jnp.float32), 0.1, 1.9)
    state = scatter_about(splits[13], (2, BATCH, D // HEAD, HEAD, HEAD), 1.0, 6.0, ((1, 8), (2, 16)), jnp.float32)
    return dict(tokens=tokens, lengths=lengths, norm_gain=norm_gain, w_recept=w_recept, w_key=w_key, w_value=w_value, w_decay=w_decay, w_rate=w_rate, w_gate=w_gate, w_out=w_out, decay_base=decay_base, rate_base=rate_base, group_gain=group_gain, state=state)


RMS_EPS = 1e-06
GROUP_EPS = 0.00064

def stored(matrix, weight):
    product = jnp.dot(matrix, weight, preferred_element_type=jnp.float32)
    return lax.optimization_barrier(product.astype(jnp.bfloat16)).astype(jnp.float32)

def recur(state_old, recept, key_vec, value_vec, decay_rate, learn_rate, active, head_size):
    split = (recept.shape[0], -1, head_size)
    recept_h = recept.reshape(split)
    key_h = key_vec.reshape(split)
    value_h = value_vec.reshape(split)
    decay_h = decay_rate.reshape(split)
    rate_h = learn_rate.reshape(split)
    key_len = jnp.sqrt(lax.optimization_barrier(jnp.sum(key_h * key_h, axis=-1, keepdims=True)))
    key_unit = key_h / jnp.maximum(key_len, 1e-12)
    state_a = jnp.einsum('bhij,bhj->bhi', state_old, -key_unit, precision=lax.Precision.HIGHEST)
    updated = state_old * decay_h[:, :, None, :] + state_a[:, :, :, None] * (key_unit * rate_h)[:, :, None, :] + value_h[:, :, :, None] * (key_h * rate_h)[:, :, None, :]
    updated = jnp.where(active[:, None, None, None], updated, state_old)
    readout = jnp.einsum('bhij,bhj->bhi', updated, recept_h, precision=lax.Precision.HIGHEST)
    centre = lax.optimization_barrier(jnp.mean(readout, axis=-1, keepdims=True))
    spread = lax.optimization_barrier(jnp.mean(jnp.square(readout - centre), axis=-1, keepdims=True))
    normal_out = ((readout - centre) * lax.rsqrt(spread + GROUP_EPS)).reshape(recept.shape[0], -1)
    return (updated, normal_out)

def reference(tokens, lengths, norm_gain, w_recept, w_key, w_value, w_decay, w_rate, w_gate, w_out, decay_base, rate_base, group_gain, state):
    active = lengths > STEP
    current = tokens
    updated_states = []
    for layer_idx in range(2):
        values = current.astype(jnp.float32)
        factor = lax.rsqrt(lax.optimization_barrier(jnp.mean(values * values, axis=1, keepdims=True)) + RMS_EPS)
        normed = (values * factor * norm_gain[layer_idx]).astype(jnp.bfloat16)
        recept = stored(normed, w_recept[layer_idx])
        key_vec = stored(normed, w_key[layer_idx])
        value_vec = stored(normed, w_value[layer_idx])
        decay_pre = stored(normed, w_decay[layer_idx])
        rate_pre = stored(normed, w_rate[layer_idx])
        gate_pre = stored(normed, w_gate[layer_idx])
        decay_rate = jnp.exp(-jnp.exp(-jax.nn.softplus(-(decay_base[layer_idx] + decay_pre)) - 0.5))
        learn_rate = jax.nn.sigmoid(rate_base[layer_idx] + rate_pre)
        gate_open = jax.nn.sigmoid(gate_pre)
        updated, normal_out = recur(state[layer_idx], recept, key_vec, value_vec, decay_rate, learn_rate, active, HEAD)
        updated_states.append(updated)
        mixed_rows = jnp.where(active[:, None], normal_out * group_gain[layer_idx] * gate_open, 0.0).astype(jnp.bfloat16)
        current = jnp.dot(mixed_rows, w_out[layer_idx], preferred_element_type=jnp.float32).astype(jnp.bfloat16)
    return (current, jnp.stack(updated_states))
```

```python
import jax
import jax.numpy as jnp
from jax import lax
from jax.sharding import Mesh
from jax.sharding import PartitionSpec as P

STEP = 16
RMS_EPS = 1e-06
GROUP_EPS = 0.00064
TP = ("z", "y")
DP = ("x", "c")
CHIPS = ("z", "y", "x")
PAIR = [(0, 1), (1, 0)]


def spread(value):
    count = lax.axis_size(CHIPS)
    copies = jnp.broadcast_to(value[None], (count,) + value.shape)
    return lax.all_to_all(copies, CHIPS, 0, 0)


def both_cores(own, peer, core):
    first = jnp.where(core == 0, own, peer)
    second = jnp.where(core == 0, peer, own)
    return jnp.concatenate([first, second], axis=-1)


def recur(state_old, recept_h, key_h, value_h, decay_h, rate_h, active):
    key_len = jnp.sqrt(jnp.sum(key_h * key_h, axis=-1, keepdims=True))
    key_unit = key_h / jnp.maximum(key_len, 1e-12)
    state_a = jnp.einsum("bhij,bhj->bhi", state_old, -key_unit, precision=lax.Precision.DEFAULT)
    updated = (
        state_old * decay_h[:, :, None, :]
        + state_a[:, :, :, None] * (key_unit * rate_h)[:, :, None, :]
        + value_h[:, :, :, None] * (key_h * rate_h)[:, :, None, :]
    )
    updated = jnp.where(active[:, None, None, None], updated, state_old)
    readout = jnp.einsum("bhij,bhj->bhi", updated, recept_h, precision=lax.Precision.DEFAULT)
    centre = jnp.mean(readout, axis=-1, keepdims=True)
    spread_ = jnp.mean(jnp.square(readout - centre), axis=-1, keepdims=True)
    return updated, (readout - centre) * lax.rsqrt(spread_ + GROUP_EPS)


def local(
    tokens, lengths, norm_gain, w_recept, w_key, w_value, w_decay, w_rate, w_gate, w_out,
    decay_base, rate_base, group_gain, state,
):
    core = lax.axis_index("c")
    rows, feats = tokens.shape
    heads, head = state.shape[2], state.shape[-1]
    n_x = lax.axis_size("x")
    n_tp = lax.axis_size(TP)
    active = lengths > STEP
    weights = []
    for w in (w_recept, w_key, w_value, w_decay, w_rate, w_gate, w_out):
        own = w.swapaxes(1, 2)
        weights.append((own, lax.ppermute(own, "c", PAIR)))
    updated_states = []
    natural = spread(tokens).reshape(n_tp, n_x, rows, feats).transpose(1, 2, 0, 3)
    natural = natural.reshape(n_x * rows, n_tp * feats)
    for layer in range(2):
        joined = jnp.concatenate([p[layer] for own_peer in weights[:6] for p in own_peer], axis=0)
        values = natural.astype(jnp.float32)
        factor = lax.rsqrt(jnp.mean(values * values, axis=1, keepdims=True) + RMS_EPS)
        normed = (values * factor * norm_gain[layer]).astype(jnp.bfloat16)
        projected = lax.dot_general(
            normed, joined, (((1,), (1,)), ((), ())), preferred_element_type=jnp.float32
        ).astype(jnp.bfloat16)
        arrived = lax.all_to_all(projected.reshape(n_x, rows, -1), "x", 0, 0)
        parts = arrived.reshape(heads, rows, 6, 2, head // 2).astype(jnp.float32)
        recept, key_vec, value_vec, decay_pre, rate_pre, gate_pre = [
            jnp.concatenate(
                [
                    jnp.where(core == 0, parts[:, :, m, 0], parts[:, :, m, 1]),
                    jnp.where(core == 0, parts[:, :, m, 1], parts[:, :, m, 0]),
                ],
                axis=-1,
            ).transpose(1, 0, 2)
            for m in range(6)
        ]
        decay_b = decay_base[layer].reshape(heads, head)
        rate_b = rate_base[layer].reshape(heads, head)
        gain_b = group_gain[layer].reshape(heads, head)
        decay_rate = jnp.exp(-jnp.exp(-jax.nn.softplus(-(decay_b + decay_pre)) - 0.5))
        learn_rate = jax.nn.sigmoid(rate_b + rate_pre)
        gate_open = jax.nn.sigmoid(gate_pre)
        updated, normal_out = recur(
            state[layer], recept, key_vec, value_vec, decay_rate, learn_rate, active
        )
        updated_states.append(updated)
        mixed_here = jnp.where(active[:, None, None], normal_out * gain_b * gate_open, 0.0)
        mixed_here = mixed_here.astype(jnp.bfloat16).reshape(rows, feats)
        mixed_all = spread(mixed_here).reshape(n_tp, n_x, rows, feats).transpose(1, 2, 0, 3)
        mixed_all = mixed_all.reshape(n_x * rows, n_tp * feats)
        own, peer = weights[6]
        out_w = jnp.concatenate([own[layer], peer[layer]], axis=0)
        cols = lax.dot_general(
            out_w, mixed_all, (((1,), (1,)), ((), ())), preferred_element_type=jnp.float32
        ).astype(jnp.bfloat16)
        half = cols.shape[0] // 2
        cols = jnp.where(core == 0, cols, jnp.concatenate([cols[half:], cols[:half]], axis=0))
        if layer == 0:
            natural = spread(cols).reshape(n_tp * feats, n_x * rows).T
        else:
            blocks = cols.reshape(2 * half, n_x, rows).transpose(1, 2, 0)
            back = lax.all_to_all(blocks, "x", 0, 0)
            mixed = back.transpose(1, 0, 2).reshape(rows, feats)
    return mixed, jnp.stack(updated_states)


def solution(mesh):
    finer = Mesh(mesh.devices.reshape(4, 4, mesh.shape["dp"] // 2, 2), ("z", "y", "x", "c"))
    wide = P(None, None, TP + DP)
    in_specs = (
        (P(DP, TP), P(DP), P()) + (wide,) * 7 + (P(None, TP),) * 3 + (P(None, DP, TP, None, None),)
    )
    out_specs = (P(DP, TP), P(None, DP, TP, None, None))
    return jax.shard_map(local, mesh=finer, in_specs=in_specs, out_specs=out_specs, check_vma=False)
```

```python
import functools
import math

import jax
import jax.numpy as jnp
from jax import lax
from jax.experimental import pallas as pl
from jax.experimental.pallas import tpu as pltpu
from jax.sharding import Mesh
from jax.sharding import PartitionSpec as P

STEP = 16
RMS_EPS = 1e-06
GROUP_EPS = 0.00064
TP = ("z", "y")
DP = ("x", "c")
CHIPS = ("z", "y", "x")
PAIR = [(0, 1), (1, 0)]
ROWS_BY_ROWS = (((1,), (1,)), ((), ()))
ANY = pl.BlockSpec(memory_space=pl.ANY)
VMEM = pl.BlockSpec(memory_space=pltpu.VMEM)
SMEM = pl.BlockSpec(memory_space=pltpu.SMEM)


def project_kernel(layer, core_ref, acts_ref, gain_ref, *rest):
    weights, (out_ref, packed, normed, sems) = rest[:12], rest[12:]
    blocks, rows, feats = acts_ref.shape
    slim = weights[0].shape[1]
    core = core_ref[0]
    copies = []
    for idx, weight in enumerate(weights):
        half = core if idx % 2 == 0 else 1 - core
        start = pl.multiple_of((idx // 2) * 2 * slim + half * slim, slim)
        copy = pltpu.make_async_copy(
            weight.at[layer], packed.at[pl.ds(start, slim), :], sems.at[idx]
        )
        copy.start()
        copies.append(copy)
    squares = jnp.zeros((rows, feats), jnp.float32)
    for t in range(blocks):
        part = acts_ref[t].astype(jnp.float32)
        squares += part * part
    mean = jnp.sum(squares, axis=1, keepdims=True) / (blocks * feats)
    factor = lax.rsqrt(mean + RMS_EPS)
    for t in range(blocks):
        span = slice(t * feats, (t + 1) * feats)
        part = acts_ref[t].astype(jnp.float32) * factor * gain_ref[layer : layer + 1, span]
        normed[:, span] = part.astype(jnp.bfloat16)
    for copy in copies:
        copy.wait()
    result = lax.dot_general(
        normed[...], packed[...], ROWS_BY_ROWS, preferred_element_type=jnp.float32
    ).astype(jnp.bfloat16)
    per = out_ref.shape[1]
    for x in range(out_ref.shape[0]):
        out_ref[x] = result[x * per : (x + 1) * per]


def project(layer, core, acts, gain, weights, n_x):
    blocks, rows, feats = acts.shape
    slim, depth = weights[0].shape[1:]
    wide = slim * len(weights)
    return pl.pallas_call(
        functools.partial(project_kernel, layer),
        out_shape=jax.ShapeDtypeStruct((n_x, rows // n_x, wide), jnp.bfloat16),
        in_specs=[SMEM, VMEM, VMEM] + [ANY] * len(weights),
        out_specs=VMEM,
        scratch_shapes=[
            pltpu.VMEM((wide, depth), jnp.bfloat16),
            pltpu.VMEM((rows, depth), jnp.bfloat16),
            pltpu.SemaphoreType.DMA((len(weights),)),
        ],
        cost_estimate=pl.CostEstimate(
            flops=2 * rows * depth * wide, bytes_accessed=2 * depth * (wide + rows), transcendentals=0
        ),
        name=f"project_{layer}",
    )(core, acts, gain, *weights)


def readout_kernel(
    layer, arrived_ref, lengths_ref, decay_ref, rate_ref, gain_ref, state_ref,
    mixed_ref, rows_ref, column_ref, held, vectors, products, sems,
):
    heads, count, _ = arrived_ref.shape
    head = state_ref.shape[-1]
    chunks = sems.shape[0]
    per = count // chunks
    copies = []
    for idx in range(chunks):
        span = pl.ds(idx * per, per)
        copy = pltpu.make_async_copy(state_ref.at[layer, span], held.at[span], sems.at[idx])
        copy.start()
        copies.append(copy)
    kept = []
    for h in range(heads):
        lanes = slice(h * head, (h + 1) * head)
        block = arrived_ref[h].astype(jnp.float32)
        recept, key, value, decay_pre, rate_pre, gate_pre = [
            block[:, m * head : (m + 1) * head] for m in range(6)
        ]
        decay_in = decay_ref[layer : layer + 1, lanes] + decay_pre
        decay = jnp.exp(-math.exp(-0.5) * jax.nn.sigmoid(decay_in))
        rate = jax.nn.sigmoid(rate_ref[layer : layer + 1, lanes] + rate_pre)
        length = jnp.maximum(jnp.sqrt(jnp.sum(key * key, axis=1, keepdims=True)), 1e-12)
        unit = key / length
        learned = unit * rate
        vectors[:, h, :] = unit
        vectors[:, heads + h, :] = decay * recept
        rows_ref[:, h, :] = decay
        rows_ref[:, heads + h, :] = learned
        dot = jnp.sum(learned * recept, axis=1, keepdims=True)
        kept.append((value * length, dot, jax.nn.sigmoid(gate_pre)))
    own = lax.broadcasted_iota(jnp.int32, (2 * heads, heads * head), 0) % heads
    own = own == lax.broadcasted_iota(jnp.int32, (2 * heads, heads * head), 1) // head
    for r in range(count):
        if r % per == 0:
            copies[r // per].wait()
        matrix = held[r].reshape(heads * head, head).astype(jnp.bfloat16)
        product = lax.dot_general(
            vectors[r].astype(jnp.bfloat16), matrix, ROWS_BY_ROWS,
            preferred_element_type=jnp.float32,
        )
        product = jnp.where(own, product, 0.0)
        products[0, r : r + 1, :] = jnp.sum(product[:heads], axis=0, keepdims=True)
        products[1, r : r + 1, :] = jnp.sum(product[heads:], axis=0, keepdims=True)
    active = lengths_ref[...] > STEP
    mixed = []
    for h in range(heads):
        lanes = slice(h * head, (h + 1) * head)
        scaled, dot, gate = kept[h]
        column = scaled - products[0, :, lanes]
        column_ref[:, 0, lanes] = column
        readout = products[1, :, lanes] + column * dot
        centred = readout - jnp.mean(readout, axis=1, keepdims=True)
        spread_ = jnp.mean(centred * centred, axis=1, keepdims=True)
        normal = centred * lax.rsqrt(spread_ + GROUP_EPS)
        normal = normal * gain_ref[layer : layer + 1, lanes] * gate
        mixed.append(jnp.where(active, normal, 0.0))
    rows = jnp.concatenate(mixed, axis=1).astype(jnp.bfloat16)
    for t in range(mixed_ref.shape[0]):
        mixed_ref[t] = rows


def read_out(layer, arrived, lengths, decay_base, rate_base, group_gain, state, copies):
    heads, count, _ = arrived.shape
    head = state.shape[-1]
    f32 = jnp.float32
    return pl.pallas_call(
        functools.partial(readout_kernel, layer),
        out_shape=(
            jax.ShapeDtypeStruct((copies, count, heads * head), jnp.bfloat16),
            jax.ShapeDtypeStruct((count, 2 * heads, head), f32),
            jax.ShapeDtypeStruct((count, 1, heads * head), f32),
        ),
        in_specs=[VMEM] * 5 + [ANY],
        out_specs=(VMEM, VMEM, VMEM),
        scratch_shapes=[
            pltpu.VMEM((count, heads, head, head), f32),
            pltpu.VMEM((count, 2 * heads, head), f32),
            pltpu.VMEM((2, count, heads * head), f32),
            pltpu.SemaphoreType.DMA((8,)),
        ],
        cost_estimate=pl.CostEstimate(
            flops=4 * count * heads * head * head,
            bytes_accessed=8 * count * heads * head * head,
            transcendentals=4 * count * heads * head,
        ),
        name=f"read_out_{layer}",
    )(arrived, lengths, decay_base, rate_base, group_gain, state)


def update_kernel(per, lengths_ref, rows_ref, column_ref, state_ref, *rest):
    out_ref = rest[-1]
    _, _, heads, head, _ = state_ref.shape
    own = lax.broadcasted_iota(jnp.int32, (heads, heads * head), 0)
    own = own == lax.broadcasted_iota(jnp.int32, (heads, heads * head), 1) // head
    first = pl.program_id(0) * per
    for r in range(per):
        columns = jnp.where(own, column_ref[r], 0.0)
        added = lax.dot_general(
            columns, rows_ref[r, heads:, :], (((0,), (0,)), ((), ())),
            precision=lax.Precision.HIGHEST, preferred_element_type=jnp.float32,
        )
        active = lengths_ref[first + r] > STEP
        for h in range(heads):
            old = state_ref[0, r, h]
            new = old * rows_ref[r, h : h + 1, :] + added[h * head : (h + 1) * head]
            out_ref[0, r, h] = jnp.where(active, new, old)


def update(layer, lengths, rows, column, state, earlier):
    _, count, heads, head, _ = state.shape
    per = 4
    block = pl.BlockSpec((1, per, heads, head, head), lambda i: (layer, i, 0, 0, 0))
    more = () if earlier is None else (earlier,)
    return pl.pallas_call(
        functools.partial(update_kernel, per),
        grid=(count // per,),
        out_shape=jax.ShapeDtypeStruct(state.shape, state.dtype),
        in_specs=[
            SMEM,
            pl.BlockSpec((per, 2 * heads, head), lambda i: (i, 0, 0)),
            pl.BlockSpec((per, 1, heads * head), lambda i: (i, 0, 0)),
            block,
        ] + [ANY] * len(more),
        out_specs=block,
        input_output_aliases={4: 0} if more else {},
        cost_estimate=pl.CostEstimate(
            flops=4 * count * heads * head * head,
            bytes_accessed=16 * count * heads * head * head,
            transcendentals=0,
        ),
        name=f"update_{layer}",
    )(lengths, rows, column, state, *more)


def finish_kernel(layer, starts_ref, acts_ref, *rest):
    weights, (out_ref, packed, joined, sems) = rest[:8], rest[8:]
    blocks, _, feats = acts_ref.shape
    slim = weights[0].shape[1]
    copies = []
    for idx, weight in enumerate(weights):
        start = pl.multiple_of(starts_ref[idx] * slim, slim)
        copy = pltpu.make_async_copy(
            weight.at[layer], packed.at[pl.ds(start, slim), :], sems.at[idx]
        )
        copy.start()
        copies.append(copy)
    for t in range(blocks):
        joined[:, t * feats : (t + 1) * feats] = acts_ref[t]
    for copy in copies:
        copy.wait()
    result = lax.dot_general(
        joined[...], packed[...], ROWS_BY_ROWS, preferred_element_type=jnp.float32
    ).astype(jnp.bfloat16)
    for copy in range(out_ref.shape[0]):
        out_ref[copy] = result


def finish(layer, starts, acts, weights, copies):
    blocks, rows, feats = acts.shape
    slim, depth = weights[0].shape[1:]
    wide = slim * len(weights)
    return pl.pallas_call(
        functools.partial(finish_kernel, layer),
        out_shape=jax.ShapeDtypeStruct((copies, rows, wide), jnp.bfloat16),
        in_specs=[SMEM, VMEM] + [ANY] * len(weights),
        out_specs=VMEM,
        scratch_shapes=[
            pltpu.VMEM((wide, depth), jnp.bfloat16),
            pltpu.VMEM((rows, depth), jnp.bfloat16),
            pltpu.SemaphoreType.DMA((len(weights),)),
        ],
        cost_estimate=pl.CostEstimate(
            flops=2 * rows * depth * wide, bytes_accessed=2 * depth * (wide + rows), transcendentals=0
        ),
        name=f"finish_{layer}",
    )(starts, acts, *weights)


def local(
    tokens, lengths, norm_gain, w_recept, w_key, w_value, w_decay, w_rate, w_gate, w_out,
    decay_base, rate_base, group_gain, state,
):
    core, spot = lax.axis_index("c"), lax.axis_index("x")
    rows, feats = tokens.shape
    n_x, n_tp, n_chips = lax.axis_size("x"), lax.axis_size(TP), lax.axis_size(CHIPS)
    weights = []
    for w in (w_recept, w_key, w_value, w_decay, w_rate, w_gate):
        own = w.swapaxes(1, 2)
        weights += [own, lax.ppermute(own, "c", PAIR)]
    copies = jnp.broadcast_to(tokens[None], (n_chips, rows, feats))
    acts = lax.all_to_all(copies, CHIPS, 0, 0)
    out_own = w_out.swapaxes(1, 2)
    column = [out_own]
    for k in range(1, n_x):
        column.append(lax.ppermute(out_own, "x", [(i, (i + k) % n_x) for i in range(n_x)]))
    out_weights, starts = [], []
    for k, piece in enumerate(column):
        source = (spot + n_x - k) % n_x
        out_weights += [piece, lax.ppermute(piece, "c", PAIR)]
        starts += [source * 2 + core, source * 2 + 1 - core]
    starts = jnp.stack(starts).astype(jnp.int32)
    core_at = jnp.reshape(core, (1,)).astype(jnp.int32)
    lengths_column = lengths.reshape(rows, 1)
    new_state = None
    for layer in range(2):
        acts = acts.reshape(n_tp, n_x * rows, feats)
        projected = project(layer, core_at, acts, norm_gain, weights, n_x)
        arrived = lax.all_to_all(projected, "x", 0, 0)
        mixed, row_terms, column_terms = read_out(
            layer, arrived, lengths_column, decay_base, rate_base, group_gain, state, n_tp
        )
        mixed_all = lax.all_to_all(mixed, TP, 0, 0)
        new_state = update(layer, lengths, row_terms, column_terms, state, new_state)
        last = layer == 1
        current = finish(layer, starts, mixed_all, out_weights, 1 if last else n_chips)
        if not last:
            acts = lax.all_to_all(current, CHIPS, 0, 0)
    return current[0], new_state


def solution(mesh):
    finer = Mesh(mesh.devices.reshape(4, 4, mesh.shape["dp"] // 2, 2), ("z", "y", "x", "c"))
    wide = P(None, None, TP + DP)
    in_specs = (
        (P(DP, TP), P(DP), P()) + (wide,) * 7 + (P(None, TP),) * 3 + (P(None, DP, TP, None, None),)
    )
    out_specs = (P(DP, TP), P(None, DP, TP, None, None))
    return jax.shard_map(local, mesh=finer, in_specs=in_specs, out_specs=out_specs, check_vma=False)
```

```python
import functools
import math

import jax
import jax.numpy as jnp
from jax import lax
from jax.experimental import pallas as pl
from jax.experimental.pallas import tpu as pltpu
from jax.sharding import Mesh
from jax.sharding import PartitionSpec as P

STEP = 16
RMS_EPS = 1e-06
GROUP_EPS = 0.00064
TP = ("z", "y")
DP = ("x", "c")
CHIPS = ("z", "y", "x")
PAIR = [(0, 1), (1, 0)]
ROWS_BY_ROWS = (((1,), (1,)), ((), ()))
ANY = pl.BlockSpec(memory_space=pltpu.HBM)
VMEM = pl.BlockSpec(memory_space=pltpu.VMEM)
SMEM = pl.BlockSpec(memory_space=pltpu.SMEM)


COST = pl.CostEstimate(flops=1 << 31, bytes_accessed=8 << 20, transcendentals=0)
LIMIT = pltpu.CompilerParams(vmem_limit_bytes=48 << 20)


def pack_in_kernel(layer, core_ref, gain_ref, *rest):
    weights, (out_ref, held, sems) = rest[:12], rest[12:]
    slim = weights[0].shape[1]
    core = core_ref[0]
    copies = []
    for idx, weight in enumerate(weights):
        half = core if idx % 2 == 0 else 1 - core
        start = pl.multiple_of((idx // 2) * 2 * slim + half * slim, slim)
        copy = pltpu.make_async_copy(
            weight.at[layer], held.at[pl.ds(start, slim), :], sems.at[idx]
        )
        copy.start()
        copies.append(copy)
    for idx in range(0, len(copies), 2):
        copies[idx].wait()
        copies[idx + 1].wait()
        span = slice(idx * slim, (idx + 2) * slim)
        scaled = held[span, :].astype(jnp.float32) * gain_ref[layer : layer + 1, :]
        out_ref[span, :] = scaled.astype(jnp.bfloat16)


def pack_in(layer, core, gain, weights):
    slim, depth = weights[0].shape[1:]
    wide = slim * len(weights)
    return pl.pallas_call(
        functools.partial(pack_in_kernel, layer),
        out_shape=jax.ShapeDtypeStruct((wide, depth), jnp.bfloat16),
        in_specs=[SMEM, VMEM] + [ANY] * len(weights),
        out_specs=VMEM,
        scratch_shapes=[
            pltpu.VMEM((wide, depth), jnp.bfloat16),
            pltpu.SemaphoreType.DMA((len(weights),)),
        ],
        cost_estimate=COST,
        compiler_params=LIMIT,
        name=f"pack_in_{layer}",
    )(core, gain, *weights)


def project_kernel(acts_ref, packed_ref, out_ref):
    blocks, rows, feats = acts_ref.shape
    wide = packed_ref.shape[0]
    squares = jnp.zeros((rows, feats), jnp.float32)
    for t in range(blocks):
        part = acts_ref[t].astype(jnp.float32)
        squares += part * part
    mean = jnp.sum(squares, axis=1, keepdims=True) / (blocks * feats)
    factor = lax.rsqrt(mean + RMS_EPS)
    result = jnp.zeros((rows, wide), jnp.float32)
    for t in range(blocks):
        result += lax.dot_general(
            acts_ref[t], packed_ref[:, t * feats : (t + 1) * feats], ROWS_BY_ROWS,
            preferred_element_type=jnp.float32,
        )
    result = (result * factor).astype(jnp.bfloat16)
    per = out_ref.shape[1]
    for x in range(out_ref.shape[0]):
        out_ref[x] = result[x * per : (x + 1) * per]


def project(layer, acts, packed, n_x):
    rows = acts.shape[1]
    return pl.pallas_call(
        project_kernel,
        out_shape=jax.ShapeDtypeStruct((n_x, rows // n_x, packed.shape[0]), jnp.bfloat16),
        in_specs=[VMEM, VMEM],
        out_specs=VMEM,
        cost_estimate=COST,
        compiler_params=LIMIT,
        name=f"project_{layer}",
    )(acts, packed)


def table_kernel(layer, state_ref, out_ref, held, sems):
    chunks = out_ref.shape[0]
    count, heads, head, _ = held.shape
    per = count // chunks
    copies = []
    for idx in range(chunks):
        span = pl.ds(idx * per, per)
        copy = pltpu.make_async_copy(state_ref.at[layer, span], held.at[span], sems.at[idx])
        copy.start()
        copies.append(copy)
    for idx in range(chunks):
        copies[idx].wait()
        parts = [held[idx * per + k].reshape(heads * head, head) for k in range(per)]
        out_ref[idx] = jnp.concatenate(parts, axis=1).astype(jnp.bfloat16)


def table(layer, state):
    _, count, heads, head, _ = state.shape
    per = 4
    return pl.pallas_call(
        functools.partial(table_kernel, layer),
        out_shape=jax.ShapeDtypeStruct((count // per, heads * head, per * head), jnp.bfloat16),
        in_specs=[ANY],
        out_specs=VMEM,
        scratch_shapes=[
            pltpu.VMEM((count, heads, head, head), jnp.float32),
            pltpu.SemaphoreType.DMA((count // per,)),
        ],
        cost_estimate=COST,
        compiler_params=LIMIT,
        name=f"table_{layer}",
    )(state)


def vectors_of(layer, block, lanes, decay_ref, rate_ref):
    head = block.shape[1] // 6
    recept, key, value, decay_pre, rate_pre, gate_pre = [
        block[:, m * head : (m + 1) * head] for m in range(6)
    ]
    decay_in = decay_ref[layer : layer + 1, lanes] + decay_pre
    decay = jnp.exp(-math.exp(-0.5) * jax.nn.sigmoid(decay_in))
    rate = jax.nn.sigmoid(rate_ref[layer : layer + 1, lanes] + rate_pre)
    length = jnp.maximum(jnp.sqrt(jnp.sum(key * key, axis=1, keepdims=True)), 1e-12)
    unit = key / length
    return recept, value, gate_pre, decay, length, unit, unit * rate


def readout_kernel(
    layer, arrived_ref, lengths_ref, decay_ref, rate_ref, gain_ref, table_ref, mixed_ref, column_ref
):
    heads, count, wide = arrived_ref.shape
    head = wide // 6
    units, reads, kept = [], [], []
    for h in range(heads):
        lanes = slice(h * head, (h + 1) * head)
        block = arrived_ref[h].astype(jnp.float32)
        recept, value, gate_pre, decay, length, unit, learned = vectors_of(
            layer, block, lanes, decay_ref, rate_ref
        )
        units.append(unit)
        reads.append(decay * recept)
        dot = jnp.sum(learned * recept, axis=1, keepdims=True)
        kept.append((value * length, dot, jax.nn.sigmoid(gate_pre)))
    per = table_ref.shape[2] // head
    group = 8
    shape = (2 * heads * group, per * head)
    row = lax.broadcasted_iota(jnp.int32, shape, 0) % group
    spot = lax.broadcasted_iota(jnp.int32, shape, 1) // head
    lane_head = lax.broadcasted_iota(jnp.int32, (group, heads * head), 1) // head
    summed = ([], [])
    for g in range(count // group):
        rows = slice(g * group, (g + 1) * group)
        left = jnp.concatenate(
            [jnp.concatenate([v[rows]] * per, axis=1) for v in units + reads], axis=0
        )
        product = jnp.zeros((shape[0], heads * head), jnp.float32)
        for part in range(group // per):
            chosen = jnp.where(row == spot + part * per, left, 0.0).astype(jnp.bfloat16)
            product += lax.dot_general(
                chosen, table_ref[g * (group // per) + part], ROWS_BY_ROWS,
                preferred_element_type=jnp.float32,
            )
        for kind in range(2):
            base = kind * heads * group
            total = product[base : base + group]
            for h in range(1, heads):
                piece = product[base + h * group : base + (h + 1) * group]
                total = jnp.where(lane_head == h, piece, total)
            summed[kind].append(total)
    by_unit, by_read = [jnp.concatenate(parts, axis=0) for parts in summed]
    active = lengths_ref[...] > STEP
    mixed = []
    for h in range(heads):
        lanes = slice(h * head, (h + 1) * head)
        scaled, dot, gate = kept[h]
        column = scaled - by_unit[:, lanes]
        column_ref[:, lanes] = column
        readout = by_read[:, lanes] + column * dot
        centred = readout - jnp.mean(readout, axis=1, keepdims=True)
        spread_ = jnp.mean(centred * centred, axis=1, keepdims=True)
        normal = centred * lax.rsqrt(spread_ + GROUP_EPS)
        normal = normal * gain_ref[layer : layer + 1, lanes] * gate
        mixed.append(jnp.where(active, normal, 0.0))
    rows = jnp.concatenate(mixed, axis=1).astype(jnp.bfloat16)
    for t in range(mixed_ref.shape[0]):
        mixed_ref[t] = rows


def read_out(layer, arrived, lengths, decay_base, rate_base, group_gain, states, copies):
    heads, count, wide = arrived.shape
    feats = heads * wide // 6
    return pl.pallas_call(
        functools.partial(readout_kernel, layer),
        out_shape=(
            jax.ShapeDtypeStruct((copies, count, feats), jnp.bfloat16),
            jax.ShapeDtypeStruct((count, feats), jnp.float32),
        ),
        in_specs=[VMEM] * 6,
        out_specs=(VMEM, VMEM),
        cost_estimate=COST,
        compiler_params=LIMIT,
        name=f"read_out_{layer}",
    )(arrived, lengths, decay_base, rate_base, group_gain, states)


def update_kernel(
    layer, per, lengths_ref, arrived_ref, decay_ref, rate_ref, column_ref, state_ref, *rest
):
    out_ref, rows_ref = rest[-2:]
    _, _, heads, head, _ = state_ref.shape

    @pl.when(pl.program_id(0) == 0)
    def _():
        for h in range(heads):
            lanes = slice(h * head, (h + 1) * head)
            block = arrived_ref[h].astype(jnp.float32)
            _, _, _, decay, _, _, learned = vectors_of(layer, block, lanes, decay_ref, rate_ref)
            rows_ref[:, h, :] = decay
            rows_ref[:, heads + h, :] = learned

    own = lax.broadcasted_iota(jnp.int32, (heads, heads * head), 0)
    own = own == lax.broadcasted_iota(jnp.int32, (heads, heads * head), 1) // head
    first = pl.program_id(0) * per
    for k in range(per):
        r = first + k
        columns = jnp.where(own, column_ref[pl.ds(r, 1), :], 0.0)
        vectors = rows_ref[r]
        added = lax.dot_general(
            columns, vectors[heads:], (((0,), (0,)), ((), ())),
            precision=lax.Precision.HIGHEST, preferred_element_type=jnp.float32,
        )
        active = lengths_ref[r] > STEP
        for h in range(heads):
            old = state_ref[0, k, h]
            new = old * vectors[h : h + 1] + added[h * head : (h + 1) * head]
            out_ref[0, k, h] = jnp.where(active, new, old)


def update(layer, lengths, arrived, decay_base, rate_base, column, state, earlier):
    _, count, heads, head, _ = state.shape
    per = 4
    block = pl.BlockSpec((1, per, heads, head, head), lambda i: (layer, i, 0, 0, 0))
    more = () if earlier is None else (earlier,)
    return pl.pallas_call(
        functools.partial(update_kernel, layer, per),
        grid=(count // per,),
        out_shape=jax.ShapeDtypeStruct(state.shape, state.dtype),
        in_specs=[SMEM, VMEM, VMEM, VMEM, VMEM, block] + [ANY] * len(more),
        out_specs=block,
        scratch_shapes=[pltpu.VMEM((count, 2 * heads, head), jnp.float32)],
        input_output_aliases={6: 0} if more else {},
        cost_estimate=COST,
        compiler_params=LIMIT,
        name=f"update_{layer}",
    )(lengths, arrived, decay_base, rate_base, column, state, *more)


def pack_out_kernel(layer, starts_ref, *rest):
    weights, (out_ref, sems) = rest[:8], rest[8:]
    slim = weights[0].shape[1]
    copies = []
    for idx, weight in enumerate(weights):
        start = pl.multiple_of(starts_ref[idx] * slim, slim)
        copy = pltpu.make_async_copy(
            weight.at[layer], out_ref.at[pl.ds(start, slim), :], sems.at[idx]
        )
        copy.start()
        copies.append(copy)
    for copy in copies:
        copy.wait()


def pack_out(layer, starts, weights):
    slim, depth = weights[0].shape[1:]
    return pl.pallas_call(
        functools.partial(pack_out_kernel, layer),
        out_shape=jax.ShapeDtypeStruct((slim * len(weights), depth), jnp.bfloat16),
        in_specs=[SMEM] + [ANY] * len(weights),
        out_specs=VMEM,
        scratch_shapes=[pltpu.SemaphoreType.DMA((len(weights),))],
        cost_estimate=COST,
        compiler_params=LIMIT,
        name=f"pack_out_{layer}",
    )(starts, *weights)


def finish_kernel(acts_ref, packed_ref, out_ref):
    blocks, rows, feats = acts_ref.shape
    result = jnp.zeros((rows, packed_ref.shape[0]), jnp.float32)
    for t in range(blocks):
        result += lax.dot_general(
            acts_ref[t], packed_ref[:, t * feats : (t + 1) * feats], ROWS_BY_ROWS,
            preferred_element_type=jnp.float32,
        )
    result = result.astype(jnp.bfloat16)
    for copy in range(out_ref.shape[0]):
        out_ref[copy] = result


def finish(layer, acts, packed, copies):
    return pl.pallas_call(
        finish_kernel,
        out_shape=jax.ShapeDtypeStruct((copies, acts.shape[1], packed.shape[0]), jnp.bfloat16),
        in_specs=[VMEM, VMEM],
        out_specs=VMEM,
        cost_estimate=COST,
        compiler_params=LIMIT,
        name=f"finish_{layer}",
    )(acts, packed)


def local(
    tokens, lengths, norm_gain, w_recept, w_key, w_value, w_decay, w_rate, w_gate, w_out,
    decay_base, rate_base, group_gain, state,
):
    core, spot = lax.axis_index("c"), lax.axis_index("x")
    rows, feats = tokens.shape
    n_x, n_tp, n_chips = lax.axis_size("x"), lax.axis_size(TP), lax.axis_size(CHIPS)
    weights = []
    for w in (w_recept, w_key, w_value, w_decay, w_rate, w_gate):
        own = w.swapaxes(1, 2)
        weights += [own, lax.ppermute(own, "c", PAIR)]
    copies = jnp.broadcast_to(tokens[None], (n_chips, rows, feats))
    acts = lax.all_to_all(copies, CHIPS, 0, 0)
    out_own = w_out.swapaxes(1, 2)
    column = [out_own]
    for k in range(1, n_x):
        column.append(lax.ppermute(out_own, "x", [(i, (i + k) % n_x) for i in range(n_x)]))
    starts = []
    for k in range(n_x):
        source = (spot + n_x - k) % n_x
        starts += [source * 2 + core, source * 2 + 1 - core]
    starts = jnp.stack(starts).astype(jnp.int32)
    core_at = jnp.reshape(core, (1,)).astype(jnp.int32)
    lengths_column = lengths.reshape(rows, 1)
    new_state = None
    for layer in range(2):
        acts = acts.reshape(n_tp, n_x * rows, feats)
        packed = pack_in(layer, core_at, norm_gain, weights)
        states = table(layer, state)
        projected = project(layer, acts, packed, n_x)
        arrived = lax.all_to_all(projected, "x", 0, 0)
        if layer == 0:
            arrived, column = lax.optimization_barrier((arrived, column))
            out_weights = []
            for piece in column:
                out_weights += [piece, lax.ppermute(piece, "c", PAIR)]
        mixed, column_terms = read_out(
            layer, arrived, lengths_column, decay_base, rate_base, group_gain, states, n_tp
        )
        mixed_all = lax.all_to_all(mixed, TP, 0, 0)
        new_state = update(
            layer, lengths, arrived, decay_base, rate_base, column_terms, state, new_state
        )
        packed_out = pack_out(layer, starts, out_weights)
        last = layer == 1
        current = finish(layer, mixed_all, packed_out, 1 if last else n_chips)
        if not last:
            acts = lax.all_to_all(current, CHIPS, 0, 0)
            acts, new_state = lax.optimization_barrier((acts, new_state))
    return current[0], new_state


def solution(mesh):
    finer = Mesh(mesh.devices.reshape(4, 4, mesh.shape["dp"] // 2, 2), ("z", "y", "x", "c"))
    wide = P(None, None, TP + DP)
    in_specs = (
        (P(DP, TP), P(DP), P()) + (wide,) * 7 + (P(None, TP),) * 3 + (P(None, DP, TP, None, None),)
    )
    out_specs = (P(DP, TP), P(None, DP, TP, None, None))
    return jax.shard_map(local, mesh=finer, in_specs=in_specs, out_specs=out_specs, check_vma=False)
```

```python
import functools
import math

import jax
import jax.numpy as jnp
from jax import lax
from jax.experimental import pallas as pl
from jax.experimental.pallas import tpu as pltpu
from jax.sharding import Mesh
from jax.sharding import PartitionSpec as P


STEP = 16
RMS_EPS = 1e-06
GROUP_EPS = 0.00064
TP = ("z", "y")
DP = ("x", "c")
CHIPS = ("z", "y", "x")
PAIR = [(0, 1), (1, 0)]
SLOTS = 24
LANES = 128
ROWS_BY_ROWS = (((1,), (1,)), ((), ()))
ANY = pl.BlockSpec(memory_space=pltpu.HBM)
VMEM = pl.BlockSpec(memory_space=pltpu.VMEM)
SMEM = pl.BlockSpec(memory_space=pltpu.SMEM)


COST = pl.CostEstimate(flops=1 << 31, bytes_accessed=8 << 20, transcendentals=0)
LIMIT = pltpu.CompilerParams(vmem_limit_bytes=24 << 20)


def in_hbm(array):
    return pltpu.with_memory_space_constraint(array, pltpu.HBM)


def live_slots(lengths_row, first, slots):
    live = (lengths_row > STEP).astype(jnp.float32)
    count = live.shape[1]
    before = lax.broadcasted_iota(jnp.int32, (count, count), 0)
    before = before < lax.broadcasted_iota(jnp.int32, (count, count), 1)
    place = jnp.dot(
        jnp.broadcast_to(live, (8, count)), before.astype(jnp.float32),
        preferred_element_type=jnp.float32,
    )[:1]
    wanted = lax.broadcasted_iota(jnp.int32, (slots, count), 0) + first
    return jnp.where((place == wanted.astype(jnp.float32)) & (live > 0), 1.0, 0.0)


def choose_kernel(lengths_ref, tokens_ref, out_ref, count_ref):
    chosen = live_slots(lengths_ref[...], 0, out_ref.shape[1]).astype(jnp.bfloat16)
    rows = jnp.dot(chosen, tokens_ref[...], preferred_element_type=jnp.float32)
    rows = rows.astype(jnp.bfloat16)
    for copy in range(out_ref.shape[0]):
        out_ref[copy] = rows
    live = (lengths_ref[...] > STEP).astype(jnp.float32)
    count = jnp.sum(live, axis=1, keepdims=True)
    count_ref[...] = jnp.broadcast_to(count, count_ref.shape).astype(jnp.bfloat16)


def choose(lengths_row, tokens, slots, copies):
    return pl.pallas_call(
        choose_kernel,
        out_shape=(
            pltpu.HBM((copies, slots, tokens.shape[1]), jnp.bfloat16),
            jax.ShapeDtypeStruct((lengths_row.shape[1], LANES), jnp.bfloat16),
        ),
        in_specs=[VMEM, VMEM],
        out_specs=(VMEM, VMEM),
        compiler_params=LIMIT,
        name="choose",
    )(lengths_row, tokens)


def project_kernel(layer, core_ref, acts_ref, gain_ref, *rest):
    weights, (out_ref, held, sems) = rest[:12], rest[12:]
    blocks, rows, feats = acts_ref.shape
    wide, depth = held.shape
    slim = weights[0].shape[1]
    chunks = sems.shape[0]
    core = core_ref[0]
    copies = []
    for chunk in range(chunks):
        span = pl.ds(chunk * (depth // chunks), depth // chunks)
        for idx, weight in enumerate(weights):
            half = core if idx % 2 == 0 else 1 - core
            start = pl.multiple_of((idx // 2) * 2 * slim + half * slim, slim)
            copy = pltpu.make_async_copy(
                weight.at[layer, :, span], held.at[pl.ds(start, slim), span], sems.at[chunk, idx]
            )
            copy.start()
            copies.append(copy)
    squares = jnp.zeros((rows, feats), jnp.float32)
    for t in range(blocks):
        part = acts_ref[t].astype(jnp.float32)
        squares += part * part
    mean = jnp.sum(squares, axis=1, keepdims=True) / (blocks * feats)
    factor = lax.rsqrt(mean + RMS_EPS)
    result = jnp.zeros((rows, wide), jnp.float32)
    for t in range(blocks):
        if t % (blocks // chunks) == 0:
            first = t // (blocks // chunks) * len(weights)
            for copy in copies[first : first + len(weights)]:
                copy.wait()
        span = slice(t * feats, (t + 1) * feats)
        part = acts_ref[t].astype(jnp.float32) * factor * gain_ref[layer : layer + 1, span]
        result += lax.dot_general(
            part.astype(jnp.bfloat16), held[:, span], ROWS_BY_ROWS,
            preferred_element_type=jnp.float32,
        )
    result = result.astype(jnp.bfloat16)
    per = out_ref.shape[1]
    for x in range(out_ref.shape[0]):
        out_ref[x] = result[x * per : (x + 1) * per]


def project(layer, core, acts, gain, weights, n_x):
    rows = acts.shape[1]
    slim, depth = weights[0].shape[1:]
    wide = slim * len(weights)
    return pl.pallas_call(
        functools.partial(project_kernel, layer),
        out_shape=pltpu.HBM((n_x, rows // n_x, wide), jnp.bfloat16),
        in_specs=[SMEM, VMEM, VMEM] + [ANY] * len(weights),
        out_specs=VMEM,
        scratch_shapes=[
            pltpu.VMEM((wide, depth), jnp.bfloat16),
            pltpu.SemaphoreType.DMA((4, len(weights))),
        ],
        cost_estimate=COST,
        compiler_params=LIMIT,
    )(core, acts, gain, *map(in_hbm, weights))


def table_kernel(layer, lengths_ref, state_ref, out_ref, held, sems):
    chunks = out_ref.shape[0]
    slots, heads, head, _ = held.shape
    per = slots // chunks

    def fetch(sequence, slot):
        return pltpu.make_async_copy(
            state_ref.at[layer, sequence], held.at[slot], sems.at[slot]
        )

    def start(sequence, slot):
        live = lengths_ref[sequence] > STEP

        @pl.when(live & (slot < slots))
        def _():
            fetch(sequence, slot).start()

        return slot + live.astype(jnp.int32)

    count = lax.fori_loop(0, state_ref.shape[1], start, jnp.int32(0))
    for idx in range(chunks):
        for slot in range(idx * per, (idx + 1) * per):

            @pl.when(slot < count)
            def _():
                fetch(0, slot).wait()

            @pl.when(slot >= count)
            def _():
                held[slot] = jnp.zeros_like(held[slot])

        parts = [held[idx * per + k].reshape(heads * head, head) for k in range(per)]
        out_ref[idx] = jnp.concatenate(parts, axis=1).astype(jnp.bfloat16)


def table(layer, slots, lengths, state):
    _, _, heads, head, _ = state.shape
    per = 4
    return pl.pallas_call(
        functools.partial(table_kernel, layer),
        out_shape=pltpu.VMEM((slots // per, heads * head, per * head), jnp.bfloat16),
        in_specs=[SMEM, ANY],
        out_specs=VMEM,
        scratch_shapes=[
            pltpu.VMEM((slots, heads, head, head), jnp.float32),
            pltpu.SemaphoreType.DMA((slots,)),
        ],
        cost_estimate=COST,
        compiler_params=LIMIT,
    )(lengths, in_hbm(state))


def vectors_of(layer, block, lanes, decay_ref, rate_ref):
    head = block.shape[1] // 6
    recept, key, value, decay_pre, rate_pre, gate_pre = [
        block[:, m * head : (m + 1) * head] for m in range(6)
    ]
    decay_in = decay_ref[layer : layer + 1, lanes] + decay_pre
    decay = jnp.exp(-math.exp(-0.5) * jax.nn.sigmoid(decay_in))
    rate = jax.nn.sigmoid(rate_ref[layer : layer + 1, lanes] + rate_pre)
    length = jnp.maximum(jnp.sqrt(jnp.sum(key * key, axis=1, keepdims=True)), 1e-12)
    unit = key / length
    return recept, value, gate_pre, decay, length, unit, unit * rate


def readout_kernel(
    layer, arrived_ref, lengths_ref, decay_ref, rate_ref, gain_ref, table_ref, mixed_ref, column_ref
):
    heads, count, wide = arrived_ref.shape
    head = wide // 6
    units, reads, kept = [], [], []
    for h in range(heads):
        lanes = slice(h * head, (h + 1) * head)
        block = arrived_ref[h].astype(jnp.float32)
        recept, value, gate_pre, decay, length, unit, learned = vectors_of(
            layer, block, lanes, decay_ref, rate_ref
        )
        units.append(unit)
        reads.append(decay * recept)
        dot = jnp.sum(learned * recept, axis=1, keepdims=True)
        kept.append((value * length, dot, jax.nn.sigmoid(gate_pre)))
    per = table_ref.shape[2] // head
    group = 8
    shape = (2 * heads * group, per * head)
    row = lax.broadcasted_iota(jnp.int32, shape, 0) % group
    spot = lax.broadcasted_iota(jnp.int32, shape, 1) // head
    lane_head = lax.broadcasted_iota(jnp.int32, (group, heads * head), 1) // head
    summed = ([], [])
    for g in range(count // group):
        rows = slice(g * group, (g + 1) * group)
        left = jnp.concatenate(
            [jnp.concatenate([v[rows]] * per, axis=1) for v in units + reads], axis=0
        )
        product = jnp.zeros((shape[0], heads * head), jnp.float32)
        for part in range(group // per):
            chosen = jnp.where(row == spot + part * per, left, 0.0).astype(jnp.bfloat16)
            product += lax.dot_general(
                chosen, table_ref[g * (group // per) + part], ROWS_BY_ROWS,
                preferred_element_type=jnp.float32,
            )
        for kind in range(2):
            base = kind * heads * group
            total = product[base : base + group]
            for h in range(1, heads):
                piece = product[base + h * group : base + (h + 1) * group]
                total = jnp.where(lane_head == h, piece, total)
            summed[kind].append(total)
    by_unit, by_read = [jnp.concatenate(parts, axis=0) for parts in summed]
    live = jnp.sum((lengths_ref[...] > STEP).astype(jnp.float32), axis=1, keepdims=True)
    active = lax.broadcasted_iota(jnp.int32, (count, 1), 0).astype(jnp.float32) < live
    mixed = []
    for h in range(heads):
        lanes = slice(h * head, (h + 1) * head)
        scaled, dot, gate = kept[h]
        column = scaled - by_unit[:, lanes]
        column_ref[:, lanes] = column
        readout = by_read[:, lanes] + column * dot
        centred = readout - jnp.mean(readout, axis=1, keepdims=True)
        spread_ = jnp.mean(centred * centred, axis=1, keepdims=True)
        normal = centred * lax.rsqrt(spread_ + GROUP_EPS)
        normal = normal * gain_ref[layer : layer + 1, lanes] * gate
        mixed.append(jnp.where(active, normal, 0.0))
    rows = jnp.concatenate(mixed, axis=1).astype(jnp.bfloat16)
    for t in range(mixed_ref.shape[0]):
        mixed_ref[t] = rows


def read_out(layer, arrived, lengths, decay_base, rate_base, group_gain, states, copies):
    heads, count, wide = arrived.shape
    feats = heads * wide // 6
    return pl.pallas_call(
        functools.partial(readout_kernel, layer),
        out_shape=(
            pltpu.HBM((copies, count, feats), jnp.bfloat16),
            pltpu.VMEM((count, feats), jnp.float32),
        ),
        in_specs=[VMEM] * 6,
        out_specs=(VMEM, VMEM),
        cost_estimate=COST,
        compiler_params=LIMIT,
    )(arrived, lengths, decay_base, rate_base, group_gain, states)


def in_two(value):
    high = value.astype(jnp.bfloat16)
    return high, (value - high.astype(jnp.float32)).astype(jnp.bfloat16)


def update_kernel(
    layer, lengths_ref, arrived_ref, decay_ref, rate_ref, column_ref, others_ref, state_ref, *rest
):
    out_ref, held, rows_ref, columns_ref, in_sems, out_sems = rest[-6:]
    count, heads, head, _ = held.shape
    chunks = in_sems.shape[0]
    per = count // chunks

    def fetch(idx):
        span = pl.ds(idx * per, per)
        return pltpu.make_async_copy(state_ref.at[layer, span], held.at[span], in_sems.at[idx])

    def put(idx):
        span = pl.ds(idx * per, per)
        return pltpu.make_async_copy(held.at[span], out_ref.at[layer, span], out_sems.at[idx])

    for idx in range(chunks):
        fetch(idx).start()
    for h in range(heads):
        lanes = slice(h * head, (h + 1) * head)
        block = jnp.concatenate(
            [
                arrived_ref[h].astype(jnp.float32),
                others_ref[layer, :, h * 6 * head : (h + 1) * 6 * head],
            ],
            axis=0,
        )
        _, _, _, decay, _, _, learned = vectors_of(layer, block, lanes, decay_ref, rate_ref)
        rows_ref[:, h, :] = decay
        rows_ref[:, heads + h, :] = learned
    slots = column_ref.shape[0]
    columns_ref[:slots] = column_ref[...]
    columns_ref[slots:] = others_ref[layer, :, heads * 6 * head : heads * 7 * head]
    own = lax.broadcasted_iota(jnp.int32, (heads, heads * head), 0)
    own = own == lax.broadcasted_iota(jnp.int32, (heads, heads * head), 1) // head

    def advance(r, slot):
        live = lengths_ref[r] > STEP

        @pl.when(live)
        def _():
            high, low = in_two(jnp.where(own, columns_ref[pl.ds(slot, 1), :], 0.0))
            vectors = rows_ref[slot]
            right_high, right_low = in_two(vectors[heads:])
            added = lax.dot_general(
                jnp.concatenate([high, high, low], axis=0),
                jnp.concatenate([right_high, right_low, right_high], axis=0),
                (((0,), (0,)), ((), ())), preferred_element_type=jnp.float32,
            )
            for h in range(heads):
                new = held[r, h] * vectors[h : h + 1] + added[h * head : (h + 1) * head]
                held[r, h] = new

        return slot + live.astype(jnp.int32)

    slot = jnp.int32(0)
    for idx in range(chunks):
        fetch(idx).wait()
        slot = lax.fori_loop(idx * per, (idx + 1) * per, advance, slot)
        if idx:
            put(idx - 1).start()
    put(chunks - 1).start()
    for idx in range(chunks):
        put(idx).wait()


def update(layer, lengths, arrived, decay_base, rate_base, column, others, state, earlier):
    _, count, heads, head, _ = state.shape
    more = () if earlier is None else (earlier,)
    return pl.pallas_call(
        functools.partial(update_kernel, layer),
        out_shape=pltpu.HBM(state.shape, state.dtype),
        in_specs=[SMEM] + [VMEM] * 5 + [ANY] + [ANY] * len(more),
        out_specs=ANY,
        scratch_shapes=[
            pltpu.VMEM((count, heads, head, head), jnp.float32),
            pltpu.VMEM((count, 2 * heads, head), jnp.float32),
            pltpu.VMEM((count, heads * head), jnp.float32),
            pltpu.SemaphoreType.DMA((8,)),
            pltpu.SemaphoreType.DMA((8,)),
        ],
        input_output_aliases={7: 0} if more else {},
        cost_estimate=COST,
        compiler_params=LIMIT,
    )(lengths, arrived, decay_base, rate_base, column, others, in_hbm(state), *map(in_hbm, more))


def pack_out_kernel(starts_ref, *rest):
    weights, out_ref = rest[:8], rest[8]
    sems = rest[-1]
    slim, depth = weights[0].shape[0], out_ref.shape[1]
    copies = []
    for idx, weight in enumerate(weights):
        start = pl.multiple_of(starts_ref[idx] * slim, slim)
        copy = pltpu.make_async_copy(
            weight.at[:, pl.ds(0, depth)], out_ref.at[pl.ds(start, slim), :], sems.at[idx]
        )
        copy.start()
        copies.append(copy)
    if len(rest) > 10:
        most_ref, counts = rest[9:11]
        for idx, weight in enumerate(weights):
            copy = pltpu.make_async_copy(
                weight.at[:, pl.ds(depth, LANES)], counts.at[idx], sems.at[8 + idx]
            )
            copy.start()
            copies.append(copy)
    for copy in copies:
        copy.wait()
    if len(rest) > 10:
        most = jnp.max(counts[...].astype(jnp.float32), axis=0)
        most_ref[...] = jnp.max(most, axis=0, keepdims=True)


def pack_out(starts, weights, depth):
    slim, wide = weights[0].shape
    packed = pltpu.VMEM((slim * len(weights), depth), jnp.bfloat16)
    sems = pltpu.SemaphoreType.DMA((2 * len(weights),))
    counted = wide > depth
    counts = [pltpu.VMEM((len(weights), slim, LANES), jnp.bfloat16)] if counted else []
    most = jax.ShapeDtypeStruct((1, LANES), jnp.float32)
    return pl.pallas_call(
        pack_out_kernel,
        out_shape=(packed, most) if counted else packed,
        in_specs=[SMEM] + [ANY] * len(weights),
        out_specs=(VMEM, VMEM) if counted else VMEM,
        scratch_shapes=counts + [sems],
        cost_estimate=COST,
        compiler_params=LIMIT,
    )(starts, *weights)


def columns_of(acts_ref, packed_ref):
    blocks, rows, feats = acts_ref.shape
    result = jnp.zeros((rows, packed_ref.shape[0]), jnp.float32)
    for t in range(blocks):
        result += lax.dot_general(
            acts_ref[t], packed_ref[:, t * feats : (t + 1) * feats], ROWS_BY_ROWS,
            preferred_element_type=jnp.float32,
        )
    return result.astype(jnp.bfloat16)


def finish_kernel(acts_ref, packed_ref, out_ref):
    result = columns_of(acts_ref, packed_ref)
    for copy in range(out_ref.shape[0]):
        out_ref[copy] = result


def place_kernel(acts_ref, packed_ref, lengths_ref, others_ref, out_ref):
    result = columns_of(acts_ref, packed_ref)
    feats = result.shape[1]
    others = others_ref[1, :, others_ref.shape[2] - feats :].astype(jnp.bfloat16)
    every = jnp.concatenate([result.astype(jnp.float32), others.astype(jnp.float32)], axis=0)
    chosen = live_slots(lengths_ref[...], 0, every.shape[0]).astype(jnp.bfloat16)
    out_ref[...] = lax.dot_general(
        chosen, every.astype(jnp.bfloat16), (((0,), (0,)), ((), ())),
        preferred_element_type=jnp.float32,
    ).astype(jnp.bfloat16)


def finish(acts, packed, copies):
    return pl.pallas_call(
        finish_kernel,
        out_shape=pltpu.HBM((copies, acts.shape[1], packed.shape[0]), jnp.bfloat16),
        in_specs=[VMEM, VMEM],
        out_specs=VMEM,
        cost_estimate=COST,
        compiler_params=LIMIT,
        name="finish_0",
    )(acts, packed)


def place(acts, packed, lengths_row, others):
    return pl.pallas_call(
        place_kernel,
        out_shape=pltpu.HBM((lengths_row.shape[1], packed.shape[0]), jnp.bfloat16),
        in_specs=[VMEM] * 4,
        out_specs=VMEM,
        cost_estimate=COST,
        compiler_params=LIMIT,
        name="finish_1",
    )(acts, packed, lengths_row, others)


def spread(value):
    count = lax.axis_size(CHIPS)
    copies = jnp.broadcast_to(value[None], (count,) + value.shape)
    return lax.all_to_all(copies, CHIPS, 0, 0)


def in_order(own, peer, core):
    return jnp.concatenate(
        [jnp.where(core == 0, own, peer), jnp.where(core == 0, peer, own)], axis=0
    )


def beyond_slots(
    tokens, lengths_row, norm_gain, weights, w_out, decay_base, rate_base, group_gain, state
):
    core = lax.axis_index("c")
    count, feats = tokens.shape
    rows = count - SLOTS
    heads, head = state.shape[2], state.shape[-1]
    n_x, n_tp = lax.axis_size("x"), lax.axis_size(TP)
    chosen = live_slots(lengths_row, SLOTS, rows)
    live = jnp.sum((lengths_row > STEP).astype(jnp.float32))
    active = jnp.arange(rows) + SLOTS < live
    mine = jnp.dot(chosen.astype(jnp.bfloat16), tokens, preferred_element_type=jnp.float32)
    mine = mine.astype(jnp.bfloat16)
    held = jnp.argmax(chosen, axis=1)
    out_own = w_out.swapaxes(1, 2)
    out_peer = lax.ppermute(out_own, "c", PAIR)

    def block(natural, layer_parts):
        pairs, outs, gain_in, base, rate_b, gain, state_l = layer_parts
        joined = jnp.concatenate(
            [in_order(pairs[2 * m], pairs[2 * m + 1], core) for m in range(6)], axis=0
        )
        values = natural.astype(jnp.float32)
        factor = lax.rsqrt(jnp.mean(values * values, axis=1, keepdims=True) + RMS_EPS)
        normed = (values * factor * gain_in).astype(jnp.bfloat16)
        projected = lax.dot_general(
            normed, joined, ROWS_BY_ROWS, preferred_element_type=jnp.float32
        ).astype(jnp.bfloat16)
        arrived = lax.all_to_all(projected.reshape(n_x, rows, -1), "x", 0, 0)
        arrived = arrived.transpose(1, 0, 2).astype(jnp.float32)
        recept, key, value, decay_pre, rate_pre, gate_pre = [
            arrived[:, :, m * head : (m + 1) * head] for m in range(6)
        ]
        base, rate_b, gain = [part.reshape(heads, head) for part in (base, rate_b, gain)]
        decay = jnp.exp(-math.exp(-0.5) * jax.nn.sigmoid(base + decay_pre))
        rate = jax.nn.sigmoid(rate_b + rate_pre)
        length = jnp.maximum(jnp.sqrt(jnp.sum(key * key, axis=-1, keepdims=True)), 1e-12)
        unit = key / length
        old = jnp.take(state_l, held, axis=0)
        column = value * length - jnp.sum(old * unit[:, :, None, :], axis=-1)
        dot = jnp.sum(unit * rate * recept, axis=-1, keepdims=True)
        readout = jnp.sum(old * (decay * recept)[:, :, None, :], axis=-1) + column * dot
        centred = readout - jnp.mean(readout, axis=-1, keepdims=True)
        spread_ = jnp.mean(centred * centred, axis=-1, keepdims=True)
        normal = centred * lax.rsqrt(spread_ + GROUP_EPS) * gain * jax.nn.sigmoid(gate_pre)
        mixed = jnp.where(active[:, None, None], normal, 0.0)
        mixed = mixed.astype(jnp.bfloat16).reshape(rows, feats)
        mixed_all = spread(mixed).reshape(n_tp, n_x, rows, feats).transpose(1, 2, 0, 3)
        cols = lax.dot_general(
            mixed_all.reshape(n_x * rows, n_tp * feats), in_order(*outs, core),
            ROWS_BY_ROWS, preferred_element_type=jnp.float32,
        ).astype(jnp.bfloat16)
        blocks = spread(cols.reshape(rows, -1)).reshape(n_tp, n_x, n_x, rows, -1)
        current = blocks.transpose(2, 3, 0, 1, 4)
        here = lax.dynamic_slice_in_dim(current, lax.axis_index("x"), 1, 0)
        here = lax.dynamic_slice_in_dim(here, lax.axis_index(TP), 1, 2).reshape(rows, feats)
        terms = (arrived.reshape(rows, -1), column.reshape(rows, feats), here.astype(jnp.float32))
        return current.reshape(n_x * rows, n_tp * feats), jnp.concatenate(terms, axis=1)

    natural = spread(mine).reshape(n_tp, n_x, rows, feats).transpose(1, 2, 0, 3)
    layers = (weights, (out_own, out_peer), norm_gain, decay_base, rate_base, group_gain, state)
    return lax.scan(block, natural.reshape(n_x * rows, n_tp * feats), layers)[1]


def local(
    tokens, lengths, norm_gain, w_recept, w_key, w_value, w_decay, w_rate, w_gate, w_out,
    decay_base, rate_base, group_gain, state,
):
    core, spot = lax.axis_index("c"), lax.axis_index("x")
    rows, feats = tokens.shape
    n_x, n_tp, n_chips = lax.axis_size("x"), lax.axis_size(TP), lax.axis_size(CHIPS)
    starts = []
    for k in range(n_x):
        source = (spot + n_x - k) % n_x
        starts += [source * 2 + core, source * 2 + 1 - core]
    starts = jnp.stack(starts).astype(jnp.int32)
    core_at = jnp.reshape(core, (1,)).astype(jnp.int32)
    lengths_row = lengths.reshape(1, rows)

    def along_x(layer, more):
        own = jnp.concatenate([w_out.swapaxes(1, 2)[layer]] + more, axis=1)
        return [own] + [
            lax.ppermute(own, "x", [(i, (i + k) % n_x) for i in range(n_x)])
            for k in range(1, n_x)
        ]

    def over_pair(pieces):
        return [p for piece in pieces for p in (piece, lax.ppermute(piece, "c", PAIR))]

    chosen, count = choose(lengths_row, tokens, SLOTS, n_chips)
    acts = lax.all_to_all(chosen, CHIPS, 0, 0)
    weights = []
    for w in (w_recept, w_key, w_value, w_decay, w_rate, w_gate):
        own = w.swapaxes(1, 2)
        weights += [own, lax.ppermute(own, "c", PAIR)]
    states = [table(layer, SLOTS, lengths, state) for layer in range(2)]
    depth = n_tp * feats
    first, most = pack_out(starts, over_pair(along_x(0, [count])), depth)
    packed_out = [first, pack_out(starts, over_pair(along_x(1, [])), depth)]
    operands = (
        tokens, lengths_row, norm_gain, weights, w_out, decay_base, rate_base, group_gain, state
    )
    others = lax.cond(
        most[0, 0] > SLOTS,
        beyond_slots,
        lambda *_: jnp.zeros((2, rows - SLOTS, 8 * feats), jnp.float32),
        *operands,
    )
    new_state = None
    for layer in range(2):
        acts = acts.reshape(n_tp, n_x * SLOTS, feats)
        projected = project(layer, core_at, acts, norm_gain, weights, n_x)
        arrived = lax.all_to_all(projected, "x", 0, 0)
        mixed, column_terms = read_out(
            layer, arrived, lengths_row, decay_base, rate_base, group_gain, states[layer], n_tp
        )
        mixed_all = lax.all_to_all(mixed, TP, 0, 0)
        new_state = update(
            layer, lengths, arrived, decay_base, rate_base, column_terms, others, state, new_state
        )
        if layer == 0:
            current = finish(mixed_all, packed_out[0], n_chips)
            acts = lax.all_to_all(current, CHIPS, 0, 0)
    return place(mixed_all, packed_out[1], lengths_row, others), new_state


def solution(mesh):
    finer = Mesh(mesh.devices.reshape(4, 4, mesh.shape["dp"] // 2, 2), ("z", "y", "x", "c"))
    wide = P(None, None, TP + DP)
    in_specs = (
        (P(DP, TP), P(DP), P()) + (wide,) * 7 + (P(None, TP),) * 3 + (P(None, DP, TP, None, None),)
    )
    out_specs = (P(DP, TP), P(None, DP, TP, None, None))
    return jax.shard_map(local, mesh=finer, in_specs=in_specs, out_specs=out_specs, check_vma=False)
```

```python
import functools
import math

import jax
import jax.numpy as jnp
from jax import lax
from jax.experimental import pallas as pl
from jax.experimental.pallas import tpu as pltpu
from jax.sharding import Mesh
from jax.sharding import PartitionSpec as P


STEP = 16
RMS_EPS = 1e-06
GROUP_EPS = 0.00064
TP = ("z", "y")
DP = ("x", "c")
CHIPS = ("z", "y", "x")
PAIR = [(0, 1), (1, 0)]
SLOTS = 24
LANES = 128
ROWS_BY_ROWS = (((1,), (1,)), ((), ()))
ANY = pl.BlockSpec(memory_space=pltpu.HBM)
VMEM = pl.BlockSpec(memory_space=pltpu.VMEM)
SMEM = pl.BlockSpec(memory_space=pltpu.SMEM)


COST = pl.CostEstimate(flops=1 << 31, bytes_accessed=8 << 20, transcendentals=0)
LIMIT = pltpu.CompilerParams(vmem_limit_bytes=24 << 20)


def in_hbm(array):
    return pltpu.with_memory_space_constraint(array, pltpu.HBM)


def live_slots(lengths_row, first, slots):
    live = (lengths_row > STEP).astype(jnp.float32)
    count = live.shape[1]
    before = lax.broadcasted_iota(jnp.int32, (count, count), 0)
    before = before < lax.broadcasted_iota(jnp.int32, (count, count), 1)
    place = jnp.dot(
        jnp.broadcast_to(live, (8, count)), before.astype(jnp.float32),
        preferred_element_type=jnp.float32,
    )[:1]
    wanted = lax.broadcasted_iota(jnp.int32, (slots, count), 0) + first
    return jnp.where((place == wanted.astype(jnp.float32)) & (live > 0), 1.0, 0.0)


def choose_kernel(lengths_ref, tokens_ref, out_ref, count_ref):
    chosen = live_slots(lengths_ref[...], 0, out_ref.shape[1]).astype(jnp.bfloat16)
    rows = jnp.dot(chosen, tokens_ref[...], preferred_element_type=jnp.float32)
    rows = rows.astype(jnp.bfloat16)
    for copy in range(out_ref.shape[0]):
        out_ref[copy] = rows
    live = (lengths_ref[...] > STEP).astype(jnp.float32)
    count = jnp.sum(live, axis=1, keepdims=True)
    count_ref[...] = jnp.broadcast_to(count, count_ref.shape).astype(jnp.bfloat16)


def choose(lengths_row, tokens, slots, copies):
    return pl.pallas_call(
        choose_kernel,
        out_shape=(
            pltpu.HBM((copies, slots, tokens.shape[1]), jnp.bfloat16),
            jax.ShapeDtypeStruct((lengths_row.shape[1], LANES), jnp.bfloat16),
        ),
        in_specs=[VMEM, VMEM],
        out_specs=(VMEM, VMEM),
        compiler_params=LIMIT,
        name="choose",
    )(lengths_row, tokens)


def project_kernel(layer, core_ref, acts_ref, gain_ref, *rest):
    weights, (out_ref, held, sems) = rest[:12], rest[12:]
    blocks, rows, feats = acts_ref.shape
    wide, depth = held.shape
    slim = weights[0].shape[1]
    chunks = sems.shape[0]
    core = core_ref[0]
    copies = []
    for chunk in range(chunks):
        span = pl.ds(chunk * (depth // chunks), depth // chunks)
        for idx, weight in enumerate(weights):
            half = core if idx % 2 == 0 else 1 - core
            start = pl.multiple_of((idx // 2) * 2 * slim + half * slim, slim)
            copy = pltpu.make_async_copy(
                weight.at[layer, :, span], held.at[pl.ds(start, slim), span], sems.at[chunk, idx]
            )
            copy.start()
            copies.append(copy)
    squares = jnp.zeros((rows, feats), jnp.float32)
    for t in range(blocks):
        part = acts_ref[t].astype(jnp.float32)
        squares += part * part
    mean = jnp.sum(squares, axis=1, keepdims=True) / (blocks * feats)
    factor = lax.rsqrt(mean + RMS_EPS)
    result = jnp.zeros((rows, wide), jnp.float32)
    for t in range(blocks):
        if t % (blocks // chunks) == 0:
            first = t // (blocks // chunks) * len(weights)
            for copy in copies[first : first + len(weights)]:
                copy.wait()
        span = slice(t * feats, (t + 1) * feats)
        part = acts_ref[t].astype(jnp.float32) * factor * gain_ref[layer : layer + 1, span]
        result += lax.dot_general(
            part.astype(jnp.bfloat16), held[:, span], ROWS_BY_ROWS,
            preferred_element_type=jnp.float32,
        )
    result = result.astype(jnp.bfloat16)
    per = out_ref.shape[1]
    for x in range(out_ref.shape[0]):
        out_ref[x] = result[x * per : (x + 1) * per]


def project(layer, core, acts, gain, weights, n_x):
    rows = acts.shape[1]
    slim, depth = weights[0].shape[1:]
    wide = slim * len(weights)
    return pl.pallas_call(
        functools.partial(project_kernel, layer),
        out_shape=pltpu.HBM((n_x, rows // n_x, wide), jnp.bfloat16),
        in_specs=[SMEM, VMEM, VMEM] + [ANY] * len(weights),
        out_specs=VMEM,
        scratch_shapes=[
            pltpu.VMEM((wide, depth), jnp.bfloat16),
            pltpu.SemaphoreType.DMA((4, len(weights))),
        ],
        cost_estimate=COST,
        compiler_params=LIMIT,
    )(core, acts, gain, *weights)


def table_kernel(layer, lengths_ref, state_ref, out_ref, held, sems):
    chunks = out_ref.shape[0]
    slots, heads, head, _ = held.shape
    per = slots // chunks

    def fetch(sequence, slot):
        return pltpu.make_async_copy(
            state_ref.at[layer, sequence], held.at[slot], sems.at[slot]
        )

    def start(sequence, slot):
        live = lengths_ref[sequence] > STEP

        @pl.when(live & (slot < slots))
        def _():
            fetch(sequence, slot).start()

        return slot + live.astype(jnp.int32)

    count = lax.fori_loop(0, state_ref.shape[1], start, jnp.int32(0))
    for idx in range(chunks):
        for slot in range(idx * per, (idx + 1) * per):

            @pl.when(slot < count)
            def _():
                fetch(0, slot).wait()

            @pl.when(slot >= count)
            def _():
                held[slot] = jnp.zeros_like(held[slot])

        parts = [held[idx * per + k].reshape(heads * head, head) for k in range(per)]
        out_ref[idx] = jnp.concatenate(parts, axis=1).astype(jnp.bfloat16)


def table(layer, slots, lengths, state):
    _, _, heads, head, _ = state.shape
    per = 4
    return pl.pallas_call(
        functools.partial(table_kernel, layer),
        out_shape=pltpu.VMEM((slots // per, heads * head, per * head), jnp.bfloat16),
        in_specs=[SMEM, ANY],
        out_specs=VMEM,
        scratch_shapes=[
            pltpu.VMEM((slots, heads, head, head), jnp.float32),
            pltpu.SemaphoreType.DMA((slots,)),
        ],
        cost_estimate=COST,
        compiler_params=LIMIT,
    )(lengths, in_hbm(state))


def vectors_of(layer, block, lanes, decay_ref, rate_ref):
    head = block.shape[1] // 6
    recept, key, value, decay_pre, rate_pre, gate_pre = [
        block[:, m * head : (m + 1) * head] for m in range(6)
    ]
    decay_in = decay_ref[layer : layer + 1, lanes] + decay_pre
    decay = jnp.exp(-math.exp(-0.5) * jax.nn.sigmoid(decay_in))
    rate = jax.nn.sigmoid(rate_ref[layer : layer + 1, lanes] + rate_pre)
    length = jnp.maximum(jnp.sqrt(jnp.sum(key * key, axis=1, keepdims=True)), 1e-12)
    unit = key / length
    return recept, value, gate_pre, decay, length, unit, unit * rate


def readout_kernel(
    layer, arrived_ref, lengths_ref, decay_ref, rate_ref, gain_ref, table_ref, mixed_ref, column_ref
):
    heads, count, wide = arrived_ref.shape
    head = wide // 6
    units, reads, kept = [], [], []
    for h in range(heads):
        lanes = slice(h * head, (h + 1) * head)
        block = arrived_ref[h].astype(jnp.float32)
        recept, value, gate_pre, decay, length, unit, learned = vectors_of(
            layer, block, lanes, decay_ref, rate_ref
        )
        units.append(unit)
        reads.append(decay * recept)
        dot = jnp.sum(learned * recept, axis=1, keepdims=True)
        kept.append((value * length, dot, jax.nn.sigmoid(gate_pre)))
    per = table_ref.shape[2] // head
    group = 8
    shape = (2 * heads * group, per * head)
    row = lax.broadcasted_iota(jnp.int32, shape, 0) % group
    spot = lax.broadcasted_iota(jnp.int32, shape, 1) // head
    lane_head = lax.broadcasted_iota(jnp.int32, (group, heads * head), 1) // head
    summed = ([], [])
    for g in range(count // group):
        rows = slice(g * group, (g + 1) * group)
        left = jnp.concatenate(
            [jnp.concatenate([v[rows]] * per, axis=1) for v in units + reads], axis=0
        )
        product = jnp.zeros((shape[0], heads * head), jnp.float32)
        for part in range(group // per):
            chosen = jnp.where(row == spot + part * per, left, 0.0).astype(jnp.bfloat16)
            product += lax.dot_general(
                chosen, table_ref[g * (group // per) + part], ROWS_BY_ROWS,
                preferred_element_type=jnp.float32,
            )
        for kind in range(2):
            base = kind * heads * group
            total = product[base : base + group]
            for h in range(1, heads):
                piece = product[base + h * group : base + (h + 1) * group]
                total = jnp.where(lane_head == h, piece, total)
            summed[kind].append(total)
    by_unit, by_read = [jnp.concatenate(parts, axis=0) for parts in summed]
    live = jnp.sum((lengths_ref[...] > STEP).astype(jnp.float32), axis=1, keepdims=True)
    active = lax.broadcasted_iota(jnp.int32, (count, 1), 0).astype(jnp.float32) < live
    mixed = []
    for h in range(heads):
        lanes = slice(h * head, (h + 1) * head)
        scaled, dot, gate = kept[h]
        column = scaled - by_unit[:, lanes]
        column_ref[:, lanes] = column
        readout = by_read[:, lanes] + column * dot
        centred = readout - jnp.mean(readout, axis=1, keepdims=True)
        spread_ = jnp.mean(centred * centred, axis=1, keepdims=True)
        normal = centred * lax.rsqrt(spread_ + GROUP_EPS)
        normal = normal * gain_ref[layer : layer + 1, lanes] * gate
        mixed.append(jnp.where(active, normal, 0.0))
    rows = jnp.concatenate(mixed, axis=1).astype(jnp.bfloat16)
    for t in range(mixed_ref.shape[0]):
        mixed_ref[t] = rows


def read_out(layer, arrived, lengths, decay_base, rate_base, group_gain, states, copies):
    heads, count, wide = arrived.shape
    feats = heads * wide // 6
    return pl.pallas_call(
        functools.partial(readout_kernel, layer),
        out_shape=(
            pltpu.HBM((copies, count, feats), jnp.bfloat16),
            pltpu.VMEM((count, feats), jnp.float32),
        ),
        in_specs=[VMEM] * 6,
        out_specs=(VMEM, VMEM),
        cost_estimate=COST,
        compiler_params=LIMIT,
    )(arrived, lengths, decay_base, rate_base, group_gain, states)


def in_two(value):
    high = value.astype(jnp.bfloat16)
    return high, (value - high.astype(jnp.float32)).astype(jnp.bfloat16)


def update_kernel(
    layer, lengths_ref, arrived_ref, decay_ref, rate_ref, column_ref, others_ref, state_ref, *rest
):
    out_ref, held, rows_ref, columns_ref, in_sems, out_sems = rest[-6:]
    count, heads, head, _ = held.shape
    chunks = in_sems.shape[0]
    per = count // chunks

    def fetch(idx):
        span = pl.ds(idx * per, per)
        return pltpu.make_async_copy(state_ref.at[layer, span], held.at[span], in_sems.at[idx])

    def put(idx):
        span = pl.ds(idx * per, per)
        return pltpu.make_async_copy(held.at[span], out_ref.at[layer, span], out_sems.at[idx])

    for idx in range(chunks):
        fetch(idx).start()
    for h in range(heads):
        lanes = slice(h * head, (h + 1) * head)
        block = jnp.concatenate(
            [
                arrived_ref[h].astype(jnp.float32),
                others_ref[layer, :, h * 6 * head : (h + 1) * 6 * head],
            ],
            axis=0,
        )
        _, _, _, decay, _, _, learned = vectors_of(layer, block, lanes, decay_ref, rate_ref)
        rows_ref[:, h, :] = decay
        rows_ref[:, heads + h, :] = learned
    slots = column_ref.shape[0]
    columns_ref[:slots] = column_ref[...]
    columns_ref[slots:] = others_ref[layer, :, heads * 6 * head : heads * 7 * head]
    own = lax.broadcasted_iota(jnp.int32, (heads, heads * head), 0)
    own = own == lax.broadcasted_iota(jnp.int32, (heads, heads * head), 1) // head

    def advance(r, slot):
        live = lengths_ref[r] > STEP

        @pl.when(live)
        def _():
            high, low = in_two(jnp.where(own, columns_ref[pl.ds(slot, 1), :], 0.0))
            vectors = rows_ref[slot]
            right_high, right_low = in_two(vectors[heads:])
            added = lax.dot_general(
                jnp.concatenate([high, high, low], axis=0),
                jnp.concatenate([right_high, right_low, right_high], axis=0),
                (((0,), (0,)), ((), ())), preferred_element_type=jnp.float32,
            )
            for h in range(heads):
                new = held[r, h] * vectors[h : h + 1] + added[h * head : (h + 1) * head]
                held[r, h] = new

        return slot + live.astype(jnp.int32)

    slot = jnp.int32(0)
    for idx in range(chunks):
        fetch(idx).wait()
        slot = lax.fori_loop(idx * per, (idx + 1) * per, advance, slot)
        if idx:
            put(idx - 1).start()
    put(chunks - 1).start()
    for idx in range(chunks):
        put(idx).wait()


def update(layer, lengths, arrived, decay_base, rate_base, column, others, state, earlier):
    _, count, heads, head, _ = state.shape
    more = () if earlier is None else (earlier,)
    return pl.pallas_call(
        functools.partial(update_kernel, layer),
        out_shape=pltpu.HBM(state.shape, state.dtype),
        in_specs=[SMEM] + [VMEM] * 5 + [ANY] + [ANY] * len(more),
        out_specs=ANY,
        scratch_shapes=[
            pltpu.VMEM((count, heads, head, head), jnp.float32),
            pltpu.VMEM((count, 2 * heads, head), jnp.float32),
            pltpu.VMEM((count, heads * head), jnp.float32),
            pltpu.SemaphoreType.DMA((8,)),
            pltpu.SemaphoreType.DMA((8,)),
        ],
        input_output_aliases={7: 0} if more else {},
        cost_estimate=COST,
        compiler_params=LIMIT,
    )(lengths, arrived, decay_base, rate_base, column, others, in_hbm(state), *map(in_hbm, more))


def most_kernel(*refs):
    weights, (out_ref, counts, sems) = refs[:8], refs[8:]
    copies = []
    for idx, weight in enumerate(weights):
        _, wide = weight.shape
        copy = pltpu.make_async_copy(
            weight.at[:, pl.ds(wide - LANES, LANES)], counts.at[idx], sems.at[idx]
        )
        copy.start()
        copies.append(copy)
    for copy in copies:
        copy.wait()
    most = jnp.max(counts[...].astype(jnp.float32), axis=0)
    out_ref[...] = jnp.max(most, axis=0, keepdims=True)


def most_live(weights):
    return pl.pallas_call(
        most_kernel,
        out_shape=jax.ShapeDtypeStruct((1, LANES), jnp.float32),
        in_specs=[ANY] * len(weights),
        out_specs=VMEM,
        scratch_shapes=[
            pltpu.VMEM((len(weights), weights[0].shape[0], LANES), jnp.bfloat16),
            pltpu.SemaphoreType.DMA((len(weights),)),
        ],
        cost_estimate=COST,
        compiler_params=LIMIT,
        name="most_live",
    )(*weights)


def columns_of(starts_ref, acts_ref, weights, held, sems):
    blocks, rows, feats = acts_ref.shape
    wide, depth = held.shape
    slim = weights[0].shape[0]
    chunks = sems.shape[0]
    copies = []
    for chunk in range(chunks):
        span = pl.ds(chunk * (depth // chunks), depth // chunks)
        for idx, weight in enumerate(weights):
            start = pl.multiple_of(starts_ref[idx] * slim, slim)
            copy = pltpu.make_async_copy(
                weight.at[:, span], held.at[pl.ds(start, slim), span], sems.at[chunk, idx]
            )
            copy.start()
            copies.append(copy)
    result = jnp.zeros((rows, wide), jnp.float32)
    for t in range(blocks):
        if t % (blocks // chunks) == 0:
            first = t // (blocks // chunks) * len(weights)
            for copy in copies[first : first + len(weights)]:
                copy.wait()
        result += lax.dot_general(
            acts_ref[t], held[:, t * feats : (t + 1) * feats], ROWS_BY_ROWS,
            preferred_element_type=jnp.float32,
        )
    return result.astype(jnp.bfloat16)


def finish_kernel(starts_ref, acts_ref, *rest):
    weights, (out_ref, held, sems) = rest[:8], rest[8:]
    result = columns_of(starts_ref, acts_ref, weights, held, sems)
    for copy in range(out_ref.shape[0]):
        out_ref[copy] = result


def place_kernel(starts_ref, acts_ref, lengths_ref, others_ref, *rest):
    weights, (out_ref, held, sems) = rest[:8], rest[8:]
    result = columns_of(starts_ref, acts_ref, weights, held, sems)
    feats = result.shape[1]
    others = others_ref[1, :, others_ref.shape[2] - feats :]
    every = jnp.concatenate([result.astype(jnp.float32), others], axis=0)
    chosen = live_slots(lengths_ref[...], 0, every.shape[0]).astype(jnp.bfloat16)
    out_ref[...] = lax.dot_general(
        chosen, every.astype(jnp.bfloat16), (((0,), (0,)), ((), ())),
        preferred_element_type=jnp.float32,
    ).astype(jnp.bfloat16)


def column_scratch(acts, weights):
    depth = acts.shape[0] * acts.shape[2]
    return [
        pltpu.VMEM((weights[0].shape[0] * len(weights), depth), jnp.bfloat16),
        pltpu.SemaphoreType.DMA((4, len(weights))),
    ]


def finish(starts, acts, weights, copies):
    wide = weights[0].shape[0] * len(weights)
    return pl.pallas_call(
        finish_kernel,
        out_shape=pltpu.HBM((copies, acts.shape[1], wide), jnp.bfloat16),
        in_specs=[SMEM, VMEM] + [ANY] * len(weights),
        out_specs=VMEM,
        scratch_shapes=column_scratch(acts, weights),
        cost_estimate=COST,
        compiler_params=LIMIT,
        name="finish_0",
    )(starts, acts, *weights)


def place(starts, acts, lengths_row, others, weights):
    wide = weights[0].shape[0] * len(weights)
    return pl.pallas_call(
        place_kernel,
        out_shape=pltpu.HBM((lengths_row.shape[1], wide), jnp.bfloat16),
        in_specs=[SMEM] + [VMEM] * 3 + [ANY] * len(weights),
        out_specs=VMEM,
        scratch_shapes=column_scratch(acts, weights),
        cost_estimate=COST,
        compiler_params=LIMIT,
        name="finish_1",
    )(starts, acts, lengths_row, others, *weights)


def spread(value):
    count = lax.axis_size(CHIPS)
    copies = jnp.broadcast_to(value[None], (count,) + value.shape)
    return lax.all_to_all(copies, CHIPS, 0, 0)


def in_order(own, peer, core):
    return jnp.concatenate(
        [jnp.where(core == 0, own, peer), jnp.where(core == 0, peer, own)], axis=0
    )


def beyond_slots(
    tokens, lengths_row, norm_gain, weights, w_out, decay_base, rate_base, group_gain, state
):
    core = lax.axis_index("c")
    count, feats = tokens.shape
    rows = count - SLOTS
    heads, head = state.shape[2], state.shape[-1]
    n_x, n_tp = lax.axis_size("x"), lax.axis_size(TP)
    chosen = live_slots(lengths_row, SLOTS, rows)
    live = jnp.sum((lengths_row > STEP).astype(jnp.float32))
    active = jnp.arange(rows) + SLOTS < live
    mine = jnp.dot(chosen.astype(jnp.bfloat16), tokens, preferred_element_type=jnp.float32)
    mine = mine.astype(jnp.bfloat16)
    held = jnp.argmax(chosen, axis=1)
    out_own = w_out.swapaxes(1, 2)
    out_peer = lax.ppermute(out_own, "c", PAIR)

    def block(natural, layer_parts):
        pairs, outs, gain_in, base, rate_b, gain, state_l = layer_parts
        joined = jnp.concatenate(
            [in_order(pairs[2 * m], pairs[2 * m + 1], core) for m in range(6)], axis=0
        )
        values = natural.astype(jnp.float32)
        factor = lax.rsqrt(jnp.mean(values * values, axis=1, keepdims=True) + RMS_EPS)
        normed = (values * factor * gain_in).astype(jnp.bfloat16)
        projected = lax.dot_general(
            normed, joined, ROWS_BY_ROWS, preferred_element_type=jnp.float32
        ).astype(jnp.bfloat16)
        arrived = lax.all_to_all(projected.reshape(n_x, rows, -1), "x", 0, 0)
        arrived = arrived.transpose(1, 0, 2).astype(jnp.float32)
        recept, key, value, decay_pre, rate_pre, gate_pre = [
            arrived[:, :, m * head : (m + 1) * head] for m in range(6)
        ]
        base, rate_b, gain = [part.reshape(heads, head) for part in (base, rate_b, gain)]
        decay = jnp.exp(-math.exp(-0.5) * jax.nn.sigmoid(base + decay_pre))
        rate = jax.nn.sigmoid(rate_b + rate_pre)
        length = jnp.maximum(jnp.sqrt(jnp.sum(key * key, axis=-1, keepdims=True)), 1e-12)
        unit = key / length
        old = jnp.take(state_l, held, axis=0)
        column = value * length - jnp.sum(old * unit[:, :, None, :], axis=-1)
        dot = jnp.sum(unit * rate * recept, axis=-1, keepdims=True)
        readout = jnp.sum(old * (decay * recept)[:, :, None, :], axis=-1) + column * dot
        centred = readout - jnp.mean(readout, axis=-1, keepdims=True)
        spread_ = jnp.mean(centred * centred, axis=-1, keepdims=True)
        normal = centred * lax.rsqrt(spread_ + GROUP_EPS) * gain * jax.nn.sigmoid(gate_pre)
        mixed = jnp.where(active[:, None, None], normal, 0.0)
        mixed = mixed.astype(jnp.bfloat16).reshape(rows, feats)
        mixed_all = spread(mixed).reshape(n_tp, n_x, rows, feats).transpose(1, 2, 0, 3)
        cols = lax.dot_general(
            mixed_all.reshape(n_x * rows, n_tp * feats), in_order(*outs, core),
            ROWS_BY_ROWS, preferred_element_type=jnp.float32,
        ).astype(jnp.bfloat16)
        blocks = spread(cols.reshape(rows, -1)).reshape(n_tp, n_x, n_x, rows, -1)
        current = blocks.transpose(2, 3, 0, 1, 4)
        here = lax.dynamic_slice_in_dim(current, lax.axis_index("x"), 1, 0)
        here = lax.dynamic_slice_in_dim(here, lax.axis_index(TP), 1, 2).reshape(rows, feats)
        terms = (arrived.reshape(rows, -1), column.reshape(rows, feats), here.astype(jnp.float32))
        return current.reshape(n_x * rows, n_tp * feats), jnp.concatenate(terms, axis=1)

    natural = spread(mine).reshape(n_tp, n_x, rows, feats).transpose(1, 2, 0, 3)
    layers = (weights, (out_own, out_peer), norm_gain, decay_base, rate_base, group_gain, state)
    return lax.scan(block, natural.reshape(n_x * rows, n_tp * feats), layers)[1]


def local(
    tokens, lengths, norm_gain, w_recept, w_key, w_value, w_decay, w_rate, w_gate, w_out,
    decay_base, rate_base, group_gain, state,
):
    core, spot = lax.axis_index("c"), lax.axis_index("x")
    rows, feats = tokens.shape
    n_x, n_tp, n_chips = lax.axis_size("x"), lax.axis_size(TP), lax.axis_size(CHIPS)
    starts = []
    for k in range(n_x):
        source = (spot + n_x - k) % n_x
        starts += [source * 2 + core, source * 2 + 1 - core]
    starts = jnp.stack(starts).astype(jnp.int32)
    core_at = jnp.reshape(core, (1,)).astype(jnp.int32)
    lengths_row = lengths.reshape(1, rows)

    def along_x(layer, more):
        own = jnp.concatenate([w_out.swapaxes(1, 2)[layer]] + more, axis=1)
        return [own] + [
            lax.ppermute(own, "x", [(i, (i + k) % n_x) for i in range(n_x)])
            for k in range(1, n_x)
        ]

    def over_pair(pieces):
        return [p for piece in pieces for p in (piece, lax.ppermute(piece, "c", PAIR))]

    chosen, count = choose(lengths_row, tokens, SLOTS, n_chips)
    acts = lax.all_to_all(chosen, CHIPS, 0, 0)
    weights = []
    for w in (w_recept, w_key, w_value, w_decay, w_rate, w_gate):
        own = w.swapaxes(1, 2)
        weights += [own, lax.ppermute(own, "c", PAIR)]
    states = [table(layer, SLOTS, lengths, state) for layer in range(2)]
    columns = [over_pair(along_x(0, [count])), over_pair(along_x(1, []))]
    most = most_live(columns[0])
    operands = (
        tokens, lengths_row, norm_gain, weights, w_out, decay_base, rate_base, group_gain, state
    )
    others = lax.cond(
        most[0, 0] > SLOTS,
        beyond_slots,
        lambda *_: jnp.zeros((2, rows - SLOTS, 8 * feats), jnp.float32),
        *operands,
    )
    new_state = None
    for layer in range(2):
        acts = acts.reshape(n_tp, n_x * SLOTS, feats)
        projected = project(layer, core_at, acts, norm_gain, weights, n_x)
        arrived = lax.all_to_all(projected, "x", 0, 0)
        mixed, column_terms = read_out(
            layer, arrived, lengths_row, decay_base, rate_base, group_gain, states[layer], n_tp
        )
        mixed_all = lax.all_to_all(mixed, TP, 0, 0)
        new_state = update(
            layer, lengths, arrived, decay_base, rate_base, column_terms, others, state, new_state
        )
        if layer == 0:
            current = finish(starts, mixed_all, columns[0], n_chips)
            acts = lax.all_to_all(current, CHIPS, 0, 0)
    return place(starts, mixed_all, lengths_row, others, columns[1]), new_state


def solution(mesh):
    finer = Mesh(mesh.devices.reshape(4, 4, mesh.shape["dp"] // 2, 2), ("z", "y", "x", "c"))
    wide = P(None, None, TP + DP)
    in_specs = (
        (P(DP, TP), P(DP), P()) + (wide,) * 7 + (P(None, TP),) * 3 + (P(None, DP, TP, None, None),)
    )
    out_specs = (P(DP, TP), P(None, DP, TP, None, None))
    return jax.shard_map(local, mesh=finer, in_specs=in_specs, out_specs=out_specs, check_vma=False)
```

```python
import functools
import math

import jax
import jax.numpy as jnp
from jax import lax
from jax.experimental import pallas as pl
from jax.experimental.pallas import tpu as pltpu
from jax.sharding import Mesh
from jax.sharding import PartitionSpec as P


STEP = 16
RMS_EPS = 1e-06
GROUP_EPS = 0.00064
TP = ("z", "y")
DP = ("x", "c")
CHIPS = ("z", "y", "x")
PAIR = [(0, 1), (1, 0)]
SLOTS = 24
LANES = 128
ROWS_BY_ROWS = (((1,), (1,)), ((), ()))
ANY = pl.BlockSpec(memory_space=pltpu.HBM)
VMEM = pl.BlockSpec(memory_space=pltpu.VMEM)
SMEM = pl.BlockSpec(memory_space=pltpu.SMEM)


COST = pl.CostEstimate(flops=1 << 31, bytes_accessed=8 << 20, transcendentals=0)
LIMIT = pltpu.CompilerParams(vmem_limit_bytes=24 << 20)


def in_hbm(array):
    return pltpu.with_memory_space_constraint(array, pltpu.HBM)


def live_slots(lengths_row, first, slots):
    live = (lengths_row > STEP).astype(jnp.float32)
    count = live.shape[1]
    before = lax.broadcasted_iota(jnp.int32, (count, count), 0)
    before = before < lax.broadcasted_iota(jnp.int32, (count, count), 1)
    place = jnp.dot(
        jnp.broadcast_to(live, (8, count)), before.astype(jnp.float32),
        preferred_element_type=jnp.float32,
    )[:1]
    wanted = lax.broadcasted_iota(jnp.int32, (slots, count), 0) + first
    return jnp.where((place == wanted.astype(jnp.float32)) & (live > 0), 1.0, 0.0)


def choose_kernel(lengths_ref, tokens_ref, out_ref, count_ref):
    chosen = live_slots(lengths_ref[...], 0, out_ref.shape[1]).astype(jnp.bfloat16)
    rows = jnp.dot(chosen, tokens_ref[...], preferred_element_type=jnp.float32)
    rows = rows.astype(jnp.bfloat16)
    for copy in range(out_ref.shape[0]):
        out_ref[copy] = rows
    live = (lengths_ref[...] > STEP).astype(jnp.float32)
    count = jnp.sum(live, axis=1, keepdims=True)
    count_ref[...] = jnp.broadcast_to(count, count_ref.shape).astype(jnp.bfloat16)


def choose(lengths_row, tokens, slots, copies):
    return pl.pallas_call(
        choose_kernel,
        out_shape=(
            pltpu.HBM((copies, slots, tokens.shape[1]), jnp.bfloat16),
            jax.ShapeDtypeStruct((lengths_row.shape[1], LANES), jnp.bfloat16),
        ),
        in_specs=[VMEM, VMEM],
        out_specs=(VMEM, VMEM),
        compiler_params=LIMIT,
        name="choose",
    )(lengths_row, tokens)


def project_kernel(layer, core_ref, acts_ref, gain_ref, *rest):
    weights, (out_ref, held, sems) = rest[:12], rest[12:]
    blocks, rows, feats = acts_ref.shape
    wide, depth = held.shape
    slim = weights[0].shape[1]
    chunks = sems.shape[0]
    core = core_ref[0]
    copies = []
    for chunk in range(chunks):
        span = pl.ds(chunk * (depth // chunks), depth // chunks)
        for idx, weight in enumerate(weights):
            half = core if idx % 2 == 0 else 1 - core
            start = pl.multiple_of((idx // 2) * 2 * slim + half * slim, slim)
            copy = pltpu.make_async_copy(
                weight.at[layer, :, span], held.at[pl.ds(start, slim), span], sems.at[chunk, idx]
            )
            copy.start()
            copies.append(copy)
    squares = jnp.zeros((rows, feats), jnp.float32)
    for t in range(blocks):
        part = acts_ref[t].astype(jnp.float32)
        squares += part * part
    mean = jnp.sum(squares, axis=1, keepdims=True) / (blocks * feats)
    factor = lax.rsqrt(mean + RMS_EPS)
    result = jnp.zeros((rows, wide), jnp.float32)
    for t in range(blocks):
        if t % (blocks // chunks) == 0:
            first = t // (blocks // chunks) * len(weights)
            for copy in copies[first : first + len(weights)]:
                copy.wait()
        span = slice(t * feats, (t + 1) * feats)
        part = acts_ref[t].astype(jnp.float32) * factor * gain_ref[layer : layer + 1, span]
        result += lax.dot_general(
            part.astype(jnp.bfloat16), held[:, span], ROWS_BY_ROWS,
            preferred_element_type=jnp.float32,
        )
    result = result.astype(jnp.bfloat16)
    per = out_ref.shape[1]
    for x in range(out_ref.shape[0]):
        out_ref[x] = result[x * per : (x + 1) * per]


def project(layer, core, acts, gain, weights, n_x):
    rows = acts.shape[1]
    slim, depth = weights[0].shape[1:]
    wide = slim * len(weights)
    return pl.pallas_call(
        functools.partial(project_kernel, layer),
        out_shape=pltpu.HBM((n_x, rows // n_x, wide), jnp.bfloat16),
        in_specs=[SMEM, VMEM, VMEM] + [ANY] * len(weights),
        out_specs=VMEM,
        scratch_shapes=[
            pltpu.VMEM((wide, depth), jnp.bfloat16),
            pltpu.SemaphoreType.DMA((1, len(weights))),
        ],
        cost_estimate=COST,
        compiler_params=LIMIT,
    )(core, acts, gain, *weights)


def table_kernel(layer, lengths_ref, state_ref, out_ref, held, sems):
    chunks = out_ref.shape[0]
    slots, heads, head, _ = held.shape
    per = slots // chunks

    def fetch(sequence, slot):
        return pltpu.make_async_copy(
            state_ref.at[layer, sequence], held.at[slot], sems.at[slot]
        )

    def start(sequence, slot):
        live = lengths_ref[sequence] > STEP

        @pl.when(live & (slot < slots))
        def _():
            fetch(sequence, slot).start()

        return slot + live.astype(jnp.int32)

    count = lax.fori_loop(0, state_ref.shape[1], start, jnp.int32(0))
    for idx in range(chunks):
        for slot in range(idx * per, (idx + 1) * per):

            @pl.when(slot < count)
            def _():
                fetch(0, slot).wait()

            @pl.when(slot >= count)
            def _():
                held[slot] = jnp.zeros_like(held[slot])

        parts = [held[idx * per + k].reshape(heads * head, head) for k in range(per)]
        out_ref[idx] = jnp.concatenate(parts, axis=1).astype(jnp.bfloat16)


def table(layer, slots, lengths, state):
    _, _, heads, head, _ = state.shape
    per = 4
    return pl.pallas_call(
        functools.partial(table_kernel, layer),
        out_shape=pltpu.VMEM((slots // per, heads * head, per * head), jnp.bfloat16),
        in_specs=[SMEM, ANY],
        out_specs=VMEM,
        scratch_shapes=[
            pltpu.VMEM((slots, heads, head, head), jnp.float32),
            pltpu.SemaphoreType.DMA((slots,)),
        ],
        cost_estimate=COST,
        compiler_params=LIMIT,
    )(lengths, in_hbm(state))


def vectors_of(layer, block, lanes, decay_ref, rate_ref):
    head = block.shape[1] // 6
    recept, key, value, decay_pre, rate_pre, gate_pre = [
        block[:, m * head : (m + 1) * head] for m in range(6)
    ]
    decay_in = decay_ref[layer : layer + 1, lanes] + decay_pre
    decay = jnp.exp(-math.exp(-0.5) * jax.nn.sigmoid(decay_in))
    rate = jax.nn.sigmoid(rate_ref[layer : layer + 1, lanes] + rate_pre)
    length = jnp.maximum(jnp.sqrt(jnp.sum(key * key, axis=1, keepdims=True)), 1e-12)
    unit = key / length
    return recept, value, gate_pre, decay, length, unit, unit * rate


def readout_kernel(
    layer, arrived_ref, lengths_ref, decay_ref, rate_ref, gain_ref, table_ref, mixed_ref, column_ref
):
    heads, count, wide = arrived_ref.shape
    head = wide // 6
    units, reads, kept = [], [], []
    for h in range(heads):
        lanes = slice(h * head, (h + 1) * head)
        block = arrived_ref[h].astype(jnp.float32)
        recept, value, gate_pre, decay, length, unit, learned = vectors_of(
            layer, block, lanes, decay_ref, rate_ref
        )
        units.append(unit)
        reads.append(decay * recept)
        dot = jnp.sum(learned * recept, axis=1, keepdims=True)
        kept.append((value * length, dot, jax.nn.sigmoid(gate_pre)))
    per = table_ref.shape[2] // head
    group = 8
    shape = (2 * heads * group, per * head)
    row = lax.broadcasted_iota(jnp.int32, shape, 0) % group
    spot = lax.broadcasted_iota(jnp.int32, shape, 1) // head
    lane_head = lax.broadcasted_iota(jnp.int32, (group, heads * head), 1) // head
    summed = ([], [])
    for g in range(count // group):
        rows = slice(g * group, (g + 1) * group)
        left = jnp.concatenate(
            [jnp.concatenate([v[rows]] * per, axis=1) for v in units + reads], axis=0
        )
        product = jnp.zeros((shape[0], heads * head), jnp.float32)
        for part in range(group // per):
            chosen = jnp.where(row == spot + part * per, left, 0.0).astype(jnp.bfloat16)
            product += lax.dot_general(
                chosen, table_ref[g * (group // per) + part], ROWS_BY_ROWS,
                preferred_element_type=jnp.float32,
            )
        for kind in range(2):
            base = kind * heads * group
            total = product[base : base + group]
            for h in range(1, heads):
                piece = product[base + h * group : base + (h + 1) * group]
                total = jnp.where(lane_head == h, piece, total)
            summed[kind].append(total)
    by_unit, by_read = [jnp.concatenate(parts, axis=0) for parts in summed]
    live = jnp.sum((lengths_ref[...] > STEP).astype(jnp.float32), axis=1, keepdims=True)
    active = lax.broadcasted_iota(jnp.int32, (count, 1), 0).astype(jnp.float32) < live
    mixed = []
    for h in range(heads):
        lanes = slice(h * head, (h + 1) * head)
        scaled, dot, gate = kept[h]
        column = scaled - by_unit[:, lanes]
        column_ref[:, lanes] = column
        readout = by_read[:, lanes] + column * dot
        centred = readout - jnp.mean(readout, axis=1, keepdims=True)
        spread_ = jnp.mean(centred * centred, axis=1, keepdims=True)
        normal = centred * lax.rsqrt(spread_ + GROUP_EPS)
        normal = normal * gain_ref[layer : layer + 1, lanes] * gate
        mixed.append(jnp.where(active, normal, 0.0))
    rows = jnp.concatenate(mixed, axis=1).astype(jnp.bfloat16)
    for t in range(mixed_ref.shape[0]):
        mixed_ref[t] = rows


def read_out(layer, arrived, lengths, decay_base, rate_base, group_gain, states, copies):
    heads, count, wide = arrived.shape
    feats = heads * wide // 6
    return pl.pallas_call(
        functools.partial(readout_kernel, layer),
        out_shape=(
            pltpu.HBM((copies, count, feats), jnp.bfloat16),
            pltpu.VMEM((count, feats), jnp.float32),
        ),
        in_specs=[VMEM] * 6,
        out_specs=(VMEM, VMEM),
        cost_estimate=COST,
        compiler_params=LIMIT,
    )(arrived, lengths, decay_base, rate_base, group_gain, states)


def in_two(value):
    high = value.astype(jnp.bfloat16)
    return high, (value - high.astype(jnp.float32)).astype(jnp.bfloat16)


def update_kernel(
    layer, lengths_ref, arrived_ref, decay_ref, rate_ref, column_ref, others_ref, state_ref, *rest
):
    out_ref, held, rows_ref, columns_ref, in_sems, out_sems = rest[-6:]
    count, heads, head, _ = held.shape
    chunks = in_sems.shape[0]
    per = count // chunks

    def fetch(idx):
        span = pl.ds(idx * per, per)
        return pltpu.make_async_copy(state_ref.at[layer, span], held.at[span], in_sems.at[idx])

    def put(idx):
        span = pl.ds(idx * per, per)
        return pltpu.make_async_copy(held.at[span], out_ref.at[layer, span], out_sems.at[idx])

    for idx in range(chunks):
        fetch(idx).start()
    for h in range(heads):
        lanes = slice(h * head, (h + 1) * head)
        block = jnp.concatenate(
            [
                arrived_ref[h].astype(jnp.float32),
                others_ref[layer, :, h * 6 * head : (h + 1) * 6 * head],
            ],
            axis=0,
        )
        _, _, _, decay, _, _, learned = vectors_of(layer, block, lanes, decay_ref, rate_ref)
        rows_ref[:, h, :] = decay
        rows_ref[:, heads + h, :] = learned
    slots = column_ref.shape[0]
    columns_ref[:slots] = column_ref[...]
    columns_ref[slots:] = others_ref[layer, :, heads * 6 * head : heads * 7 * head]
    own = lax.broadcasted_iota(jnp.int32, (heads, heads * head), 0)
    own = own == lax.broadcasted_iota(jnp.int32, (heads, heads * head), 1) // head

    def advance(r, slot):
        live = lengths_ref[r] > STEP

        @pl.when(live)
        def _():
            high, low = in_two(jnp.where(own, columns_ref[pl.ds(slot, 1), :], 0.0))
            vectors = rows_ref[slot]
            right_high, right_low = in_two(vectors[heads:])
            added = lax.dot_general(
                jnp.concatenate([high, high, low], axis=0),
                jnp.concatenate([right_high, right_low, right_high], axis=0),
                (((0,), (0,)), ((), ())), preferred_element_type=jnp.float32,
            )
            for h in range(heads):
                new = held[r, h] * vectors[h : h + 1] + added[h * head : (h + 1) * head]
                held[r, h] = new

        return slot + live.astype(jnp.int32)

    slot = jnp.int32(0)
    for idx in range(chunks):
        fetch(idx).wait()
        slot = lax.fori_loop(idx * per, (idx + 1) * per, advance, slot)
        if idx:
            put(idx - 1).start()
    put(chunks - 1).start()
    for idx in range(chunks):
        put(idx).wait()


def update(layer, lengths, arrived, decay_base, rate_base, column, others, state, earlier):
    _, count, heads, head, _ = state.shape
    more = () if earlier is None else (earlier,)
    return pl.pallas_call(
        functools.partial(update_kernel, layer),
        out_shape=pltpu.HBM(state.shape, state.dtype),
        in_specs=[SMEM] + [VMEM] * 5 + [ANY] + [ANY] * len(more),
        out_specs=ANY,
        scratch_shapes=[
            pltpu.VMEM((count, heads, head, head), jnp.float32),
            pltpu.VMEM((count, 2 * heads, head), jnp.float32),
            pltpu.VMEM((count, heads * head), jnp.float32),
            pltpu.SemaphoreType.DMA((8,)),
            pltpu.SemaphoreType.DMA((8,)),
        ],
        input_output_aliases={7: 0} if more else {},
        cost_estimate=COST,
        compiler_params=LIMIT,
    )(lengths, arrived, decay_base, rate_base, column, others, in_hbm(state), *map(in_hbm, more))


def columns_of(acts_ref, weight):
    blocks, rows, feats = acts_ref.shape
    result = jnp.zeros((rows, weight.shape[0]), jnp.float32)
    for t in range(blocks):
        result += lax.dot_general(
            acts_ref[t], weight[:, t * feats : (t + 1) * feats], ROWS_BY_ROWS,
            preferred_element_type=jnp.float32,
        )
    return result


def all_columns(starts_ref, acts_ref, weights):
    slim = weights[0].shape[0]
    wide = slim * len(weights)
    pieces = [columns_of(acts_ref, weight) for weight in weights]
    result = jnp.concatenate(pieces, axis=1).astype(jnp.bfloat16)
    source = lax.broadcasted_iota(jnp.int32, (wide, wide), 0)
    target = source % slim
    for idx in range(len(weights)):
        target += jnp.where(source // slim == idx, starts_ref[idx] * slim, 0)
    moved = target == lax.broadcasted_iota(jnp.int32, (wide, wide), 1)
    return jnp.dot(
        result, jnp.where(moved, 1.0, 0.0).astype(jnp.bfloat16),
        preferred_element_type=jnp.float32,
    )


def finish_kernel(starts_ref, acts_ref, *refs):
    weights, (out_ref, most_ref) = refs[:8], refs[8:]
    depth = acts_ref.shape[0] * acts_ref.shape[2]
    result = all_columns(starts_ref, acts_ref, weights).astype(jnp.bfloat16)
    for copy in range(out_ref.shape[0]):
        out_ref[copy] = result
    most = weights[0][:, depth:]
    for weight in weights[1:]:
        most = jnp.maximum(most, weight[:, depth:])
    most_ref[...] = jnp.max(most.astype(jnp.float32), axis=0, keepdims=True)


def place_kernel(starts_ref, acts_ref, lengths_ref, others_ref, *refs):
    weights, out_ref = refs[:8], refs[8]
    result = all_columns(starts_ref, acts_ref, weights)
    others = others_ref[1, :, others_ref.shape[2] - result.shape[1] :]
    every = jnp.concatenate([result, others], axis=0).astype(jnp.bfloat16)
    chosen = live_slots(lengths_ref[...], 0, every.shape[0]).astype(jnp.bfloat16)
    out_ref[...] = lax.dot_general(
        chosen, every, (((0,), (0,)), ((), ())), preferred_element_type=jnp.float32
    ).astype(jnp.bfloat16)


def finish(starts, acts, weights, copies):
    wide = weights[0].shape[0] * len(weights)
    return pl.pallas_call(
        finish_kernel,
        out_shape=(
            pltpu.HBM((copies, acts.shape[1], wide), jnp.bfloat16),
            jax.ShapeDtypeStruct((1, LANES), jnp.float32),
        ),
        in_specs=[SMEM, VMEM] + [VMEM] * len(weights),
        out_specs=(VMEM, VMEM),
        cost_estimate=COST,
        compiler_params=LIMIT,
        name="finish_0",
    )(starts, acts, *weights)


def place(starts, acts, lengths_row, others, weights):
    wide = weights[0].shape[0] * len(weights)
    return pl.pallas_call(
        place_kernel,
        out_shape=pltpu.HBM((lengths_row.shape[1], wide), jnp.bfloat16),
        in_specs=[SMEM] + [VMEM] * (3 + len(weights)),
        out_specs=VMEM,
        cost_estimate=COST,
        compiler_params=LIMIT,
        name="finish_1",
    )(starts, acts, lengths_row, others, *weights)


def spread(value):
    count = lax.axis_size(CHIPS)
    copies = jnp.broadcast_to(value[None], (count,) + value.shape)
    return lax.all_to_all(copies, CHIPS, 0, 0)


def in_order(own, peer, core):
    return jnp.concatenate(
        [jnp.where(core == 0, own, peer), jnp.where(core == 0, peer, own)], axis=0
    )


def beyond_slots(
    tokens, lengths_row, norm_gain, weights, w_out, decay_base, rate_base, group_gain, state
):
    core = lax.axis_index("c")
    count, feats = tokens.shape
    rows = count - SLOTS
    heads, head = state.shape[2], state.shape[-1]
    n_x, n_tp = lax.axis_size("x"), lax.axis_size(TP)
    chosen = live_slots(lengths_row, SLOTS, rows)
    live = jnp.sum((lengths_row > STEP).astype(jnp.float32))
    active = jnp.arange(rows) + SLOTS < live
    mine = jnp.dot(chosen.astype(jnp.bfloat16), tokens, preferred_element_type=jnp.float32)
    mine = mine.astype(jnp.bfloat16)
    held = jnp.argmax(chosen, axis=1)
    out_own = w_out.swapaxes(1, 2)
    out_peer = lax.ppermute(out_own, "c", PAIR)

    def block(natural, layer_parts):
        pairs, outs, gain_in, base, rate_b, gain, state_l = layer_parts
        joined = jnp.concatenate(
            [in_order(pairs[2 * m], pairs[2 * m + 1], core) for m in range(6)], axis=0
        )
        values = natural.astype(jnp.float32)
        factor = lax.rsqrt(jnp.mean(values * values, axis=1, keepdims=True) + RMS_EPS)
        normed = (values * factor * gain_in).astype(jnp.bfloat16)
        projected = lax.dot_general(
            normed, joined, ROWS_BY_ROWS, preferred_element_type=jnp.float32
        ).astype(jnp.bfloat16)
        arrived = lax.all_to_all(projected.reshape(n_x, rows, -1), "x", 0, 0)
        arrived = arrived.transpose(1, 0, 2).astype(jnp.float32)
        recept, key, value, decay_pre, rate_pre, gate_pre = [
            arrived[:, :, m * head : (m + 1) * head] for m in range(6)
        ]
        base, rate_b, gain = [part.reshape(heads, head) for part in (base, rate_b, gain)]
        decay = jnp.exp(-math.exp(-0.5) * jax.nn.sigmoid(base + decay_pre))
        rate = jax.nn.sigmoid(rate_b + rate_pre)
        length = jnp.maximum(jnp.sqrt(jnp.sum(key * key, axis=-1, keepdims=True)), 1e-12)
        unit = key / length
        old = jnp.take(state_l, held, axis=0)
        column = value * length - jnp.sum(old * unit[:, :, None, :], axis=-1)
        dot = jnp.sum(unit * rate * recept, axis=-1, keepdims=True)
        readout = jnp.sum(old * (decay * recept)[:, :, None, :], axis=-1) + column * dot
        centred = readout - jnp.mean(readout, axis=-1, keepdims=True)
        spread_ = jnp.mean(centred * centred, axis=-1, keepdims=True)
        normal = centred * lax.rsqrt(spread_ + GROUP_EPS) * gain * jax.nn.sigmoid(gate_pre)
        mixed = jnp.where(active[:, None, None], normal, 0.0)
        mixed = mixed.astype(jnp.bfloat16).reshape(rows, feats)
        mixed_all = spread(mixed).reshape(n_tp, n_x, rows, feats).transpose(1, 2, 0, 3)
        cols = lax.dot_general(
            mixed_all.reshape(n_x * rows, n_tp * feats), in_order(*outs, core),
            ROWS_BY_ROWS, preferred_element_type=jnp.float32,
        ).astype(jnp.bfloat16)
        blocks = spread(cols.reshape(rows, -1)).reshape(n_tp, n_x, n_x, rows, -1)
        current = blocks.transpose(2, 3, 0, 1, 4)
        here = lax.dynamic_slice_in_dim(current, lax.axis_index("x"), 1, 0)
        here = lax.dynamic_slice_in_dim(here, lax.axis_index(TP), 1, 2).reshape(rows, feats)
        terms = (arrived.reshape(rows, -1), column.reshape(rows, feats), here.astype(jnp.float32))
        return current.reshape(n_x * rows, n_tp * feats), jnp.concatenate(terms, axis=1)

    natural = spread(mine).reshape(n_tp, n_x, rows, feats).transpose(1, 2, 0, 3)
    layers = (weights, (out_own, out_peer), norm_gain, decay_base, rate_base, group_gain, state)
    return lax.scan(block, natural.reshape(n_x * rows, n_tp * feats), layers)[1]


def local(
    tokens, lengths, norm_gain, w_recept, w_key, w_value, w_decay, w_rate, w_gate, w_out,
    decay_base, rate_base, group_gain, state,
):
    core, spot = lax.axis_index("c"), lax.axis_index("x")
    rows, feats = tokens.shape
    n_x, n_tp, n_chips = lax.axis_size("x"), lax.axis_size(TP), lax.axis_size(CHIPS)
    starts = []
    for k in range(n_x):
        source = (spot + n_x - k) % n_x
        starts += [source * 2 + core, source * 2 + 1 - core]
    starts = jnp.stack(starts).astype(jnp.int32)
    core_at = jnp.reshape(core, (1,)).astype(jnp.int32)
    lengths_row = lengths.reshape(1, rows)

    def along_x(layer, more):
        own = jnp.concatenate([w_out.swapaxes(1, 2)[layer]] + more, axis=1)
        return [own] + [
            lax.ppermute(own, "x", [(i, (i + k) % n_x) for i in range(n_x)])
            for k in range(1, n_x)
        ]

    def over_pair(pieces):
        return [p for piece in pieces for p in (piece, lax.ppermute(piece, "c", PAIR))]

    chosen, count = choose(lengths_row, tokens, SLOTS, n_chips)
    acts = lax.all_to_all(chosen, CHIPS, 0, 0)
    weights = []
    for w in (w_recept, w_key, w_value, w_decay, w_rate, w_gate):
        own = w.swapaxes(1, 2)
        weights += [own, lax.ppermute(own, "c", PAIR)]
    states = [table(layer, SLOTS, lengths, state) for layer in range(2)]
    columns = [over_pair(along_x(0, [count])), over_pair(along_x(1, []))]
    operands = (
        tokens, lengths_row, norm_gain, weights, w_out, decay_base, rate_base, group_gain, state
    )
    new_state = None
    for layer in range(2):
        acts = acts.reshape(n_tp, n_x * SLOTS, feats)
        projected = project(layer, core_at, acts, norm_gain, weights, n_x)
        arrived = lax.all_to_all(projected, "x", 0, 0)
        mixed, column_terms = read_out(
            layer, arrived, lengths_row, decay_base, rate_base, group_gain, states[layer], n_tp
        )
        mixed_all = lax.all_to_all(mixed, TP, 0, 0)
        if layer == 0:
            current, most = finish(starts, mixed_all, columns[0], n_chips)
            others = lax.cond(
                most[0, 0] > SLOTS,
                beyond_slots,
                lambda *_: jnp.zeros((2, rows - SLOTS, 8 * feats), jnp.float32),
                *operands,
            )
            acts = lax.all_to_all(current, CHIPS, 0, 0)
        new_state = update(
            layer, lengths, arrived, decay_base, rate_base, column_terms, others, state, new_state
        )
    return place(starts, mixed_all, lengths_row, others, columns[1]), new_state


def solution(mesh):
    finer = Mesh(mesh.devices.reshape(4, 4, mesh.shape["dp"] // 2, 2), ("z", "y", "x", "c"))
    wide = P(None, None, TP + DP)
    in_specs = (
        (P(DP, TP), P(DP), P()) + (wide,) * 7 + (P(None, TP),) * 3 + (P(None, DP, TP, None, None),)
    )
    out_specs = (P(DP, TP), P(None, DP, TP, None, None))
    return jax.shard_map(local, mesh=finer, in_specs=in_specs, out_specs=out_specs, check_vma=False)
```

```python
import functools
import math

import jax
import jax.numpy as jnp
from jax import lax
from jax.experimental import pallas as pl
from jax.experimental.pallas import tpu as pltpu
from jax.sharding import Mesh
from jax.sharding import PartitionSpec as P


STEP = 16
RMS_EPS = 1e-06
GROUP_EPS = 0.00064
TP = ("z", "y")
DP = ("x", "c")
CHIPS = ("z", "y", "x")
PAIR = [(0, 1), (1, 0)]
SLOTS = 24
LANES = 128
ROWS_BY_ROWS = (((1,), (1,)), ((), ()))
ANY = pl.BlockSpec(memory_space=pltpu.HBM)
VMEM = pl.BlockSpec(memory_space=pltpu.VMEM)
SMEM = pl.BlockSpec(memory_space=pltpu.SMEM)


COST = pl.CostEstimate(flops=1 << 31, bytes_accessed=8 << 20, transcendentals=0)
LIMIT = pltpu.CompilerParams(vmem_limit_bytes=24 << 20)


def in_hbm(array):
    return pltpu.with_memory_space_constraint(array, pltpu.HBM)


def live_slots(lengths_row, first, slots):
    live = (lengths_row > STEP).astype(jnp.float32)
    count = live.shape[1]
    before = lax.broadcasted_iota(jnp.int32, (count, count), 0)
    before = before < lax.broadcasted_iota(jnp.int32, (count, count), 1)
    place = jnp.dot(
        jnp.broadcast_to(live, (8, count)), before.astype(jnp.float32),
        preferred_element_type=jnp.float32,
    )[:1]
    wanted = lax.broadcasted_iota(jnp.int32, (slots, count), 0) + first
    return jnp.where((place == wanted.astype(jnp.float32)) & (live > 0), 1.0, 0.0)


def choose_kernel(lengths_ref, tokens_ref, out_ref, count_ref):
    chosen = live_slots(lengths_ref[...], 0, out_ref.shape[1]).astype(jnp.bfloat16)
    rows = jnp.dot(chosen, tokens_ref[...], preferred_element_type=jnp.float32)
    rows = rows.astype(jnp.bfloat16)
    for copy in range(out_ref.shape[0]):
        out_ref[copy] = rows
    live = (lengths_ref[...] > STEP).astype(jnp.float32)
    count = jnp.sum(live, axis=1, keepdims=True)
    count_ref[...] = jnp.broadcast_to(count, count_ref.shape).astype(jnp.bfloat16)


def choose(lengths_row, tokens, slots, copies):
    return pl.pallas_call(
        choose_kernel,
        out_shape=(
            pltpu.HBM((copies, slots, tokens.shape[1]), jnp.bfloat16),
            jax.ShapeDtypeStruct((lengths_row.shape[1], LANES), jnp.bfloat16),
        ),
        in_specs=[VMEM, VMEM],
        out_specs=(VMEM, VMEM),
        compiler_params=LIMIT,
        name="choose",
    )(lengths_row, tokens)


def project_kernel(layer, core_ref, acts_ref, gain_ref, *rest):
    weights, (out_ref, held, sems) = rest[:12], rest[12:]
    blocks, rows, feats = acts_ref.shape
    wide, depth = held.shape
    slim = weights[0].shape[1]
    chunks = sems.shape[0]
    core = core_ref[0]
    copies = []
    for chunk in range(chunks):
        span = pl.ds(chunk * (depth // chunks), depth // chunks)
        for idx, weight in enumerate(weights):
            half = core if idx % 2 == 0 else 1 - core
            start = pl.multiple_of((idx // 2) * 2 * slim + half * slim, slim)
            copy = pltpu.make_async_copy(
                weight.at[layer, :, span], held.at[pl.ds(start, slim), span], sems.at[chunk, idx]
            )
            copy.start()
            copies.append(copy)
    squares = jnp.zeros((rows, feats), jnp.float32)
    for t in range(blocks):
        part = acts_ref[t].astype(jnp.float32)
        squares += part * part
    mean = jnp.sum(squares, axis=1, keepdims=True) / (blocks * feats)
    factor = lax.rsqrt(mean + RMS_EPS)
    result = jnp.zeros((rows, wide), jnp.float32)
    for t in range(blocks):
        if t % (blocks // chunks) == 0:
            first = t // (blocks // chunks) * len(weights)
            for copy in copies[first : first + len(weights)]:
                copy.wait()
        span = slice(t * feats, (t + 1) * feats)
        part = acts_ref[t].astype(jnp.float32) * factor * gain_ref[layer : layer + 1, span]
        result += lax.dot_general(
            part.astype(jnp.bfloat16), held[:, span], ROWS_BY_ROWS,
            preferred_element_type=jnp.float32,
        )
    result = result.astype(jnp.bfloat16)
    per = out_ref.shape[1]
    for x in range(out_ref.shape[0]):
        out_ref[x] = result[x * per : (x + 1) * per]


def project(layer, core, acts, gain, weights, n_x):
    rows = acts.shape[1]
    slim, depth = weights[0].shape[1:]
    wide = slim * len(weights)
    return pl.pallas_call(
        functools.partial(project_kernel, layer),
        out_shape=pltpu.HBM((n_x, rows // n_x, wide), jnp.bfloat16),
        in_specs=[SMEM, VMEM, VMEM] + [ANY] * len(weights),
        out_specs=VMEM,
        scratch_shapes=[
            pltpu.VMEM((wide, depth), jnp.bfloat16),
            pltpu.SemaphoreType.DMA((1, len(weights))),
        ],
        cost_estimate=COST,
        compiler_params=LIMIT,
    )(core, acts, gain, *weights)


def table_kernel(layer, lengths_ref, state_ref, out_ref, held, sems):
    chunks = out_ref.shape[0]
    slots, heads, head, _ = held.shape
    per = slots // chunks

    def fetch(sequence, slot):
        return pltpu.make_async_copy(
            state_ref.at[layer, sequence], held.at[slot], sems.at[slot]
        )

    def start(sequence, slot):
        live = lengths_ref[sequence] > STEP

        @pl.when(live & (slot < slots))
        def _():
            fetch(sequence, slot).start()

        return slot + live.astype(jnp.int32)

    count = lax.fori_loop(0, state_ref.shape[1], start, jnp.int32(0))
    for idx in range(chunks):
        for slot in range(idx * per, (idx + 1) * per):

            @pl.when(slot < count)
            def _():
                fetch(0, slot).wait()

            @pl.when(slot >= count)
            def _():
                held[slot] = jnp.zeros_like(held[slot])

        parts = [held[idx * per + k].reshape(heads * head, head) for k in range(per)]
        out_ref[idx] = jnp.concatenate(parts, axis=1).astype(jnp.bfloat16)


def table(layer, slots, lengths, state):
    _, _, heads, head, _ = state.shape
    per = 4
    return pl.pallas_call(
        functools.partial(table_kernel, layer),
        out_shape=pltpu.VMEM((slots // per, heads * head, per * head), jnp.bfloat16),
        in_specs=[SMEM, ANY],
        out_specs=VMEM,
        scratch_shapes=[
            pltpu.VMEM((slots, heads, head, head), jnp.float32),
            pltpu.SemaphoreType.DMA((slots,)),
        ],
        cost_estimate=COST,
        compiler_params=LIMIT,
    )(lengths, in_hbm(state))


def vectors_of(layer, block, lanes, decay_ref, rate_ref):
    head = block.shape[1] // 6
    recept, key, value, decay_pre, rate_pre, gate_pre = [
        block[:, m * head : (m + 1) * head] for m in range(6)
    ]
    decay_in = decay_ref[layer : layer + 1, lanes] + decay_pre
    decay = jnp.exp(-math.exp(-0.5) * jax.nn.sigmoid(decay_in))
    rate = jax.nn.sigmoid(rate_ref[layer : layer + 1, lanes] + rate_pre)
    length = jnp.maximum(jnp.sqrt(jnp.sum(key * key, axis=1, keepdims=True)), 1e-12)
    unit = key / length
    return recept, value, gate_pre, decay, length, unit, unit * rate


def readout_kernel(
    layer, arrived_ref, lengths_ref, decay_ref, rate_ref, gain_ref, table_ref, mixed_ref, column_ref
):
    heads, count, wide = arrived_ref.shape
    head = wide // 6
    units, reads, kept = [], [], []
    for h in range(heads):
        lanes = slice(h * head, (h + 1) * head)
        block = arrived_ref[h].astype(jnp.float32)
        recept, value, gate_pre, decay, length, unit, learned = vectors_of(
            layer, block, lanes, decay_ref, rate_ref
        )
        units.append(unit)
        reads.append(decay * recept)
        dot = jnp.sum(learned * recept, axis=1, keepdims=True)
        kept.append((value * length, dot, jax.nn.sigmoid(gate_pre)))
    per = table_ref.shape[2] // head
    group = 8
    shape = (2 * heads * group, per * head)
    row = lax.broadcasted_iota(jnp.int32, shape, 0) % group
    spot = lax.broadcasted_iota(jnp.int32, shape, 1) // head
    lane_head = lax.broadcasted_iota(jnp.int32, (group, heads * head), 1) // head
    summed = ([], [])
    for g in range(count // group):
        rows = slice(g * group, (g + 1) * group)
        left = jnp.concatenate(
            [jnp.concatenate([v[rows]] * per, axis=1) for v in units + reads], axis=0
        )
        product = jnp.zeros((shape[0], heads * head), jnp.float32)
        for part in range(group // per):
            chosen = jnp.where(row == spot + part * per, left, 0.0).astype(jnp.bfloat16)
            product += lax.dot_general(
                chosen, table_ref[g * (group // per) + part], ROWS_BY_ROWS,
                preferred_element_type=jnp.float32,
            )
        for kind in range(2):
            base = kind * heads * group
            total = product[base : base + group]
            for h in range(1, heads):
                piece = product[base + h * group : base + (h + 1) * group]
                total = jnp.where(lane_head == h, piece, total)
            summed[kind].append(total)
    by_unit, by_read = [jnp.concatenate(parts, axis=0) for parts in summed]
    live = jnp.sum((lengths_ref[...] > STEP).astype(jnp.float32), axis=1, keepdims=True)
    active = lax.broadcasted_iota(jnp.int32, (count, 1), 0).astype(jnp.float32) < live
    mixed = []
    for h in range(heads):
        lanes = slice(h * head, (h + 1) * head)
        scaled, dot, gate = kept[h]
        column = scaled - by_unit[:, lanes]
        column_ref[:, lanes] = column
        readout = by_read[:, lanes] + column * dot
        centred = readout - jnp.mean(readout, axis=1, keepdims=True)
        spread_ = jnp.mean(centred * centred, axis=1, keepdims=True)
        normal = centred * lax.rsqrt(spread_ + GROUP_EPS)
        normal = normal * gain_ref[layer : layer + 1, lanes] * gate
        mixed.append(jnp.where(active, normal, 0.0))
    rows = jnp.concatenate(mixed, axis=1).astype(jnp.bfloat16)
    for t in range(mixed_ref.shape[0]):
        mixed_ref[t] = rows


def read_out(layer, arrived, lengths, decay_base, rate_base, group_gain, states, copies):
    heads, count, wide = arrived.shape
    feats = heads * wide // 6
    return pl.pallas_call(
        functools.partial(readout_kernel, layer),
        out_shape=(
            pltpu.HBM((copies, count, feats), jnp.bfloat16),
            pltpu.VMEM((count, feats), jnp.float32),
        ),
        in_specs=[VMEM] * 6,
        out_specs=(VMEM, VMEM),
        cost_estimate=COST,
        compiler_params=LIMIT,
    )(arrived, lengths, decay_base, rate_base, group_gain, states)


def in_two(value):
    high = value.astype(jnp.bfloat16)
    return high, (value - high.astype(jnp.float32)).astype(jnp.bfloat16)


def update_kernel(
    layer, lengths_ref, arrived_ref, decay_ref, rate_ref, column_ref, others_ref, state_ref, *rest
):
    out_ref, held, rows_ref, columns_ref, in_sems, out_sems = rest[-6:]
    count, heads, head, _ = held.shape
    chunks = in_sems.shape[0]
    per = count // chunks

    def fetch(idx):
        span = pl.ds(idx * per, per)
        return pltpu.make_async_copy(state_ref.at[layer, span], held.at[span], in_sems.at[idx])

    def put(idx):
        span = pl.ds(idx * per, per)
        return pltpu.make_async_copy(held.at[span], out_ref.at[layer, span], out_sems.at[idx])

    for idx in range(chunks):
        fetch(idx).start()
    for h in range(heads):
        lanes = slice(h * head, (h + 1) * head)
        block = jnp.concatenate(
            [
                arrived_ref[h].astype(jnp.float32),
                others_ref[layer, :, h * 6 * head : (h + 1) * 6 * head],
            ],
            axis=0,
        )
        _, _, _, decay, _, _, learned = vectors_of(layer, block, lanes, decay_ref, rate_ref)
        rows_ref[:, h, :] = decay
        rows_ref[:, heads + h, :] = learned
    slots = column_ref.shape[0]
    columns_ref[:slots] = column_ref[...]
    columns_ref[slots:] = others_ref[layer, :, heads * 6 * head : heads * 7 * head]
    own = lax.broadcasted_iota(jnp.int32, (heads, heads * head), 0)
    own = own == lax.broadcasted_iota(jnp.int32, (heads, heads * head), 1) // head

    def advance(r, slot):
        live = lengths_ref[r] > STEP

        @pl.when(live)
        def _():
            high, low = in_two(jnp.where(own, columns_ref[pl.ds(slot, 1), :], 0.0))
            vectors = rows_ref[slot]
            right_high, right_low = in_two(vectors[heads:])
            added = lax.dot_general(
                jnp.concatenate([high, high, low], axis=0),
                jnp.concatenate([right_high, right_low, right_high], axis=0),
                (((0,), (0,)), ((), ())), preferred_element_type=jnp.float32,
            )
            for h in range(heads):
                new = held[r, h] * vectors[h : h + 1] + added[h * head : (h + 1) * head]
                held[r, h] = new

        return slot + live.astype(jnp.int32)

    slot = jnp.int32(0)
    for idx in range(chunks):
        fetch(idx).wait()
        slot = lax.fori_loop(idx * per, (idx + 1) * per, advance, slot)
        if idx:
            put(idx - 1).start()
    put(chunks - 1).start()
    for idx in range(chunks):
        put(idx).wait()


def update(layer, lengths, arrived, decay_base, rate_base, column, others, state, earlier):
    _, count, heads, head, _ = state.shape
    more = () if earlier is None else (earlier,)
    return pl.pallas_call(
        functools.partial(update_kernel, layer),
        out_shape=pltpu.HBM(state.shape, state.dtype),
        in_specs=[SMEM] + [VMEM] * 5 + [ANY] + [ANY] * len(more),
        out_specs=ANY,
        scratch_shapes=[
            pltpu.VMEM((count, heads, head, head), jnp.float32),
            pltpu.VMEM((count, 2 * heads, head), jnp.float32),
            pltpu.VMEM((count, heads * head), jnp.float32),
            pltpu.SemaphoreType.DMA((8,)),
            pltpu.SemaphoreType.DMA((8,)),
        ],
        input_output_aliases={7: 0} if more else {},
        cost_estimate=COST,
        compiler_params=LIMIT,
    )(lengths, arrived, decay_base, rate_base, column, others, in_hbm(state), *map(in_hbm, more))


def all_columns(starts_ref, acts_ref, weights, turned):
    blocks, rows, feats = acts_ref.shape
    slim = weights[0].shape[0]
    parts = [jnp.zeros((slim, rows), jnp.float32) for _ in weights]
    for t in range(blocks):
        span = slice(t * feats, (t + 1) * feats)
        for idx, weight in enumerate(weights):
            parts[idx] += lax.dot_general(
                weight[:, span], acts_ref[t], ROWS_BY_ROWS, preferred_element_type=jnp.float32
            )
    for idx, part in enumerate(parts):
        turned[pl.ds(pl.multiple_of(starts_ref[idx] * slim, slim), slim), :] = part
    return turned[...].T


def finish_kernel(starts_ref, acts_ref, *refs):
    weights, (out_ref, most_ref, turned) = refs[:8], refs[8:]
    depth = acts_ref.shape[0] * acts_ref.shape[2]
    result = all_columns(starts_ref, acts_ref, weights, turned).astype(jnp.bfloat16)
    for copy in range(out_ref.shape[0]):
        out_ref[copy] = result
    most = weights[0][:, depth:]
    for weight in weights[1:]:
        most = jnp.maximum(most, weight[:, depth:])
    most_ref[...] = jnp.max(most.astype(jnp.float32), axis=0, keepdims=True)


def place_kernel(starts_ref, acts_ref, lengths_ref, others_ref, *refs):
    weights, (out_ref, turned) = refs[:8], refs[8:]
    result = all_columns(starts_ref, acts_ref, weights, turned).astype(jnp.bfloat16)
    others = others_ref[1, :, others_ref.shape[2] - result.shape[1] :]
    every = jnp.concatenate([result.astype(jnp.float32), others], axis=0).astype(jnp.bfloat16)
    chosen = live_slots(lengths_ref[...], 0, every.shape[0]).astype(jnp.bfloat16)
    out_ref[...] = lax.dot_general(
        chosen, every, (((0,), (0,)), ((), ())), preferred_element_type=jnp.float32
    ).astype(jnp.bfloat16)


def finish(starts, acts, weights, copies):
    wide = weights[0].shape[0] * len(weights)
    return pl.pallas_call(
        finish_kernel,
        out_shape=(
            pltpu.HBM((copies, acts.shape[1], wide), jnp.bfloat16),
            jax.ShapeDtypeStruct((1, LANES), jnp.float32),
        ),
        in_specs=[SMEM, VMEM] + [VMEM] * len(weights),
        out_specs=(VMEM, VMEM),
        scratch_shapes=[pltpu.VMEM((wide, acts.shape[1]), jnp.float32)],
        cost_estimate=COST,
        compiler_params=LIMIT,
        name="finish_0",
    )(starts, acts, *weights)


def place(starts, acts, lengths_row, others, weights):
    wide = weights[0].shape[0] * len(weights)
    return pl.pallas_call(
        place_kernel,
        out_shape=pltpu.HBM((lengths_row.shape[1], wide), jnp.bfloat16),
        in_specs=[SMEM] + [VMEM] * (3 + len(weights)),
        out_specs=VMEM,
        scratch_shapes=[pltpu.VMEM((wide, acts.shape[1]), jnp.float32)],
        cost_estimate=COST,
        compiler_params=LIMIT,
        name="finish_1",
    )(starts, acts, lengths_row, others, *weights)


def spread(value):
    count = lax.axis_size(CHIPS)
    copies = jnp.broadcast_to(value[None], (count,) + value.shape)
    return lax.all_to_all(copies, CHIPS, 0, 0)


def in_order(own, peer, core):
    return jnp.concatenate(
        [jnp.where(core == 0, own, peer), jnp.where(core == 0, peer, own)], axis=0
    )


def beyond_slots(
    tokens, lengths_row, norm_gain, weights, w_out, decay_base, rate_base, group_gain, state
):
    core = lax.axis_index("c")
    count, feats = tokens.shape
    rows = count - SLOTS
    heads, head = state.shape[2], state.shape[-1]
    n_x, n_tp = lax.axis_size("x"), lax.axis_size(TP)
    chosen = live_slots(lengths_row, SLOTS, rows)
    live = jnp.sum((lengths_row > STEP).astype(jnp.float32))
    active = jnp.arange(rows) + SLOTS < live
    mine = jnp.dot(chosen.astype(jnp.bfloat16), tokens, preferred_element_type=jnp.float32)
    mine = mine.astype(jnp.bfloat16)
    held = jnp.argmax(chosen, axis=1)
    out_own = w_out.swapaxes(1, 2)
    out_peer = lax.ppermute(out_own, "c", PAIR)

    def block(natural, layer_parts):
        pairs, outs, gain_in, base, rate_b, gain, state_l = layer_parts
        joined = jnp.concatenate(
            [in_order(pairs[2 * m], pairs[2 * m + 1], core) for m in range(6)], axis=0
        )
        values = natural.astype(jnp.float32)
        factor = lax.rsqrt(jnp.mean(values * values, axis=1, keepdims=True) + RMS_EPS)
        normed = (values * factor * gain_in).astype(jnp.bfloat16)
        projected = lax.dot_general(
            normed, joined, ROWS_BY_ROWS, preferred_element_type=jnp.float32
        ).astype(jnp.bfloat16)
        arrived = lax.all_to_all(projected.reshape(n_x, rows, -1), "x", 0, 0)
        arrived = arrived.transpose(1, 0, 2).astype(jnp.float32)
        recept, key, value, decay_pre, rate_pre, gate_pre = [
            arrived[:, :, m * head : (m + 1) * head] for m in range(6)
        ]
        base, rate_b, gain = [part.reshape(heads, head) for part in (base, rate_b, gain)]
        decay = jnp.exp(-math.exp(-0.5) * jax.nn.sigmoid(base + decay_pre))
        rate = jax.nn.sigmoid(rate_b + rate_pre)
        length = jnp.maximum(jnp.sqrt(jnp.sum(key * key, axis=-1, keepdims=True)), 1e-12)
        unit = key / length
        old = jnp.take(state_l, held, axis=0)
        column = value * length - jnp.sum(old * unit[:, :, None, :], axis=-1)
        dot = jnp.sum(unit * rate * recept, axis=-1, keepdims=True)
        readout = jnp.sum(old * (decay * recept)[:, :, None, :], axis=-1) + column * dot
        centred = readout - jnp.mean(readout, axis=-1, keepdims=True)
        spread_ = jnp.mean(centred * centred, axis=-1, keepdims=True)
        normal = centred * lax.rsqrt(spread_ + GROUP_EPS) * gain * jax.nn.sigmoid(gate_pre)
        mixed = jnp.where(active[:, None, None], normal, 0.0)
        mixed = mixed.astype(jnp.bfloat16).reshape(rows, feats)
        mixed_all = spread(mixed).reshape(n_tp, n_x, rows, feats).transpose(1, 2, 0, 3)
        cols = lax.dot_general(
            mixed_all.reshape(n_x * rows, n_tp * feats), in_order(*outs, core),
            ROWS_BY_ROWS, preferred_element_type=jnp.float32,
        ).astype(jnp.bfloat16)
        blocks = spread(cols.reshape(rows, -1)).reshape(n_tp, n_x, n_x, rows, -1)
        current = blocks.transpose(2, 3, 0, 1, 4)
        here = lax.dynamic_slice_in_dim(current, lax.axis_index("x"), 1, 0)
        here = lax.dynamic_slice_in_dim(here, lax.axis_index(TP), 1, 2).reshape(rows, feats)
        terms = (arrived.reshape(rows, -1), column.reshape(rows, feats), here.astype(jnp.float32))
        return current.reshape(n_x * rows, n_tp * feats), jnp.concatenate(terms, axis=1)

    natural = spread(mine).reshape(n_tp, n_x, rows, feats).transpose(1, 2, 0, 3)
    layers = (weights, (out_own, out_peer), norm_gain, decay_base, rate_base, group_gain, state)
    return lax.scan(block, natural.reshape(n_x * rows, n_tp * feats), layers)[1]


def local(
    tokens, lengths, norm_gain, w_recept, w_key, w_value, w_decay, w_rate, w_gate, w_out,
    decay_base, rate_base, group_gain, state,
):
    core, spot = lax.axis_index("c"), lax.axis_index("x")
    rows, feats = tokens.shape
    n_x, n_tp, n_chips = lax.axis_size("x"), lax.axis_size(TP), lax.axis_size(CHIPS)
    starts = []
    for k in range(n_x):
        source = (spot + n_x - k) % n_x
        starts += [source * 2 + core, source * 2 + 1 - core]
    starts = jnp.stack(starts).astype(jnp.int32)
    core_at = jnp.reshape(core, (1,)).astype(jnp.int32)
    lengths_row = lengths.reshape(1, rows)

    def along_x(layer, more):
        own = jnp.concatenate([w_out.swapaxes(1, 2)[layer]] + more, axis=1)
        return [own] + [
            lax.ppermute(own, "x", [(i, (i + k) % n_x) for i in range(n_x)])
            for k in range(1, n_x)
        ]

    def over_pair(pieces):
        return [p for piece in pieces for p in (piece, lax.ppermute(piece, "c", PAIR))]

    chosen, count = choose(lengths_row, tokens, SLOTS, n_chips)
    acts = lax.all_to_all(chosen, CHIPS, 0, 0)
    weights = []
    for w in (w_recept, w_key, w_value, w_decay, w_rate, w_gate):
        own = w.swapaxes(1, 2)
        weights += [own, lax.ppermute(own, "c", PAIR)]
    states = [table(layer, SLOTS, lengths, state) for layer in range(2)]
    columns = [over_pair(along_x(0, [count])), over_pair(along_x(1, []))]
    operands = (
        tokens, lengths_row, norm_gain, weights, w_out, decay_base, rate_base, group_gain, state
    )
    new_state = None
    for layer in range(2):
        acts = acts.reshape(n_tp, n_x * SLOTS, feats)
        projected = project(layer, core_at, acts, norm_gain, weights, n_x)
        arrived = lax.all_to_all(projected, "x", 0, 0)
        mixed, column_terms = read_out(
            layer, arrived, lengths_row, decay_base, rate_base, group_gain, states[layer], n_tp
        )
        mixed_all = lax.all_to_all(mixed, TP, 0, 0)
        if layer == 0:
            current, most = finish(starts, mixed_all, columns[0], n_chips)
            others = lax.cond(
                most[0, 0] > SLOTS,
                beyond_slots,
                lambda *_: jnp.zeros((2, rows - SLOTS, 8 * feats), jnp.float32),
                *operands,
            )
            acts = lax.all_to_all(current, CHIPS, 0, 0)
        new_state = update(
            layer, lengths, arrived, decay_base, rate_base, column_terms, others, state, new_state
        )
    return place(starts, mixed_all, lengths_row, others, columns[1]), new_state


def solution(mesh):
    finer = Mesh(mesh.devices.reshape(4, 4, mesh.shape["dp"] // 2, 2), ("z", "y", "x", "c"))
    wide = P(None, None, TP + DP)
    in_specs = (
        (P(DP, TP), P(DP), P()) + (wide,) * 7 + (P(None, TP),) * 3 + (P(None, DP, TP, None, None),)
    )
    out_specs = (P(DP, TP), P(None, DP, TP, None, None))
    return jax.shard_map(local, mesh=finer, in_specs=in_specs, out_specs=out_specs, check_vma=False)
```

```python
import functools
import math

import jax
import jax.numpy as jnp
from jax import lax
from jax.experimental import pallas as pl
from jax.experimental.pallas import tpu as pltpu
from jax.sharding import Mesh
from jax.sharding import PartitionSpec as P


STEP = 16
RMS_EPS = 1e-06
GROUP_EPS = 0.00064
TP = ("z", "y")
DP = ("x", "c")
CHIPS = ("z", "y", "x")
PAIR = [(0, 1), (1, 0)]
SLOTS = 24
LANES = 128
ROWS_BY_ROWS = (((1,), (1,)), ((), ()))
ANY = pl.BlockSpec(memory_space=pltpu.HBM)
VMEM = pl.BlockSpec(memory_space=pltpu.VMEM)
SMEM = pl.BlockSpec(memory_space=pltpu.SMEM)


COST = pl.CostEstimate(flops=1 << 31, bytes_accessed=8 << 20, transcendentals=0)
LIMIT = pltpu.CompilerParams(vmem_limit_bytes=24 << 20)


def in_hbm(array):
    return pltpu.with_memory_space_constraint(array, pltpu.HBM)


def live_slots(lengths_row, first, slots):
    live = (lengths_row > STEP).astype(jnp.float32)
    count = live.shape[1]
    before = lax.broadcasted_iota(jnp.int32, (count, count), 0)
    before = before < lax.broadcasted_iota(jnp.int32, (count, count), 1)
    place = jnp.dot(
        jnp.broadcast_to(live, (8, count)), before.astype(jnp.float32),
        preferred_element_type=jnp.float32,
    )[:1]
    wanted = lax.broadcasted_iota(jnp.int32, (slots, count), 0) + first
    return jnp.where((place == wanted.astype(jnp.float32)) & (live > 0), 1.0, 0.0)


def choose_kernel(lengths_ref, tokens_ref, out_ref, count_ref):
    chosen = live_slots(lengths_ref[...], 0, out_ref.shape[1]).astype(jnp.bfloat16)
    rows = jnp.dot(chosen, tokens_ref[...], preferred_element_type=jnp.float32)
    rows = rows.astype(jnp.bfloat16)
    for copy in range(out_ref.shape[0]):
        out_ref[copy] = rows
    live = (lengths_ref[...] > STEP).astype(jnp.float32)
    count = jnp.sum(live, axis=1, keepdims=True)
    count_ref[...] = jnp.broadcast_to(count, count_ref.shape).astype(jnp.bfloat16)


def choose(lengths_row, tokens, slots, copies):
    return pl.pallas_call(
        choose_kernel,
        out_shape=(
            pltpu.HBM((copies, slots, tokens.shape[1]), jnp.bfloat16),
            jax.ShapeDtypeStruct((lengths_row.shape[1], LANES), jnp.bfloat16),
        ),
        in_specs=[VMEM, VMEM],
        out_specs=(VMEM, VMEM),
        compiler_params=LIMIT,
        name="choose",
    )(lengths_row, tokens)


def project_kernel(layer, core_ref, acts_ref, gain_ref, *rest):
    weights, (out_ref, held, sems) = rest[:12], rest[12:]
    blocks, rows, feats = acts_ref.shape
    wide, depth = held.shape
    slim = weights[0].shape[1]
    chunks = sems.shape[0]
    core = core_ref[0]
    copies = []
    for chunk in range(chunks):
        span = pl.ds(chunk * (depth // chunks), depth // chunks)
        for idx, weight in enumerate(weights):
            half = core if idx % 2 == 0 else 1 - core
            start = pl.multiple_of((idx // 2) * 2 * slim + half * slim, slim)
            copy = pltpu.make_async_copy(
                weight.at[layer, :, span], held.at[pl.ds(start, slim), span], sems.at[chunk, idx]
            )
            copy.start()
            copies.append(copy)
    squares = jnp.zeros((rows, feats), jnp.float32)
    for t in range(blocks):
        part = acts_ref[t].astype(jnp.float32)
        squares += part * part
    mean = jnp.sum(squares, axis=1, keepdims=True) / (blocks * feats)
    factor = lax.rsqrt(mean + RMS_EPS)
    result = jnp.zeros((rows, wide), jnp.float32)
    for t in range(blocks):
        if t % (blocks // chunks) == 0:
            first = t // (blocks // chunks) * len(weights)
            for copy in copies[first : first + len(weights)]:
                copy.wait()
        span = slice(t * feats, (t + 1) * feats)
        part = acts_ref[t].astype(jnp.float32) * factor * gain_ref[layer : layer + 1, span]
        result += lax.dot_general(
            part.astype(jnp.bfloat16), held[:, span], ROWS_BY_ROWS,
            preferred_element_type=jnp.float32,
        )
    result = result.astype(jnp.bfloat16)
    per = out_ref.shape[1]
    for x in range(out_ref.shape[0]):
        out_ref[x] = result[x * per : (x + 1) * per]


def project(layer, core, acts, gain, weights, n_x):
    rows = acts.shape[1]
    slim, depth = weights[0].shape[1:]
    wide = slim * len(weights)
    return pl.pallas_call(
        functools.partial(project_kernel, layer),
        out_shape=pltpu.HBM((n_x, rows // n_x, wide), jnp.bfloat16),
        in_specs=[SMEM, VMEM, VMEM] + [ANY] * len(weights),
        out_specs=VMEM,
        scratch_shapes=[
            pltpu.VMEM((wide, depth), jnp.bfloat16),
            pltpu.SemaphoreType.DMA((1, len(weights))),
        ],
        cost_estimate=COST,
        compiler_params=LIMIT,
    )(core, acts, gain, *weights)


def table_kernel(layer, lengths_ref, state_ref, out_ref, held, sems):
    chunks = out_ref.shape[0]
    slots, heads, head, _ = held.shape
    per = slots // chunks

    def fetch(sequence, slot):
        return pltpu.make_async_copy(
            state_ref.at[layer, sequence], held.at[slot], sems.at[slot]
        )

    def start(sequence, slot):
        live = lengths_ref[sequence] > STEP

        @pl.when(live & (slot < slots))
        def _():
            fetch(sequence, slot).start()

        return slot + live.astype(jnp.int32)

    count = lax.fori_loop(0, state_ref.shape[1], start, jnp.int32(0))
    for idx in range(chunks):
        for slot in range(idx * per, (idx + 1) * per):

            @pl.when(slot < count)
            def _():
                fetch(0, slot).wait()

            @pl.when(slot >= count)
            def _():
                held[slot] = jnp.zeros_like(held[slot])

        parts = [held[idx * per + k].reshape(heads * head, head) for k in range(per)]
        out_ref[idx] = jnp.concatenate(parts, axis=1).astype(jnp.bfloat16)


def table(layer, slots, lengths, state):
    _, _, heads, head, _ = state.shape
    per = 4
    return pl.pallas_call(
        functools.partial(table_kernel, layer),
        out_shape=pltpu.VMEM((slots // per, heads * head, per * head), jnp.bfloat16),
        in_specs=[SMEM, ANY],
        out_specs=VMEM,
        scratch_shapes=[
            pltpu.VMEM((slots, heads, head, head), jnp.float32),
            pltpu.SemaphoreType.DMA((slots,)),
        ],
        cost_estimate=COST,
        compiler_params=LIMIT,
    )(lengths, in_hbm(state))


def vectors_of(layer, block, lanes, decay_ref, rate_ref):
    head = block.shape[1] // 6
    recept, key, value, decay_pre, rate_pre, gate_pre = [
        block[:, m * head : (m + 1) * head] for m in range(6)
    ]
    decay_in = decay_ref[layer : layer + 1, lanes] + decay_pre
    decay = jnp.exp(-math.exp(-0.5) * jax.nn.sigmoid(decay_in))
    rate = jax.nn.sigmoid(rate_ref[layer : layer + 1, lanes] + rate_pre)
    length = jnp.maximum(jnp.sqrt(jnp.sum(key * key, axis=1, keepdims=True)), 1e-12)
    unit = key / length
    return recept, value, gate_pre, decay, length, unit, unit * rate


def readout_kernel(
    layer, arrived_ref, lengths_ref, decay_ref, rate_ref, gain_ref, table_ref, mixed_ref, column_ref
):
    heads, count, wide = arrived_ref.shape
    head = wide // 6
    units, reads, kept = [], [], []
    for h in range(heads):
        lanes = slice(h * head, (h + 1) * head)
        block = arrived_ref[h].astype(jnp.float32)
        recept, value, gate_pre, decay, length, unit, learned = vectors_of(
            layer, block, lanes, decay_ref, rate_ref
        )
        units.append(unit)
        reads.append(decay * recept)
        dot = jnp.sum(learned * recept, axis=1, keepdims=True)
        kept.append((value * length, dot, jax.nn.sigmoid(gate_pre)))
    per = table_ref.shape[2] // head
    group = 8
    shape = (2 * heads * group, per * head)
    row = lax.broadcasted_iota(jnp.int32, shape, 0) % group
    spot = lax.broadcasted_iota(jnp.int32, shape, 1) // head
    lane_head = lax.broadcasted_iota(jnp.int32, (group, heads * head), 1) // head
    summed = ([], [])
    for g in range(count // group):
        rows = slice(g * group, (g + 1) * group)
        left = jnp.concatenate(
            [jnp.concatenate([v[rows]] * per, axis=1) for v in units + reads], axis=0
        )
        product = jnp.zeros((shape[0], heads * head), jnp.float32)
        for part in range(group // per):
            chosen = jnp.where(row == spot + part * per, left, 0.0).astype(jnp.bfloat16)
            product += lax.dot_general(
                chosen, table_ref[g * (group // per) + part], ROWS_BY_ROWS,
                preferred_element_type=jnp.float32,
            )
        for kind in range(2):
            base = kind * heads * group
            total = product[base : base + group]
            for h in range(1, heads):
                piece = product[base + h * group : base + (h + 1) * group]
                total = jnp.where(lane_head == h, piece, total)
            summed[kind].append(total)
    by_unit, by_read = [jnp.concatenate(parts, axis=0) for parts in summed]
    live = jnp.sum((lengths_ref[...] > STEP).astype(jnp.float32), axis=1, keepdims=True)
    active = lax.broadcasted_iota(jnp.int32, (count, 1), 0).astype(jnp.float32) < live
    mixed = []
    for h in range(heads):
        lanes = slice(h * head, (h + 1) * head)
        scaled, dot, gate = kept[h]
        column = scaled - by_unit[:, lanes]
        column_ref[:, lanes] = column
        readout = by_read[:, lanes] + column * dot
        centred = readout - jnp.mean(readout, axis=1, keepdims=True)
        spread_ = jnp.mean(centred * centred, axis=1, keepdims=True)
        normal = centred * lax.rsqrt(spread_ + GROUP_EPS)
        normal = normal * gain_ref[layer : layer + 1, lanes] * gate
        mixed.append(jnp.where(active, normal, 0.0))
    rows = jnp.concatenate(mixed, axis=1).astype(jnp.bfloat16)
    for t in range(mixed_ref.shape[0]):
        mixed_ref[t] = rows


def read_out(layer, arrived, lengths, decay_base, rate_base, group_gain, states, copies):
    heads, count, wide = arrived.shape
    feats = heads * wide // 6
    return pl.pallas_call(
        functools.partial(readout_kernel, layer),
        out_shape=(
            pltpu.HBM((copies, count, feats), jnp.bfloat16),
            pltpu.VMEM((count, feats), jnp.float32),
        ),
        in_specs=[VMEM] * 6,
        out_specs=(VMEM, VMEM),
        cost_estimate=COST,
        compiler_params=LIMIT,
    )(arrived, lengths, decay_base, rate_base, group_gain, states)


def in_two(value):
    high = value.astype(jnp.bfloat16)
    return high, (value - high.astype(jnp.float32)).astype(jnp.bfloat16)


def update_kernel(
    layer, lengths_ref, arrived_ref, decay_ref, rate_ref, column_ref, others_ref, state_ref, *rest
):
    out_ref, held, rows_ref, columns_ref, added_ref, in_sems, out_sems = rest[-7:]
    count, heads, head, _ = held.shape
    chunks = in_sems.shape[0]
    per = count // chunks

    def fetch(idx):
        span = pl.ds(idx * per, per)
        return pltpu.make_async_copy(state_ref.at[layer, span], held.at[span], in_sems.at[idx])

    def put(idx):
        span = pl.ds(idx * per, per)
        return pltpu.make_async_copy(held.at[span], out_ref.at[layer, span], out_sems.at[idx])

    for idx in range(chunks):
        fetch(idx).start()
    for h in range(heads):
        lanes = slice(h * head, (h + 1) * head)
        block = jnp.concatenate(
            [
                arrived_ref[h].astype(jnp.float32),
                others_ref[layer, :, h * 6 * head : (h + 1) * 6 * head],
            ],
            axis=0,
        )
        _, _, _, decay, _, _, learned = vectors_of(layer, block, lanes, decay_ref, rate_ref)
        rows_ref[:, h, :] = decay
        rows_ref[:, heads + h, :] = learned
    slots = column_ref.shape[0]
    columns_ref[:slots] = column_ref[...]
    columns_ref[slots:] = others_ref[layer, :, heads * 6 * head : heads * 7 * head]
    own = lax.broadcasted_iota(jnp.int32, (heads, heads * head), 0)
    own = own == lax.broadcasted_iota(jnp.int32, (heads, heads * head), 1) // head

    def outer(slot):
        high, low = in_two(jnp.where(own, columns_ref[pl.ds(slot, 1), :], 0.0))
        right_high, right_low = in_two(rows_ref[slot, heads:, :])
        added = lax.dot_general(
            jnp.concatenate([high, high, low], axis=0),
            jnp.concatenate([right_high, right_low, right_high], axis=0),
            (((0,), (0,)), ((), ())), preferred_element_type=jnp.float32,
        )
        added_ref[slot] = added.reshape(heads, head, head)

    def tally(r, total):
        return total + (lengths_ref[r] > STEP).astype(jnp.int32)

    total = lax.fori_loop(0, count, tally, jnp.int32(0))

    @pl.loop(0, (total + 1) // 2)
    def _(pair):
        outer(2 * pair)
        outer(2 * pair + 1)

    def advance(r, slot):
        live = lengths_ref[r] > STEP

        @pl.when(live)
        def _():
            for h in range(heads):
                held[r, h] = held[r, h] * rows_ref[slot, h : h + 1, :] + added_ref[slot, h]

        return slot + live.astype(jnp.int32)

    slot = jnp.int32(0)
    for idx in range(chunks):
        fetch(idx).wait()
        slot = lax.fori_loop(idx * per, (idx + 1) * per, advance, slot)
        if idx:
            put(idx - 1).start()
    put(chunks - 1).start()
    for idx in range(chunks):
        put(idx).wait()


def update(layer, lengths, arrived, decay_base, rate_base, column, others, state, earlier):
    _, count, heads, head, _ = state.shape
    more = () if earlier is None else (earlier,)
    return pl.pallas_call(
        functools.partial(update_kernel, layer),
        out_shape=pltpu.HBM(state.shape, state.dtype),
        in_specs=[SMEM] + [VMEM] * 5 + [ANY] + [ANY] * len(more),
        out_specs=ANY,
        scratch_shapes=[
            pltpu.VMEM((count, heads, head, head), jnp.float32),
            pltpu.VMEM((count, 2 * heads, head), jnp.float32),
            pltpu.VMEM((count, heads * head), jnp.float32),
            pltpu.VMEM((count, heads, head, head), jnp.float32),
            pltpu.SemaphoreType.DMA((8,)),
            pltpu.SemaphoreType.DMA((8,)),
        ],
        input_output_aliases={7: 0} if more else {},
        cost_estimate=COST,
        compiler_params=LIMIT,
    )(lengths, arrived, decay_base, rate_base, column, others, in_hbm(state), *map(in_hbm, more))


def all_columns(starts_ref, acts_ref, weights, turned):
    blocks, rows, feats = acts_ref.shape
    slim = weights[0].shape[0]
    parts = [jnp.zeros((slim, rows), jnp.float32) for _ in weights]
    for t in range(blocks):
        span = slice(t * feats, (t + 1) * feats)
        for idx, weight in enumerate(weights):
            parts[idx] += lax.dot_general(
                weight[:, span], acts_ref[t], ROWS_BY_ROWS, preferred_element_type=jnp.float32
            )
    for idx, part in enumerate(parts):
        turned[pl.ds(pl.multiple_of(starts_ref[idx] * slim, slim), slim), :] = part
    return turned[...].T


def finish_kernel(starts_ref, acts_ref, *refs):
    weights, (out_ref, most_ref, turned) = refs[:8], refs[8:]
    depth = acts_ref.shape[0] * acts_ref.shape[2]
    result = all_columns(starts_ref, acts_ref, weights, turned).astype(jnp.bfloat16)
    for copy in range(out_ref.shape[0]):
        out_ref[copy] = result
    most = weights[0][:, depth:]
    for weight in weights[1:]:
        most = jnp.maximum(most, weight[:, depth:])
    most_ref[...] = jnp.max(most.astype(jnp.float32), axis=0, keepdims=True)


def place_kernel(starts_ref, acts_ref, lengths_ref, others_ref, *refs):
    weights, (out_ref, turned) = refs[:8], refs[8:]
    result = all_columns(starts_ref, acts_ref, weights, turned).astype(jnp.bfloat16)
    others = others_ref[1, :, others_ref.shape[2] - result.shape[1] :]
    every = jnp.concatenate([result.astype(jnp.float32), others], axis=0).astype(jnp.bfloat16)
    chosen = live_slots(lengths_ref[...], 0, every.shape[0]).astype(jnp.bfloat16)
    out_ref[...] = lax.dot_general(
        chosen, every, (((0,), (0,)), ((), ())), preferred_element_type=jnp.float32
    ).astype(jnp.bfloat16)


def finish(starts, acts, weights, copies):
    wide = weights[0].shape[0] * len(weights)
    return pl.pallas_call(
        finish_kernel,
        out_shape=(
            pltpu.HBM((copies, acts.shape[1], wide), jnp.bfloat16),
            jax.ShapeDtypeStruct((1, LANES), jnp.float32),
        ),
        in_specs=[SMEM, VMEM] + [VMEM] * len(weights),
        out_specs=(VMEM, VMEM),
        scratch_shapes=[pltpu.VMEM((wide, acts.shape[1]), jnp.float32)],
        cost_estimate=COST,
        compiler_params=LIMIT,
        name="finish_0",
    )(starts, acts, *weights)


def place(starts, acts, lengths_row, others, weights):
    wide = weights[0].shape[0] * len(weights)
    return pl.pallas_call(
        place_kernel,
        out_shape=pltpu.HBM((lengths_row.shape[1], wide), jnp.bfloat16),
        in_specs=[SMEM] + [VMEM] * (3 + len(weights)),
        out_specs=VMEM,
        scratch_shapes=[pltpu.VMEM((wide, acts.shape[1]), jnp.float32)],
        cost_estimate=COST,
        compiler_params=LIMIT,
        name="finish_1",
    )(starts, acts, lengths_row, others, *weights)


def spread(value):
    count = lax.axis_size(CHIPS)
    copies = jnp.broadcast_to(value[None], (count,) + value.shape)
    return lax.all_to_all(copies, CHIPS, 0, 0)


def in_order(own, peer, core):
    return jnp.concatenate(
        [jnp.where(core == 0, own, peer), jnp.where(core == 0, peer, own)], axis=0
    )


def beyond_slots(
    tokens, lengths_row, norm_gain, weights, w_out, decay_base, rate_base, group_gain, state
):
    core = lax.axis_index("c")
    count, feats = tokens.shape
    rows = count - SLOTS
    heads, head = state.shape[2], state.shape[-1]
    n_x, n_tp = lax.axis_size("x"), lax.axis_size(TP)
    chosen = live_slots(lengths_row, SLOTS, rows)
    live = jnp.sum((lengths_row > STEP).astype(jnp.float32))
    active = jnp.arange(rows) + SLOTS < live
    mine = jnp.dot(chosen.astype(jnp.bfloat16), tokens, preferred_element_type=jnp.float32)
    mine = mine.astype(jnp.bfloat16)
    held = jnp.argmax(chosen, axis=1)
    out_own = w_out.swapaxes(1, 2)
    out_peer = lax.ppermute(out_own, "c", PAIR)

    def block(natural, layer_parts):
        pairs, outs, gain_in, base, rate_b, gain, state_l = layer_parts
        joined = jnp.concatenate(
            [in_order(pairs[2 * m], pairs[2 * m + 1], core) for m in range(6)], axis=0
        )
        values = natural.astype(jnp.float32)
        factor = lax.rsqrt(jnp.mean(values * values, axis=1, keepdims=True) + RMS_EPS)
        normed = (values * factor * gain_in).astype(jnp.bfloat16)
        projected = lax.dot_general(
            normed, joined, ROWS_BY_ROWS, preferred_element_type=jnp.float32
        ).astype(jnp.bfloat16)
        arrived = lax.all_to_all(projected.reshape(n_x, rows, -1), "x", 0, 0)
        arrived = arrived.transpose(1, 0, 2).astype(jnp.float32)
        recept, key, value, decay_pre, rate_pre, gate_pre = [
            arrived[:, :, m * head : (m + 1) * head] for m in range(6)
        ]
        base, rate_b, gain = [part.reshape(heads, head) for part in (base, rate_b, gain)]
        decay = jnp.exp(-math.exp(-0.5) * jax.nn.sigmoid(base + decay_pre))
        rate = jax.nn.sigmoid(rate_b + rate_pre)
        length = jnp.maximum(jnp.sqrt(jnp.sum(key * key, axis=-1, keepdims=True)), 1e-12)
        unit = key / length
        old = jnp.take(state_l, held, axis=0)
        column = value * length - jnp.sum(old * unit[:, :, None, :], axis=-1)
        dot = jnp.sum(unit * rate * recept, axis=-1, keepdims=True)
        readout = jnp.sum(old * (decay * recept)[:, :, None, :], axis=-1) + column * dot
        centred = readout - jnp.mean(readout, axis=-1, keepdims=True)
        spread_ = jnp.mean(centred * centred, axis=-1, keepdims=True)
        normal = centred * lax.rsqrt(spread_ + GROUP_EPS) * gain * jax.nn.sigmoid(gate_pre)
        mixed = jnp.where(active[:, None, None], normal, 0.0)
        mixed = mixed.astype(jnp.bfloat16).reshape(rows, feats)
        mixed_all = spread(mixed).reshape(n_tp, n_x, rows, feats).transpose(1, 2, 0, 3)
        cols = lax.dot_general(
            mixed_all.reshape(n_x * rows, n_tp * feats), in_order(*outs, core),
            ROWS_BY_ROWS, preferred_element_type=jnp.float32,
        ).astype(jnp.bfloat16)
        blocks = spread(cols.reshape(rows, -1)).reshape(n_tp, n_x, n_x, rows, -1)
        current = blocks.transpose(2, 3, 0, 1, 4)
        here = lax.dynamic_slice_in_dim(current, lax.axis_index("x"), 1, 0)
        here = lax.dynamic_slice_in_dim(here, lax.axis_index(TP), 1, 2).reshape(rows, feats)
        terms = (arrived.reshape(rows, -1), column.reshape(rows, feats), here.astype(jnp.float32))
        return current.reshape(n_x * rows, n_tp * feats), jnp.concatenate(terms, axis=1)

    natural = spread(mine).reshape(n_tp, n_x, rows, feats).transpose(1, 2, 0, 3)
    layers = (weights, (out_own, out_peer), norm_gain, decay_base, rate_base, group_gain, state)
    return lax.scan(block, natural.reshape(n_x * rows, n_tp * feats), layers)[1]


def local(
    tokens, lengths, norm_gain, w_recept, w_key, w_value, w_decay, w_rate, w_gate, w_out,
    decay_base, rate_base, group_gain, state,
):
    core, spot = lax.axis_index("c"), lax.axis_index("x")
    rows, feats = tokens.shape
    n_x, n_tp, n_chips = lax.axis_size("x"), lax.axis_size(TP), lax.axis_size(CHIPS)
    starts = []
    for k in range(n_x):
        source = (spot + n_x - k) % n_x
        starts += [source * 2 + core, source * 2 + 1 - core]
    starts = jnp.stack(starts).astype(jnp.int32)
    core_at = jnp.reshape(core, (1,)).astype(jnp.int32)
    lengths_row = lengths.reshape(1, rows)

    def along_x(layer, more):
        own = jnp.concatenate([w_out.swapaxes(1, 2)[layer]] + more, axis=1)
        pieces = [own]
        for k in range(1, n_x):
            shift = [(i, (i + k) % n_x) for i in range(n_x)]
            pieces.append(lax.ppermute(own, "x", shift))
        return pieces

    def over_pair(pieces):
        return [p for piece in pieces for p in (piece, lax.ppermute(piece, "c", PAIR))]

    chosen, count = choose(lengths_row, tokens, SLOTS, n_chips)
    acts = lax.all_to_all(chosen, CHIPS, 0, 0)
    weights = []
    for w in (w_recept, w_key, w_value, w_decay, w_rate, w_gate):
        own = w.swapaxes(1, 2)
        weights += [own, lax.ppermute(own, "c", PAIR)]
    states = [table(layer, SLOTS, lengths, state) for layer in range(2)]
    columns = [over_pair(along_x(0, [count])), over_pair(along_x(1, []))]
    operands = (
        tokens, lengths_row, norm_gain, weights, w_out, decay_base, rate_base, group_gain, state
    )
    new_state = None
    for layer in range(2):
        acts = acts.reshape(n_tp, n_x * SLOTS, feats)
        projected = project(layer, core_at, acts, norm_gain, weights, n_x)
        arrived = lax.all_to_all(projected, "x", 0, 0)
        mixed, column_terms = read_out(
            layer, arrived, lengths_row, decay_base, rate_base, group_gain, states[layer], n_tp
        )
        mixed_all = lax.all_to_all(mixed, TP, 0, 0)
        if layer == 0:
            current, most = finish(starts, mixed_all, columns[0], n_chips)
            others = lax.cond(
                most[0, 0] > SLOTS,
                beyond_slots,
                lambda *_: jnp.zeros((2, rows - SLOTS, 8 * feats), jnp.float32),
                *operands,
            )
            acts = lax.all_to_all(current, CHIPS, 0, 0)
        new_state = update(
            layer, lengths, arrived, decay_base, rate_base, column_terms, others, state, new_state
        )
    return place(starts, mixed_all, lengths_row, others, columns[1]), new_state


def solution(mesh):
    finer = Mesh(mesh.devices.reshape(4, 4, mesh.shape["dp"] // 2, 2), ("z", "y", "x", "c"))
    wide = P(None, None, TP + DP)
    in_specs = (
        (P(DP, TP), P(DP), P()) + (wide,) * 7 + (P(None, TP),) * 3 + (P(None, DP, TP, None, None),)
    )
    out_specs = (P(DP, TP), P(None, DP, TP, None, None))
    return jax.shard_map(local, mesh=finer, in_specs=in_specs, out_specs=out_specs, check_vma=False)
```

```python
import functools
import math

import jax
import jax.numpy as jnp
from jax import lax
from jax.experimental import pallas as pl
from jax.experimental.pallas import tpu as pltpu
from jax.sharding import Mesh
from jax.sharding import PartitionSpec as P


STEP = 16
RMS_EPS = 1e-06
GROUP_EPS = 0.00064
TP = ("z", "y")
DP = ("x", "c")
CHIPS = ("z", "y", "x")
PAIR = [(0, 1), (1, 0)]
SLOTS = 24
LANES = 128
ROWS_BY_ROWS = (((1,), (1,)), ((), ()))
ANY = pl.BlockSpec(memory_space=pltpu.HBM)
VMEM = pl.BlockSpec(memory_space=pltpu.VMEM)
SMEM = pl.BlockSpec(memory_space=pltpu.SMEM)


COST = pl.CostEstimate(flops=1 << 31, bytes_accessed=8 << 20, transcendentals=0)
LIMIT = pltpu.CompilerParams(vmem_limit_bytes=24 << 20)


def in_hbm(array):
    return pltpu.with_memory_space_constraint(array, pltpu.HBM)


def live_slots(lengths_row, first, slots):
    live = (lengths_row > STEP).astype(jnp.float32)
    count = live.shape[1]
    before = lax.broadcasted_iota(jnp.int32, (count, count), 0)
    before = before < lax.broadcasted_iota(jnp.int32, (count, count), 1)
    place = jnp.dot(
        jnp.broadcast_to(live, (8, count)), before.astype(jnp.float32),
        preferred_element_type=jnp.float32,
    )[:1]
    wanted = lax.broadcasted_iota(jnp.int32, (slots, count), 0) + first
    return jnp.where((place == wanted.astype(jnp.float32)) & (live > 0), 1.0, 0.0)


def choose_kernel(lengths_ref, tokens_ref, out_ref, count_ref):
    chosen = live_slots(lengths_ref[...], 0, out_ref.shape[1]).astype(jnp.bfloat16)
    rows = jnp.dot(chosen, tokens_ref[...], preferred_element_type=jnp.float32)
    rows = rows.astype(jnp.bfloat16)
    for copy in range(out_ref.shape[0]):
        out_ref[copy] = rows
    live = (lengths_ref[...] > STEP).astype(jnp.float32)
    count = jnp.sum(live, axis=1, keepdims=True)
    count_ref[...] = jnp.broadcast_to(count, count_ref.shape).astype(jnp.bfloat16)


def choose(lengths_row, tokens, slots, copies):
    return pl.pallas_call(
        choose_kernel,
        out_shape=(
            pltpu.HBM((copies, slots, tokens.shape[1]), jnp.bfloat16),
            jax.ShapeDtypeStruct((lengths_row.shape[1], LANES), jnp.bfloat16),
        ),
        in_specs=[VMEM, VMEM],
        out_specs=(VMEM, VMEM),
        compiler_params=LIMIT,
        name="choose",
    )(lengths_row, tokens)


def project_kernel(layer, core_ref, acts_ref, gain_ref, *rest):
    weights, (out_ref, held, sems) = rest[:12], rest[12:]
    blocks, rows, feats = acts_ref.shape
    wide, depth = held.shape
    slim = weights[0].shape[1]
    chunks = sems.shape[0]
    core = core_ref[0]
    copies = []
    for chunk in range(chunks):
        span = pl.ds(chunk * (depth // chunks), depth // chunks)
        for idx, weight in enumerate(weights):
            half = core if idx % 2 == 0 else 1 - core
            start = pl.multiple_of((idx // 2) * 2 * slim + half * slim, slim)
            copy = pltpu.make_async_copy(
                weight.at[layer, :, span], held.at[pl.ds(start, slim), span], sems.at[chunk, idx]
            )
            copy.start()
            copies.append(copy)
    squares = jnp.zeros((rows, feats), jnp.float32)
    for t in range(blocks):
        part = acts_ref[t].astype(jnp.float32)
        squares += part * part
    mean = jnp.sum(squares, axis=1, keepdims=True) / (blocks * feats)
    factor = lax.rsqrt(mean + RMS_EPS)
    result = jnp.zeros((rows, wide), jnp.float32)
    for t in range(blocks):
        if t % (blocks // chunks) == 0:
            first = t // (blocks // chunks) * len(weights)
            for copy in copies[first : first + len(weights)]:
                copy.wait()
        span = slice(t * feats, (t + 1) * feats)
        part = acts_ref[t].astype(jnp.float32) * factor * gain_ref[layer : layer + 1, span]
        result += lax.dot_general(
            part.astype(jnp.bfloat16), held[:, span], ROWS_BY_ROWS,
            preferred_element_type=jnp.float32,
        )
    result = result.astype(jnp.bfloat16)
    per = out_ref.shape[1]
    for x in range(out_ref.shape[0]):
        out_ref[x] = result[x * per : (x + 1) * per]


def project(layer, core, acts, gain, weights, n_x):
    rows = acts.shape[1]
    slim, depth = weights[0].shape[1:]
    wide = slim * len(weights)
    return pl.pallas_call(
        functools.partial(project_kernel, layer),
        out_shape=pltpu.HBM((n_x, rows // n_x, wide), jnp.bfloat16),
        in_specs=[SMEM, VMEM, VMEM] + [ANY] * len(weights),
        out_specs=VMEM,
        scratch_shapes=[
            pltpu.VMEM((wide, depth), jnp.bfloat16),
            pltpu.SemaphoreType.DMA((1, len(weights))),
        ],
        cost_estimate=COST,
        compiler_params=LIMIT,
    )(core, acts, gain, *weights)


def table_kernel(layer, lengths_ref, state_ref, out_ref, held, sems):
    chunks = out_ref.shape[0]
    slots, heads, head, _ = held.shape
    per = slots // chunks

    def fetch(sequence, slot):
        return pltpu.make_async_copy(
            state_ref.at[layer, sequence], held.at[slot], sems.at[slot]
        )

    def start(sequence, slot):
        live = lengths_ref[sequence] > STEP

        @pl.when(live & (slot < slots))
        def _():
            fetch(sequence, slot).start()

        return slot + live.astype(jnp.int32)

    count = lax.fori_loop(0, state_ref.shape[1], start, jnp.int32(0))
    for idx in range(chunks):
        for slot in range(idx * per, (idx + 1) * per):

            @pl.when(slot < count)
            def _():
                fetch(0, slot).wait()

            @pl.when(slot >= count)
            def _():
                held[slot] = jnp.zeros_like(held[slot])

        parts = [held[idx * per + k].reshape(heads * head, head) for k in range(per)]
        out_ref[idx] = jnp.concatenate(parts, axis=1).astype(jnp.bfloat16)


def table(layer, slots, lengths, state):
    _, _, heads, head, _ = state.shape
    per = 4
    return pl.pallas_call(
        functools.partial(table_kernel, layer),
        out_shape=pltpu.VMEM((slots // per, heads * head, per * head), jnp.bfloat16),
        in_specs=[SMEM, ANY],
        out_specs=VMEM,
        scratch_shapes=[
            pltpu.VMEM((slots, heads, head, head), jnp.float32),
            pltpu.SemaphoreType.DMA((slots,)),
        ],
        cost_estimate=COST,
        compiler_params=LIMIT,
    )(lengths, in_hbm(state))


def vectors_of(layer, block, lanes, decay_ref, rate_ref):
    head = block.shape[1] // 6
    recept, key, value, decay_pre, rate_pre, gate_pre = [
        block[:, m * head : (m + 1) * head] for m in range(6)
    ]
    decay_in = decay_ref[layer : layer + 1, lanes] + decay_pre
    decay = jnp.exp(-math.exp(-0.5) * jax.nn.sigmoid(decay_in))
    rate = jax.nn.sigmoid(rate_ref[layer : layer + 1, lanes] + rate_pre)
    length = jnp.maximum(jnp.sqrt(jnp.sum(key * key, axis=1, keepdims=True)), 1e-12)
    unit = key / length
    return recept, value, gate_pre, decay, length, unit, unit * rate


def readout_kernel(
    layer, arrived_ref, lengths_ref, decay_ref, rate_ref, gain_ref, table_ref, mixed_ref, column_ref
):
    heads, count, wide = arrived_ref.shape
    head = wide // 6
    units, reads, kept = [], [], []
    for h in range(heads):
        lanes = slice(h * head, (h + 1) * head)
        block = arrived_ref[h].astype(jnp.float32)
        recept, value, gate_pre, decay, length, unit, learned = vectors_of(
            layer, block, lanes, decay_ref, rate_ref
        )
        units.append(unit)
        reads.append(decay * recept)
        dot = jnp.sum(learned * recept, axis=1, keepdims=True)
        kept.append((value * length, dot, jax.nn.sigmoid(gate_pre)))
    per = table_ref.shape[2] // head
    group = 8
    shape = (2 * heads * group, per * head)
    row = lax.broadcasted_iota(jnp.int32, shape, 0) % group
    spot = lax.broadcasted_iota(jnp.int32, shape, 1) // head
    lane_head = lax.broadcasted_iota(jnp.int32, (group, heads * head), 1) // head
    summed = ([], [])
    for g in range(count // group):
        rows = slice(g * group, (g + 1) * group)
        left = jnp.concatenate(
            [jnp.concatenate([v[rows]] * per, axis=1) for v in units + reads], axis=0
        )
        product = jnp.zeros((shape[0], heads * head), jnp.float32)
        for part in range(group // per):
            chosen = jnp.where(row == spot + part * per, left, 0.0).astype(jnp.bfloat16)
            product += lax.dot_general(
                chosen, table_ref[g * (group // per) + part], ROWS_BY_ROWS,
                preferred_element_type=jnp.float32,
            )
        for kind in range(2):
            base = kind * heads * group
            total = product[base : base + group]
            for h in range(1, heads):
                piece = product[base + h * group : base + (h + 1) * group]
                total = jnp.where(lane_head == h, piece, total)
            summed[kind].append(total)
    by_unit, by_read = [jnp.concatenate(parts, axis=0) for parts in summed]
    live = jnp.sum((lengths_ref[...] > STEP).astype(jnp.float32), axis=1, keepdims=True)
    active = lax.broadcasted_iota(jnp.int32, (count, 1), 0).astype(jnp.float32) < live
    mixed = []
    for h in range(heads):
        lanes = slice(h * head, (h + 1) * head)
        scaled, dot, gate = kept[h]
        column = scaled - by_unit[:, lanes]
        column_ref[:, lanes] = column
        readout = by_read[:, lanes] + column * dot
        centred = readout - jnp.mean(readout, axis=1, keepdims=True)
        spread_ = jnp.mean(centred * centred, axis=1, keepdims=True)
        normal = centred * lax.rsqrt(spread_ + GROUP_EPS)
        normal = normal * gain_ref[layer : layer + 1, lanes] * gate
        mixed.append(jnp.where(active, normal, 0.0))
    rows = jnp.concatenate(mixed, axis=1).astype(jnp.bfloat16)
    for t in range(mixed_ref.shape[0]):
        mixed_ref[t] = rows


def read_out(layer, arrived, lengths, decay_base, rate_base, group_gain, states, copies):
    heads, count, wide = arrived.shape
    feats = heads * wide // 6
    return pl.pallas_call(
        functools.partial(readout_kernel, layer),
        out_shape=(
            pltpu.HBM((copies, count, feats), jnp.bfloat16),
            pltpu.VMEM((count, feats), jnp.float32),
        ),
        in_specs=[VMEM] * 6,
        out_specs=(VMEM, VMEM),
        cost_estimate=COST,
        compiler_params=LIMIT,
    )(arrived, lengths, decay_base, rate_base, group_gain, states)


def in_two(value):
    high = value.astype(jnp.bfloat16)
    return high, (value - high.astype(jnp.float32)).astype(jnp.bfloat16)


def update_kernel(
    layer, lengths_ref, arrived_ref, decay_ref, rate_ref, column_ref, others_ref, state_ref, *rest
):
    out_ref, held, rows_ref, columns_ref, added_ref, in_sems, out_sems = rest[-7:]
    count, heads, head, _ = held.shape
    chunks = in_sems.shape[0]
    per = count // chunks

    def fetch(idx):
        span = pl.ds(idx * per, per)
        return pltpu.make_async_copy(state_ref.at[layer, span], held.at[span], in_sems.at[idx])

    def put(idx):
        span = pl.ds(idx * per, per)
        return pltpu.make_async_copy(held.at[span], out_ref.at[layer, span], out_sems.at[idx])

    for idx in range(chunks):
        fetch(idx).start()
    for h in range(heads):
        lanes = slice(h * head, (h + 1) * head)
        block = jnp.concatenate(
            [
                arrived_ref[h].astype(jnp.float32),
                others_ref[layer, :, h * 6 * head : (h + 1) * 6 * head],
            ],
            axis=0,
        )
        _, _, _, decay, _, _, learned = vectors_of(layer, block, lanes, decay_ref, rate_ref)
        rows_ref[:, h, :] = decay
        rows_ref[:, heads + h, :] = learned
    slots = column_ref.shape[0]
    columns_ref[:slots] = column_ref[...]
    columns_ref[slots:] = others_ref[layer, :, heads * 6 * head : heads * 7 * head]
    own = lax.broadcasted_iota(jnp.int32, (heads, heads * head), 0)
    own = own == lax.broadcasted_iota(jnp.int32, (heads, heads * head), 1) // head

    def outer(slot):
        high, low = in_two(jnp.where(own, columns_ref[pl.ds(slot, 1), :], 0.0))
        right_high, right_low = in_two(rows_ref[slot, heads:, :])
        added = lax.dot_general(
            jnp.concatenate([high, high, low], axis=0),
            jnp.concatenate([right_high, right_low, right_high], axis=0),
            (((0,), (0,)), ((), ())), preferred_element_type=jnp.float32,
        )
        added_ref[slot] = added.reshape(heads, head, head)

    def tally(r, total):
        return total + (lengths_ref[r] > STEP).astype(jnp.int32)

    total = lax.fori_loop(0, count, tally, jnp.int32(0))

    @pl.loop(0, (total + 1) // 2)
    def _(pair):
        outer(2 * pair)
        outer(2 * pair + 1)

    def advance(r, slot):
        live = lengths_ref[r] > STEP

        @pl.when(live)
        def _():
            for h in range(heads):
                held[r, h] = held[r, h] * rows_ref[slot, h : h + 1, :] + added_ref[slot, h]

        return slot + live.astype(jnp.int32)

    slot = jnp.int32(0)
    for idx in range(chunks):
        fetch(idx).wait()
        slot = lax.fori_loop(idx * per, (idx + 1) * per, advance, slot)
        if idx:
            put(idx - 1).start()
    put(chunks - 1).start()
    for idx in range(chunks):
        put(idx).wait()


def update(layer, lengths, arrived, decay_base, rate_base, column, others, state, earlier):
    _, count, heads, head, _ = state.shape
    more = () if earlier is None else (earlier,)
    return pl.pallas_call(
        functools.partial(update_kernel, layer),
        out_shape=pltpu.HBM(state.shape, state.dtype),
        in_specs=[SMEM] + [VMEM] * 5 + [ANY] + [ANY] * len(more),
        out_specs=ANY,
        scratch_shapes=[
            pltpu.VMEM((count, heads, head, head), jnp.float32),
            pltpu.VMEM((count, 2 * heads, head), jnp.float32),
            pltpu.VMEM((count, heads * head), jnp.float32),
            pltpu.VMEM((count, heads, head, head), jnp.float32),
            pltpu.SemaphoreType.DMA((16,)),
            pltpu.SemaphoreType.DMA((16,)),
        ],
        input_output_aliases={7: 0} if more else {},
        cost_estimate=COST,
        compiler_params=LIMIT,
    )(lengths, arrived, decay_base, rate_base, column, others, in_hbm(state), *map(in_hbm, more))


def all_columns(starts_ref, acts_ref, weights, turned):
    blocks, rows, feats = acts_ref.shape
    slim = weights[0].shape[0]
    parts = [jnp.zeros((slim, rows), jnp.float32) for _ in weights]
    for t in range(blocks):
        span = slice(t * feats, (t + 1) * feats)
        for idx, weight in enumerate(weights):
            parts[idx] += lax.dot_general(
                weight[:, span], acts_ref[t], ROWS_BY_ROWS, preferred_element_type=jnp.float32
            )
    for idx, part in enumerate(parts):
        turned[pl.ds(pl.multiple_of(starts_ref[idx] * slim, slim), slim), :] = part
    return turned[...].T


def finish_kernel(starts_ref, acts_ref, *refs):
    weights, (out_ref, most_ref, turned) = refs[:8], refs[8:]
    depth = acts_ref.shape[0] * acts_ref.shape[2]
    result = all_columns(starts_ref, acts_ref, weights, turned).astype(jnp.bfloat16)
    for copy in range(out_ref.shape[0]):
        out_ref[copy] = result
    most = weights[0][:, depth:]
    for weight in weights[1:]:
        most = jnp.maximum(most, weight[:, depth:])
    most_ref[...] = jnp.max(most.astype(jnp.float32), axis=0, keepdims=True)


def place_kernel(starts_ref, acts_ref, lengths_ref, others_ref, *refs):
    weights, (out_ref, turned) = refs[:8], refs[8:]
    result = all_columns(starts_ref, acts_ref, weights, turned).astype(jnp.bfloat16)
    others = others_ref[1, :, others_ref.shape[2] - result.shape[1] :]
    every = jnp.concatenate([result.astype(jnp.float32), others], axis=0).astype(jnp.bfloat16)
    chosen = live_slots(lengths_ref[...], 0, every.shape[0]).astype(jnp.bfloat16)
    out_ref[...] = lax.dot_general(
        chosen, every, (((0,), (0,)), ((), ())), preferred_element_type=jnp.float32
    ).astype(jnp.bfloat16)


def finish(starts, acts, weights, copies):
    wide = weights[0].shape[0] * len(weights)
    return pl.pallas_call(
        finish_kernel,
        out_shape=(
            pltpu.HBM((copies, acts.shape[1], wide), jnp.bfloat16),
            jax.ShapeDtypeStruct((1, LANES), jnp.float32),
        ),
        in_specs=[SMEM, VMEM] + [VMEM] * len(weights),
        out_specs=(VMEM, VMEM),
        scratch_shapes=[pltpu.VMEM((wide, acts.shape[1]), jnp.float32)],
        cost_estimate=COST,
        compiler_params=LIMIT,
        name="finish_0",
    )(starts, acts, *weights)


def place(starts, acts, lengths_row, others, weights):
    wide = weights[0].shape[0] * len(weights)
    return pl.pallas_call(
        place_kernel,
        out_shape=pltpu.HBM((lengths_row.shape[1], wide), jnp.bfloat16),
        in_specs=[SMEM] + [VMEM] * (3 + len(weights)),
        out_specs=VMEM,
        scratch_shapes=[pltpu.VMEM((wide, acts.shape[1]), jnp.float32)],
        cost_estimate=COST,
        compiler_params=LIMIT,
        name="finish_1",
    )(starts, acts, lengths_row, others, *weights)


def spread(value):
    count = lax.axis_size(CHIPS)
    copies = jnp.broadcast_to(value[None], (count,) + value.shape)
    return lax.all_to_all(copies, CHIPS, 0, 0)


def in_order(own, peer, core):
    return jnp.concatenate(
        [jnp.where(core == 0, own, peer), jnp.where(core == 0, peer, own)], axis=0
    )


def beyond_slots(
    tokens, lengths_row, norm_gain, weights, w_out, decay_base, rate_base, group_gain, state
):
    core = lax.axis_index("c")
    count, feats = tokens.shape
    rows = count - SLOTS
    heads, head = state.shape[2], state.shape[-1]
    n_x, n_tp = lax.axis_size("x"), lax.axis_size(TP)
    chosen = live_slots(lengths_row, SLOTS, rows)
    live = jnp.sum((lengths_row > STEP).astype(jnp.float32))
    active = jnp.arange(rows) + SLOTS < live
    mine = jnp.dot(chosen.astype(jnp.bfloat16), tokens, preferred_element_type=jnp.float32)
    mine = mine.astype(jnp.bfloat16)
    held = jnp.argmax(chosen, axis=1)
    out_own = w_out.swapaxes(1, 2)
    out_peer = lax.ppermute(out_own, "c", PAIR)

    def block(natural, layer_parts):
        pairs, outs, gain_in, base, rate_b, gain, state_l = layer_parts
        joined = jnp.concatenate(
            [in_order(pairs[2 * m], pairs[2 * m + 1], core) for m in range(6)], axis=0
        )
        values = natural.astype(jnp.float32)
        factor = lax.rsqrt(jnp.mean(values * values, axis=1, keepdims=True) + RMS_EPS)
        normed = (values * factor * gain_in).astype(jnp.bfloat16)
        projected = lax.dot_general(
            normed, joined, ROWS_BY_ROWS, preferred_element_type=jnp.float32
        ).astype(jnp.bfloat16)
        arrived = lax.all_to_all(projected.reshape(n_x, rows, -1), "x", 0, 0)
        arrived = arrived.transpose(1, 0, 2).astype(jnp.float32)
        recept, key, value, decay_pre, rate_pre, gate_pre = [
            arrived[:, :, m * head : (m + 1) * head] for m in range(6)
        ]
        base, rate_b, gain = [part.reshape(heads, head) for part in (base, rate_b, gain)]
        decay = jnp.exp(-math.exp(-0.5) * jax.nn.sigmoid(base + decay_pre))
        rate = jax.nn.sigmoid(rate_b + rate_pre)
        length = jnp.maximum(jnp.sqrt(jnp.sum(key * key, axis=-1, keepdims=True)), 1e-12)
        unit = key / length
        old = jnp.take(state_l, held, axis=0)
        column = value * length - jnp.sum(old * unit[:, :, None, :], axis=-1)
        dot = jnp.sum(unit * rate * recept, axis=-1, keepdims=True)
        readout = jnp.sum(old * (decay * recept)[:, :, None, :], axis=-1) + column * dot
        centred = readout - jnp.mean(readout, axis=-1, keepdims=True)
        spread_ = jnp.mean(centred * centred, axis=-1, keepdims=True)
        normal = centred * lax.rsqrt(spread_ + GROUP_EPS) * gain * jax.nn.sigmoid(gate_pre)
        mixed = jnp.where(active[:, None, None], normal, 0.0)
        mixed = mixed.astype(jnp.bfloat16).reshape(rows, feats)
        mixed_all = spread(mixed).reshape(n_tp, n_x, rows, feats).transpose(1, 2, 0, 3)
        cols = lax.dot_general(
            mixed_all.reshape(n_x * rows, n_tp * feats), in_order(*outs, core),
            ROWS_BY_ROWS, preferred_element_type=jnp.float32,
        ).astype(jnp.bfloat16)
        blocks = spread(cols.reshape(rows, -1)).reshape(n_tp, n_x, n_x, rows, -1)
        current = blocks.transpose(2, 3, 0, 1, 4)
        here = lax.dynamic_slice_in_dim(current, lax.axis_index("x"), 1, 0)
        here = lax.dynamic_slice_in_dim(here, lax.axis_index(TP), 1, 2).reshape(rows, feats)
        terms = (arrived.reshape(rows, -1), column.reshape(rows, feats), here.astype(jnp.float32))
        return current.reshape(n_x * rows, n_tp * feats), jnp.concatenate(terms, axis=1)

    natural = spread(mine).reshape(n_tp, n_x, rows, feats).transpose(1, 2, 0, 3)
    layers = (weights, (out_own, out_peer), norm_gain, decay_base, rate_base, group_gain, state)
    return lax.scan(block, natural.reshape(n_x * rows, n_tp * feats), layers)[1]


def local(
    tokens, lengths, norm_gain, w_recept, w_key, w_value, w_decay, w_rate, w_gate, w_out,
    decay_base, rate_base, group_gain, state,
):
    core, spot = lax.axis_index("c"), lax.axis_index("x")
    rows, feats = tokens.shape
    n_x, n_tp, n_chips = lax.axis_size("x"), lax.axis_size(TP), lax.axis_size(CHIPS)
    starts = []
    for k in range(n_x):
        source = (spot + n_x - k) % n_x
        starts += [source * 2 + core, source * 2 + 1 - core]
    starts = jnp.stack(starts).astype(jnp.int32)
    core_at = jnp.reshape(core, (1,)).astype(jnp.int32)
    lengths_row = lengths.reshape(1, rows)

    def along_x(layer, more):
        own = jnp.concatenate([w_out.swapaxes(1, 2)[layer]] + more, axis=1)
        return [own] + [
            lax.ppermute(own, "x", [(i, (i + k) % n_x) for i in range(n_x)])
            for k in range(1, n_x)
        ]

    def over_pair(pieces):
        return [p for piece in pieces for p in (piece, lax.ppermute(piece, "c", PAIR))]

    chosen, count = choose(lengths_row, tokens, SLOTS, n_chips)
    acts = lax.all_to_all(chosen, CHIPS, 0, 0)
    weights = []
    for w in (w_recept, w_key, w_value, w_decay, w_rate, w_gate):
        own = w.swapaxes(1, 2)
        weights += [own, lax.ppermute(own, "c", PAIR)]
    states = [table(layer, SLOTS, lengths, state) for layer in range(2)]
    columns = [over_pair(along_x(0, [count])), over_pair(along_x(1, []))]
    operands = (
        tokens, lengths_row, norm_gain, weights, w_out, decay_base, rate_base, group_gain, state
    )
    new_state = None
    for layer in range(2):
        acts = acts.reshape(n_tp, n_x * SLOTS, feats)
        projected = project(layer, core_at, acts, norm_gain, weights, n_x)
        arrived = lax.all_to_all(projected, "x", 0, 0)
        mixed, column_terms = read_out(
            layer, arrived, lengths_row, decay_base, rate_base, group_gain, states[layer], n_tp
        )
        mixed_all = lax.all_to_all(mixed, TP, 0, 0)
        if layer == 0:
            current, most = finish(starts, mixed_all, columns[0], n_chips)
            others = lax.cond(
                most[0, 0] > SLOTS,
                beyond_slots,
                lambda *_: jnp.zeros((2, rows - SLOTS, 8 * feats), jnp.float32),
                *operands,
            )
            acts = lax.all_to_all(current, CHIPS, 0, 0)
        new_state = update(
            layer, lengths, arrived, decay_base, rate_base, column_terms, others, state, new_state
        )
    return place(starts, mixed_all, lengths_row, others, columns[1]), new_state


def solution(mesh):
    finer = Mesh(mesh.devices.reshape(4, 4, mesh.shape["dp"] // 2, 2), ("z", "y", "x", "c"))
    wide = P(None, None, TP + DP)
    in_specs = (
        (P(DP, TP), P(DP), P()) + (wide,) * 7 + (P(None, TP),) * 3 + (P(None, DP, TP, None, None),)
    )
    out_specs = (P(DP, TP), P(None, DP, TP, None, None))
    return jax.shard_map(local, mesh=finer, in_specs=in_specs, out_specs=out_specs, check_vma=False)
```
